128 devices in a mesh: sp: 32 (over z, y, core), tp: 4 (over x).
Axes of the slice: x: 4, y: 4, z: 4, core: 2. Of those that a mesh axis runs over, the one named last changes fastest.
Arguments:
- tokens: bfloat16 [16384, 2048], P(('sp', 'tp')), may hold values from -6 to 6
- norm_gain: float32 [2048], replicated, may hold values from 0.25 to 5
- w_query_one: bfloat16 [2048, 512], P(None, 'tp'), may hold values from -0.21875 to 0.21875
- w_query_two: bfloat16 [2048, 512], P(None, 'tp'), may hold values from -0.21875 to 0.21875
- w_key_one: bfloat16 [2048, 512], P(None, 'tp'), may hold values from -0.125 to 0.125
- w_key_two: bfloat16 [2048, 512], P(None, 'tp'), may hold values from -0.125 to 0.125
- w_value: bfloat16 [2048, 1024], P(None, 'tp'), may hold values from -0.125 to 0.125
- mix_lambda: float32 [8], P('tp'), may hold values from 0.3 to 0.8
- head_gain: float32 [128], replicated, may hold values from 0.1 to 1.9
- w_ret_query: bfloat16 [2048, 512], P(None, 'tp'), may hold values from -0.125 to 0.125
- w_ret_key: bfloat16 [2048, 512], P(None, 'tp'), may hold values from -0.125 to 0.125
- w_ret_value: bfloat16 [2048, 1024], P(None, 'tp'), may hold values from -0.125 to 0.125
- retain_log: float32 [8, 16384], P('tp', 'sp'), may hold values from -1 to 0
- init_state: float32 [8, 64, 128], P('tp'), may hold values from -144 to 144
- w_out_diff: bfloat16 [1024, 2048], P('tp'), may hold values from -0.125 to 0.125
- w_out_ret: bfloat16 [1024, 2048], P('tp'), may hold values from -0.125 to 0.125
Outputs:
- mixed: bfloat16 [16384, 2048], P(('sp', 'tp'))
The draws below stay inside these ranges and needn't reach their ends.
All inputs are finite; a program needn't handle non-finite values.
Results may differ from the reference program's by a relative error of at most 0.015.
The reference program's roundings to bfloat16 on the way count: a program that leaves them out, or rounds other values in their place, can miss the bound.
Values may be sent and summed in bfloat16 or wider, within the bound.
A program may use at most 128 MiB of HBM per device.

```python
import math
import jax
import jax.numpy as jnp
from jax import lax

D = 2048
HEADS_DIFF = 8
HEADS_RET = 8
HEAD = 64
VAL = 128
BLOCK = 256
TOK_DEV = 512
TOKENS = 16384


def draw_retain_log(key, part):
    keys = jax.random.split(jax.random.fold_in(key, 11), 7)
    slow = jax.random.bernoulli(keys[0], 0.5, (HEADS_RET,))
    slow_rate = jax.random.uniform(keys[1], (HEADS_RET,), minval=0.1, maxval=0.3) / TOKENS
    fast_rate = jnp.exp(jax.random.uniform(keys[2], (HEADS_RET,), minval=math.log(1.0 / 100.0), maxval=math.log(1.0 / 30.0)))
    fading_speed = jnp.where(slow, slow_rate, fast_rate)
    pace = jnp.exp(jax.random.uniform(keys[3], (TOKENS // TOK_DEV,), minval=-0.7, maxval=0.7))
    fading_speeds_list = jnp.repeat(pace, TOK_DEV)
    sampled_displacement = jnp.exp(jax.random.uniform(keys[4], (HEADS_RET, TOKENS), minval=-0.5, maxval=0.5))
    sequence_indices = jax.random.randint(keys[5], (HEADS_RET, 3), 0, TOKENS)
    stack_level = jnp.log(jax.random.uniform(keys[6], (HEADS_RET, 3), minval=0.5, maxval=0.8))
    sequence_index = jnp.arange(TOKENS, dtype=jnp.int32)
    cluster_sets = jnp.sum(jnp.where(sequence_index[None, None, :] == sequence_indices[:, :, None], stack_level[:, :, None], 0.0), axis=1)
    return (-fading_speed[:, None] * fading_speeds_list[None, :] * sampled_displacement + cluster_sets).astype(jnp.float32)


def draw_norm_gain(key, part):
    inner = jax.random.fold_in(key, 23)
    gains = 1.0 + 0.18 * jax.random.truncated_normal(inner, -4.0, 4.0, (D,))
    return gains.astype(jnp.float32)


def block_levels(stream_key, extent, pieces, low, largest):
    loudness, own = 1.0, jax.random.fold_in(stream_key, 6)
    for axis_at, parts in pieces:
        steps = jnp.exp(jax.random.uniform(jax.random.fold_in(own, axis_at), (parts,), jnp.float32, low / len(pieces), largest / len(pieces)))
        loudness = loudness * jnp.repeat(steps, extent[axis_at] // parts).reshape([-1 if axis == axis_at else 1 for axis in range(len(extent))])
    return loudness


def normal_values(own_key, dims, width, most, cuts=(), kind=jnp.bfloat16):
    gain = block_levels(own_key, dims, cuts, -0.22, 0.18) if cuts else 1.0
    entries = jax.random.normal(own_key, dims, jnp.float32) * width * gain
    return jnp.minimum(jnp.maximum(entries, -most), most).astype(kind)


def setup_inputs(seed: int = 0) -> dict:
    seeds = jax.random.split(jax.random.key(seed), 17)
    return {
        "tokens": normal_values(seeds[0], (TOKENS, D), 1.0, 6.0, ((0, 128),)),
        "norm_gain": draw_norm_gain(jax.random.fold_in(seeds[16], 71), 0),
        "w_query_one": normal_values(seeds[2], (D, HEADS_DIFF * HEAD), (D // 3) ** -0.5, 0.21875, ((1, 4),)),
        "w_query_two": normal_values(seeds[3], (D, HEADS_DIFF * HEAD), (D // 3) ** -0.5, 0.21875, ((1, 4),)),
        "w_key_one": normal_values(seeds[4], (D, HEADS_DIFF * HEAD), D ** -0.5, 0.125, ((1, 4),)),
        "w_key_two": normal_values(seeds[5], (D, HEADS_DIFF * HEAD), D ** -0.5, 0.125, ((1, 4),)),
        "w_value": normal_values(seeds[6], (D, HEADS_DIFF * VAL), D ** -0.5, 0.125, ((1, 4),)),
        "mix_lambda": jnp.clip(0.3 + 0.5 * jax.random.uniform(seeds[7], (HEADS_DIFF,), jnp.float32) ** block_levels(seeds[7], (HEADS_DIFF,), ((0, 4),), -0.2, 0.2), 0.3, 0.8),
        "head_gain": jnp.clip(1.0 + 0.18 * jax.random.normal(seeds[8], (VAL,), jnp.float32), 0.1, 1.9),
        "w_ret_query": normal_values(seeds[9], (D, HEADS_RET * HEAD), D ** -0.5, 0.125, ((1, 4),)),
        "w_ret_key": normal_values(seeds[10], (D, HEADS_RET * HEAD), D ** -0.5, 0.125, ((1, 4),)),
        "w_ret_value": normal_values(seeds[11], (D, HEADS_RET * VAL), D ** -0.5, 0.125, ((1, 4),)),
        "retain_log": draw_retain_log(jax.random.fold_in(seeds[16], 71), 0),
        "init_state": normal_values(seeds[13], (HEADS_RET, HEAD, VAL), 24.0, 144.0, ((0, 4),), jnp.float32),
        "w_out_diff": normal_values(seeds[14], (HEADS_DIFF * VAL, D), ((HEADS_DIFF + HEADS_RET) * VAL) ** -0.5, 0.125, ((0, 4),)),
        "w_out_ret": normal_values(seeds[15], (HEADS_RET * VAL, D), ((HEADS_DIFF + HEADS_RET) * VAL) ** -0.5, 0.125, ((0, 4),)),
    }


NORM_EPS = 1e-06
HEAD_EPS = 1e-05
DIFF_SCALE = 0.8
HIGHEST = lax.Precision.HIGHEST

def head_norm(values):
    return values * lax.rsqrt(lax.optimization_barrier(jnp.mean(values * values, axis=-1, keepdims=True)) + HEAD_EPS)

def diff_head(query_one, query_two, key_one, key_two, values, weight_two):
    total_rows = query_one.shape[0]
    block_rows = math.gcd(total_rows, 512)
    key_pos = jnp.arange(total_rows, dtype=jnp.int32)

    def one_block(number):
        begin_at = (number * block_rows).astype(jnp.int32)
        allowed = (begin_at + jnp.arange(block_rows, dtype=jnp.int32))[:, None] >= key_pos[None, :]

        def soft_map(query, keys):
            portion = lax.dynamic_slice_in_dim(query, begin_at, block_rows, 0)
            scores = jnp.dot(portion, keys.T, preferred_element_type=jnp.float32) * HEAD ** (-0.5)
            scores = jnp.where(allowed, scores, -jnp.inf)
            shifted = jnp.exp(scores - lax.optimization_barrier(jnp.max(scores, axis=-1, keepdims=True)))
            weighted = jnp.dot(shifted.astype(jnp.bfloat16), values, preferred_element_type=jnp.float32)
            return weighted / lax.optimization_barrier(jnp.sum(shifted, axis=-1, keepdims=True))
        return soft_map(query_one, key_one) - weight_two * soft_map(query_two, key_two)
    blocks = lax.map(one_block, jnp.arange(total_rows // block_rows, dtype=jnp.int32))
    return blocks.reshape(total_rows, VAL)

def retention(ret_query, ret_key, ret_value, retain_log, init_state):
    nblocks = TOKENS // BLOCK

    def split_blocks(data, size):
        return data.reshape(nblocks, BLOCK, HEADS_RET, size).transpose(0, 2, 1, 3)
    block_query = split_blocks(ret_query, HEAD)
    block_key = split_blocks(ret_key, HEAD)
    block_value = split_blocks(ret_value, VAL)
    log_blocks = retain_log.reshape(HEADS_RET, nblocks, BLOCK).transpose(1, 0, 2)
    sequence_index = jnp.arange(BLOCK, dtype=jnp.int32)
    causal = sequence_index[:, None] >= sequence_index[None, :]

    def ret_step(memory, inputs):
        query, keys, values, logs = inputs
        query_f = query.astype(jnp.float32)
        keys_f = keys.astype(jnp.float32)
        values_f = values.astype(jnp.float32)
        cumulative = jnp.cumsum(logs, axis=-1)
        gap_log = jnp.where(causal[None], cumulative[:, :, None] - cumulative[:, None, :], -jnp.inf)
        raw = jnp.einsum('hqd,hkd->hqk', query_f, keys_f, precision=HIGHEST)
        decayed = (raw * HEAD ** (-0.5) * jnp.exp(gap_log)).astype(jnp.bfloat16).astype(jnp.float32)
        result = jnp.einsum('hqk,hke->hqe', decayed, values_f, precision=HIGHEST)
        result = result + jnp.einsum('hqd,hde->hqe', query_f * jnp.exp(cumulative)[:, :, None], memory, precision=HIGHEST)
        last_log = cumulative[:, -1:]
        key_scaled = (keys_f * HEAD ** (-0.5) * jnp.exp(last_log - cumulative)[:, :, None]).astype(jnp.bfloat16).astype(jnp.float32)
        memory = jnp.exp(last_log)[:, :, None] * memory + jnp.einsum('hkd,hke->hde', key_scaled, values_f, precision=HIGHEST)
        return (memory, result)
    final_state, outputs = lax.scan(ret_step, init_state, (block_query, block_key, block_value, log_blocks))
    outputs = outputs.transpose(0, 2, 1, 3).reshape(TOKENS, HEADS_RET, VAL)
    return head_norm(outputs).reshape(TOKENS, HEADS_RET * VAL).astype(jnp.bfloat16)

def reference(tokens, norm_gain, w_query_one, w_query_two, w_key_one, w_key_two, w_value, mix_lambda, head_gain, w_ret_query, w_ret_key, w_ret_value, retain_log, init_state, w_out_diff, w_out_ret):
    floats = tokens.astype(jnp.float32)
    normed = (floats * lax.rsqrt(lax.optimization_barrier(jnp.mean(floats * floats, axis=-1, keepdims=True)) + NORM_EPS) * norm_gain).astype(jnp.bfloat16)

    def project(weight):
        return jnp.dot(normed, weight, preferred_element_type=jnp.float32).astype(jnp.bfloat16)
    query_one = project(w_query_one).reshape(TOKENS, HEADS_DIFF, HEAD)
    query_two = project(w_query_two).reshape(TOKENS, HEADS_DIFF, HEAD)
    key_one = project(w_key_one).reshape(TOKENS, HEADS_DIFF, HEAD)
    key_two = project(w_key_two).reshape(TOKENS, HEADS_DIFF, HEAD)
    values = project(w_value).reshape(TOKENS, HEADS_DIFF, VAL)
    head_outs = []
    for number in range(HEADS_DIFF):
        head_outs.append(diff_head(query_one[:, number], query_two[:, number], key_one[:, number], key_two[:, number], values[:, number], mix_lambda[number]))
    mixed_heads = jnp.stack(head_outs, axis=1)
    diff_out = (head_norm(mixed_heads) * head_gain * DIFF_SCALE).reshape(TOKENS, HEADS_DIFF * VAL).astype(jnp.bfloat16)
    ret_out = retention(project(w_ret_query), project(w_ret_key), project(w_ret_value), retain_log, init_state)
    total = jnp.dot(diff_out, w_out_diff, preferred_element_type=jnp.float32) + jnp.dot(ret_out, w_out_ret, preferred_element_type=jnp.float32)
    return total.astype(jnp.bfloat16)
```

```python
import jax
import jax.numpy as jnp
from jax import lax
from jax.experimental import pallas as pl
from jax.experimental.pallas import tpu as pltpu
from jax.sharding import PartitionSpec as P

NORM_EPS = 1e-06
HEAD_EPS = 1e-05
DIFF_SCALE = 0.8
MESH = pl.DeviceIdType.MESH
F32 = jnp.float32
BF16 = jnp.bfloat16
HIGHEST = lax.Precision.HIGHEST
LOWEST = -3.0e38

ORDER = (
    (0, 0), (0, 1), (0, -1), (1, 0), (-1, 0), (0, 2), (2, 0), (1, 1),
    (1, -1), (-1, 1), (-1, -1), (1, 2), (2, 1), (-1, 2), (2, -1), (2, 2),
)
PLUS_Y, MINUS_Y, PLUS_Z, MINUS_Z = range(4)


def nt(a, b, precision=None):
    return lax.dot_general(
        a, b, (((1,), (1,)), ((), ())), preferred_element_type=F32, precision=precision
    )


def mm(a, b, precision=None):
    return jnp.dot(a, b, preferred_element_type=F32, precision=precision)


def head_norm(values, axis):
    return values * lax.rsqrt(jnp.mean(values * values, axis=axis, keepdims=True) + HEAD_EPS)


def kernel(
    tokens, gain, wq1, wq2, wk1, wk2, wv, mix, hgain, wrq, wrk, wrv, logs, init, wod, wor,
    out,
    rows, weights, proj, kva, kvb, wout, lgs, qrecv, qpad, acc, peak, denom, local, rgate,
    dsend, rsend, heads,
    load_sem, x_send, x_recv, w_send, w_recv, l_send, l_recv, lsib_send, kv_send, kv_recv,
    sib_send, q_sem, o_send, o_recv,
):
    sp = lax.axis_index("sp")
    t = lax.axis_index("tp")
    z, y, c = lax.div(sp, 8), lax.rem(lax.div(sp, 2), 4), lax.rem(sp, 2)
    partner = 31 - sp
    sib = (sp + 1 - 2 * c, t)
    kv = (kva, kvb)

    def place(dz, dy, lane):
        return (lax.rem(z + dz + 4, 4) * 4 + lax.rem(y + dy + 4, 4)) * 2 + lane

    near = (
        (place(0, 1, c), t), (place(0, -1, c), t), (place(1, 0, c), t), (place(-1, 0, c), t),
    )
    xs = [(sp, lax.rem(t + d, 4)) for d in range(4)]

    loads = []
    sources = (
        (wq1, 0, 128), (wq2, 128, 128), (wk1, 256, 128), (wk2, 384, 128), (wv, 512, 256),
        (wrq, 768, 128), (wrk, 896, 128), (wrv, 1024, 256),
    )
    for k, (ref, at, width) in enumerate(sources):
        loads.append(pltpu.make_async_copy(ref, weights.at[:, pl.ds(at, width)], load_sem.at[k]))
    for k, ref in enumerate((wod, wor)):
        loads.append(pltpu.make_async_copy(ref, wout.at[t, k], load_sem.at[8 + k]))
    for load in loads:
        load.start()

    barrier = pltpu.get_barrier_semaphore()
    peers = [xs[1], xs[2], xs[3], sib, *near] + [(partner, d) for d in range(4)]
    for peer in peers:
        pl.semaphore_signal(barrier, inc=1, device_id=peer, device_id_type=MESH)

    for chunk in range(2):
        floats = tokens[chunk * 64 : chunk * 64 + 64].astype(F32)
        scale = lax.rsqrt(jnp.mean(floats * floats, axis=-1, keepdims=True) + NORM_EPS)
        rows[t, chunk * 64 : chunk * 64 + 64] = (floats * scale * gain[...]).astype(BF16)
    lg = logs[...]
    total = jnp.sum(lg, axis=1, keepdims=True)
    head_row = lax.broadcasted_iota(jnp.int32, (8, 128), 0)
    lgs[sp] = jnp.where(head_row == 0, total[0:1], total[1:2])

    pl.semaphore_wait(barrier, len(peers))

    def remote(src, dst, ssem, rsem, dev):
        return pltpu.make_async_remote_copy(
            src_ref=src, dst_ref=dst, send_sem=ssem, recv_sem=rsem, device_id=dev,
            device_id_type=MESH,
        )

    def x_copy(slot, chunk, way, n):
        piece = rows.at[slot, pl.ds(chunk * 64, 64)]
        return remote(piece, piece, x_send.at[n], x_recv.at[slot, chunk], xs[way])

    def w_copy(slot, parts, way, n):
        piece = wout.at[slot, c] if parts is None else wout.at[slot, c, pl.ds(parts * 128, 128)]
        rsem = w_recv.at[slot, 0 if parts is None else parts]
        return remote(piece, piece, w_send.at[n], rsem, xs[way])

    def w_sib(slot, n, kind):
        piece = wout.at[slot, kind]
        return remote(piece, piece, w_send.at[4 + n], w_recv.at[slot, 2], sib)

    l_sends = []

    def l_copy(dz, dy, way):
        j = place(dz, dy, c)
        n = len(l_sends)
        copy = remote(lgs.at[j], lgs.at[j], l_send.at[n], l_recv.at[j], near[way])
        l_sends.append(n)
        copy.start()

    l_sibs = []

    def l_sib(dz, dy):
        j = place(dz, dy, c)
        n = len(l_sibs)
        l_sibs.append(n)
        remote(lgs.at[j], lgs.at[j], lsib_send.at[n], l_recv.at[j], sib).start()

    def l_wait(dz, dy, lane=None):
        j = place(dz, dy, c if lane is None else lane)
        remote(lgs.at[j], lgs.at[j], l_send.at[0], l_recv.at[j], sib).wait_recv()

    def l_stage(stage):
        if stage == 0:
            for way in range(4):
                l_copy(0, 0, way)
            l_sib(0, 0)
        elif stage == 1:
            for dy in (1, -1):
                l_wait(0, dy)
                l_copy(0, dy, PLUS_Z)
                l_copy(0, dy, MINUS_Z)
                l_sib(0, dy)
            l_copy(0, -1, PLUS_Y)
            for dz in (1, -1):
                l_wait(dz, 0)
                l_sib(dz, 0)
            l_copy(-1, 0, PLUS_Z)
        elif stage == 2:
            l_wait(0, 2)
            l_copy(0, 2, PLUS_Z)
            l_copy(0, 2, MINUS_Z)
            l_sib(0, 2)
            for dy in (1, -1):
                for dz in (1, -1):
                    l_wait(dz, dy)
                    l_sib(dz, dy)
                l_copy(-1, dy, PLUS_Z)
            l_wait(2, 0)
            l_sib(2, 0)
        elif stage == 3:
            for dz in (1, -1):
                l_wait(dz, 2)
                l_sib(dz, 2)
            l_copy(-1, 2, PLUS_Z)
            for dy in (1, -1):
                l_wait(2, dy)
                l_sib(2, dy)
        else:
            l_wait(2, 2)
            l_sib(2, 2)

    x_copy(t, 0, 1, 0).start()
    x_copy(t, 1, 3, 1).start()
    x_copy(t, 1, 1, 2).start()
    x_copy(t, 0, 3, 3).start()
    l_stage(0)

    for load in loads[:8]:
        load.wait()

    left, right, far = lax.rem(t + 3, 4), lax.rem(t + 1, 4), lax.rem(t + 2, 4)

    def project(k, carry):
        @pl.when(k == 1)
        def _():
            x_copy(left, 0, 1, 0).wait_recv()
            x_copy(left, 0, 1, 4).start()
            x_copy(right, 1, 3, 0).wait_recv()
            x_copy(right, 1, 3, 5).start()
            x_copy(left, 1, 1, 0).wait_recv()
            l_stage(1)

        @pl.when(k == 2)
        def _():
            x_copy(right, 0, 3, 0).wait_recv()
            l_stage(2)
            for load in loads[8:]:
                load.wait()
            w_copy(t, None, 1, 0).start()
            w_copy(t, None, 3, 1).start()

        @pl.when(k == 3)
        def _():
            l_stage(3)
            x_copy(far, 0, 1, 0).wait_recv()
            x_copy(far, 1, 3, 0).wait_recv()

        slot = lax.rem(t + jnp.where(k == 1, 3, jnp.where(k == 2, 1, jnp.where(k == 3, 2, 0))), 4)
        at = pl.multiple_of(slot * 128, 128)
        for n in range(5):
            block = mm(rows[slot], weights[:, n * 256 : n * 256 + 256])
            proj[n, pl.ds(at, 128)] = block.astype(BF16)
        return carry

    lax.fori_loop(0, 4, project, 0)
    l_stage(4)

    def transposed(n, e):
        return proj[n, e * 256 : e * 256 + 256].astype(F32).T.astype(BF16)

    kva[sp, 0] = proj[1, 0:256]
    kva[sp, 1] = transposed(2, 0)
    for way in (PLUS_Y, MINUS_Y, PLUS_Z, MINUS_Z):
        remote(
            kva.at[sp], kva.at[sp], kv_send.at[way, 0], kv_recv.at[sp, 0, 0], near[way]
        ).start()

    local[1] = transposed(0, 1)
    q_copy = remote(local.at[1], qrecv, q_sem.at[0], q_sem.at[1], (partner, t))
    q_copy.start()

    row = lax.broadcasted_iota(jnp.int32, (256, 256), 0)
    col = lax.broadcasted_iota(jnp.int32, (256, 256), 1)
    lane = lax.broadcasted_iota(jnp.int32, (256, 128), 1)
    state_row = lax.broadcasted_iota(jnp.int32, (128, 128), 0)
    upper = jnp.where(row <= col, 1.0, 0.0)
    adds, fades, queries = [], [], []
    for b in range(2):
        span = slice(b * 256, b * 256 + 256)
        lb = lg[:, span]
        cum_rows = mm(jnp.concatenate([lb, lb, lb, lb], axis=0), upper, HIGHEST)
        rq, rk = proj[3, span, 0:128], proj[3, span, 128:256]
        cols, lasts = [], []
        for h in range(2):
            cum_col = jnp.sum(jnp.where(col <= row, lb[h : h + 1], 0.0), axis=1, keepdims=True)
            cols.append(cum_col)
            lasts.append(jnp.sum(lb[h : h + 1], axis=1, keepdims=True))
            mine = (lane < 64) if h == 0 else (lane >= 64)
            raw = nt(jnp.where(mine, rq, jnp.zeros_like(rq)), rk)
            gap = jnp.where(col <= row, cum_col - cum_rows[h : h + 1], -jnp.inf)
            gate = (raw * 0.125 * jnp.exp(gap)).astype(BF16)
            rgate[b, h] = mm(gate, proj[4, span, h * 128 : h * 128 + 128])
        factor = jnp.where(lane < 64, jnp.exp(lasts[0] - cols[0]), jnp.exp(lasts[1] - cols[1]))
        keys = (rk.astype(F32) * 0.125 * factor).T.astype(BF16)
        both = mm(keys, proj[4, span])
        adds.append(jnp.where(state_row < 64, both[:, 0:128], both[:, 128:256]))
        fades.append(jnp.where(state_row < 64, jnp.exp(lasts[0]), jnp.exp(lasts[1])))
        grow = jnp.where(lane < 64, jnp.exp(cols[0]), jnp.exp(cols[1]))
        queries.append(rq.astype(F32) * grow)
    own_state = (fades[1] * adds[0] + adds[1]).astype(BF16)
    pack = jnp.concatenate([own_state[0:64], own_state[64:128]], axis=1)

    kvb[sp, 0, 0:256] = proj[1, 256:512]
    kvb[sp, 1, 0:256] = transposed(2, 1)
    kvb[sp, 0, 256:288] = pack[0:32]
    kvb[sp, 1, 256:288] = pack[32:64]
    for way in (PLUS_Z, MINUS_Z, PLUS_Y, MINUS_Y):
        remote(
            kvb.at[sp], kvb.at[sp], kv_send.at[way, 1], kv_recv.at[sp, 1, 0], near[way]
        ).start()

    sib_number = {}

    def to_sib(e, dz, dy):
        j = place(dz, dy, c)
        n = sib_number.setdefault((e, dz, dy), len(sib_number))
        remote(kv[e].at[j], kv[e].at[j], sib_send.at[n], kv_recv.at[j, e, 0], sib).start()

    ways_used = [2, 2, 2, 2]
    sends = []

    def whole(e, dz, dy, way):
        j = place(dz, dy, c)
        n = ways_used[way]
        ways_used[way] += 1
        sends.append((way, n, e, None))
        remote(kv[e].at[j], kv[e].at[j], kv_send.at[way, n], kv_recv.at[j, e, 0], near[way]).start()

    def part(e, dz, dy, p, way):
        j = place(dz, dy, c)
        n = ways_used[way]
        ways_used[way] += 1
        sends.append((way, n, e, p))
        remote(
            kv[e].at[j, p], kv[e].at[j, p], kv_send.at[way, n], kv_recv.at[j, e, p], near[way]
        ).start()

    def wait_whole(e, dz, dy, from_lane=None):
        j = place(dz, dy, c if from_lane is None else from_lane)
        remote(kv[e].at[j], kv[e].at[j], kv_send.at[0, 0], kv_recv.at[j, e, 0], sib).wait_recv()

    def wait_parts(e, dz, dy):
        j = place(dz, dy, c)
        for p in range(2):
            remote(
                kv[e].at[j, p], kv[e].at[j, p], kv_send.at[0, 0], kv_recv.at[j, e, p], sib
            ).wait_recv()

    to_sib(0, 0, 0)
    to_sib(1, 0, 0)

    def queries_of(half, block):
        big = block.astype(F32) * 0.125
        for hm in range(4):
            own = lax.div(row, 64) == hm
            qpad[half, hm] = jnp.where(own, big, 0.0).astype(BF16)

    queries_of(0, transposed(0, 0))
    for half in range(2):
        for hm in range(4):
            peak[half, hm] = jnp.full((1, 256), LOWEST, F32)
            denom[half, hm] = jnp.zeros((1, 256), F32)
            acc[half, hm] = jnp.zeros((128, 256), F32)
    q_copy.wait_recv()
    queries_of(1, qrecv[...])

    def attend(half, j, masked):
        def scores(hm):
            return [mm(kv[e][j, 0, 0:256], qpad[half, hm]) for e in range(2)]

        later = scores(0)
        for hm in range(4):
            now = later
            if hm < 3:
                later = scores(hm + 1)
            if masked:
                now = [
                    jnp.where(row + e * 256 <= col + half * 256, now[e], -jnp.inf) for e in range(2)
                ]
            old = peak[half, hm]
            new = jnp.maximum(old, jnp.max(jnp.maximum(now[0], now[1]), axis=0, keepdims=True))
            fade = jnp.exp(old - new)
            terms = [jnp.exp(now[e] - new) for e in range(2)]
            denom[half, hm] = denom[half, hm] * fade + jnp.sum(
                terms[0] + terms[1], axis=0, keepdims=True
            )
            h = hm % 2
            weighted = sum(
                mm(kv[e][j, 1, h * 128 : h * 128 + 128], terms[e].astype(BF16)) for e in range(2)
            )
            acc[half, hm] = acc[half, hm] * fade + weighted
            peak[half, hm] = new

    def event(n):
        if n == 2:
            for dy in (1, -1):
                wait_whole(0, 0, dy)
            part(0, 0, -1, 0, PLUS_Y)
            part(0, 0, 1, 1, MINUS_Y)
            for dz in (1, -1):
                wait_whole(0, dz, 0)
            part(0, -1, 0, 0, PLUS_Z)
            part(0, 1, 0, 1, MINUS_Z)
            for d in (1, -1):
                to_sib(0, 0, d)
                to_sib(0, d, 0)
        elif n == 4:
            for dz in (1, -1):
                wait_whole(1, dz, 0)
            part(1, -1, 0, 0, PLUS_Z)
            part(1, 1, 0, 1, MINUS_Z)
            for dy in (1, -1):
                wait_whole(1, 0, dy)
            part(1, 0, -1, 0, PLUS_Y)
            part(1, 0, 1, 1, MINUS_Y)
            for d in (1, -1):
                for way in (PLUS_Z, MINUS_Z):
                    whole(0, 0, d, way)
                for way in (PLUS_Y, MINUS_Y):
                    whole(1, d, 0, way)
            for d in (1, -1):
                to_sib(1, 0, d)
                to_sib(1, d, 0)
        elif n == 6:
            wait_parts(0, 0, 2)
            for way in (PLUS_Z, MINUS_Z):
                whole(0, 0, 2, way)
            wait_parts(1, 2, 0)
            for way in (PLUS_Y, MINUS_Y):
                whole(1, 2, 0, way)
            wait_parts(0, 2, 0)
            wait_parts(1, 0, 2)
            for e in range(2):
                to_sib(e, 0, 2)
                to_sib(e, 2, 0)
        elif n in (8, 10, 12):
            d = {8: 1, 10: -1, 12: 2}[n]
            for s in (1, -1):
                wait_whole(0, s, d)
                wait_whole(1, d, s)
            part(0, -1, d, 0, PLUS_Z)
            part(0, 1, d, 1, MINUS_Z)
            part(1, d, -1, 0, PLUS_Y)
            part(1, d, 1, 1, MINUS_Y)
            for s in (1, -1):
                to_sib(0, s, d)
                to_sib(1, d, s)
        else:
            d = {13: 1, 14: -1, 15: 2}[n]
            wait_parts(0, 2, d)
            wait_parts(1, d, 2)
            to_sib(0, 2, d)
            to_sib(1, d, 2)

    def w_stage(stage):
        if stage == 1:
            w_copy(left, None, 1, 0).wait_recv()
            w_copy(left, 0, 1, 2).start()
            w_copy(right, None, 3, 0).wait_recv()
            w_copy(right, 1, 3, 3).start()
            w_sib(left, 0, c).start()
            w_sib(right, 1, c).start()
        else:
            w_copy(far, 0, 1, 0).wait_recv()
            w_copy(far, 1, 3, 0).wait_recv()
            w_sib(far, 2, c).start()

    bounds = (sp, partner)

    def pick(values, s):
        chosen = jnp.int32(values[0])
        for k, value in enumerate(values[1:], 1):
            chosen = jnp.where(s == k, jnp.int32(value), chosen)
        return chosen

    def step(s, carry):
        for at, events in ((1, (2, 4)), (5, (6,)), (7, (8,)), (8, (10,)), (11, (12, 13)), (13, (14,)), (15, (15,))):
            @pl.when(s == at)
            def _():
                for n in events:
                    event(n)
                if at == 8:
                    w_stage(1)
                if at == 13:
                    w_stage(2)

        dz, dy = pick([o[0] for o in ORDER], s), pick([o[1] for o in ORDER], s)

        def one_lane(l, carry):
            lane_of = lax.rem(c + l, 2)
            j = place(dz, dy, lane_of)

            @pl.when(l == 1)
            def _():
                for e in range(2):
                    remote(
                        kv[e].at[j], kv[e].at[j], kv_send.at[0, 0], kv_recv.at[j, e, 0], sib
                    ).wait_recv()

            def one_half(half, carry):
                bound = jnp.where(half == 0, bounds[0], bounds[1])

                @pl.when(j < bound)
                def _():
                    attend(half, j, False)

                @pl.when(j == bound)
                def _():
                    attend(half, j, True)

                return carry

            return lax.fori_loop(0, 2, one_half, carry)

        return lax.fori_loop(0, 2, one_lane, carry)

    lax.fori_loop(0, 16, step, 0)
    assert ways_used == [10] * 4 and len(sends) == 32 and len(sib_number) == 32
    assert len(l_sends) == 15 and len(l_sibs) == 16

    def finish(half):
        sides = []
        for h in range(2):
            weight_two = mix[pl.ds(h, 1), :]
            first = acc[half, h] / denom[half, h]
            second = acc[half, 2 + h] / denom[half, 2 + h]
            attn = first - weight_two * second
            normal = (head_norm(attn, 0) * DIFF_SCALE).T * hgain[...]
            sides.append(normal)
        dsend[half] = jnp.concatenate(sides, axis=1).astype(BF16)

    def o_copy(kind, src, dev, n):
        return remote(src, heads.at[kind, t], o_send.at[n], o_recv.at[kind, t], dev)

    def o_local(kind, src, n):
        return pltpu.make_async_copy(src, heads.at[kind, t], o_send.at[n])

    finish(0)
    for d in range(2):
        piece = dsend.at[0, pl.ds(d * 128, 128)]

        @pl.when(t == d)
        def _():
            o_local(0, piece, d).start()

        @pl.when(t != d)
        def _():
            o_copy(0, piece, (sp, d), d).start()

    finish(1)
    for d in range(2):
        o_copy(0, dsend.at[1, pl.ds(d * 128, 128)], (partner, 2 + d), 2 + d).start()

    def chain(j, state):
        fade = jnp.exp(lgs[j])
        pair = jnp.concatenate([kvb[j, 0, 256:288], kvb[j, 1, 256:288]], axis=0).astype(F32)
        own = jnp.concatenate([pair[:, 0:128], pair[:, 128:256]], axis=0)
        return state * jnp.where(state_row < 64, fade[0:1], fade[1:2]) + own

    for dz, dy in ORDER:
        l_wait(dz, dy, 1 - c)
    state = lax.fori_loop(0, sp, chain, jnp.concatenate([init[0], init[1]], axis=0))
    for b in range(2):
        for h in range(2):
            mine = (lane < 64) if h == 0 else (lane >= 64)
            older = mm(jnp.where(mine, queries[b], 0.0), state, HIGHEST)
            r = rgate[b, h] + older
            rsend[b * 256 : b * 256 + 256, h * 128 : h * 128 + 128] = head_norm(r, 1).astype(BF16)
        state = fades[b] * state + adds[b]
    for d in range(4):
        piece = rsend.at[pl.ds(d * 128, 128)]

        @pl.when(t == d)
        def _():
            o_local(1, piece, 4 + d).start()

        @pl.when(t != d)
        def _():
            o_copy(1, piece, (sp, d), 4 + d).start()

    for slot, _ in ((left, 0), (right, 1), (far, 2)):
        piece = wout.at[slot, 1 - c]
        remote(piece, piece, w_send.at[0], w_recv.at[slot, 2], sib).wait_recv()

    for slot in range(4):
        landed = remote(heads.at[0, slot], heads.at[0, slot], o_send.at[0], o_recv.at[0, slot], sib)

        @pl.when(jnp.logical_or(t != slot, t >= 2))
        def _():
            landed.wait_recv()

        ret = remote(heads.at[1, slot], heads.at[1, slot], o_send.at[0], o_recv.at[1, slot], sib)

        @pl.when(t != slot)
        def _():
            ret.wait_recv()

    for n in range(2):
        piece = dsend.at[0, pl.ds(n * 128, 128)]

        @pl.when(t == n)
        def _():
            o_local(0, piece, n).wait()

        @pl.when(t != n)
        def _():
            o_copy(0, piece, sib, n).wait_send()

        o_copy(0, piece, sib, 2 + n).wait_send()
    for n in range(4):
        piece = rsend.at[pl.ds(n * 128, 128)]

        @pl.when(t == n)
        def _():
            o_local(1, piece, 4 + n).wait()

        @pl.when(t != n)
        def _():
            o_copy(1, piece, sib, 4 + n).wait_send()

    def columns(n, carry):
        at = pl.ds(pl.multiple_of(n * 512, 512), 512)
        block = jnp.zeros((128, 512), F32)
        for slot in range(4):
            for kind in range(2):
                block += mm(heads[kind, slot], wout[slot, kind, :, at])
        out[:, at] = block.astype(BF16)
        return carry

    lax.fori_loop(0, 4, columns, 0)

    for n in range(6):
        x_copy(t, 0, 1, n).wait_send()
    for n in range(2):
        w_copy(t, None, 1, n).wait_send()
        w_copy(t, n, 1, 2 + n).wait_send()
    for n in range(3):
        w_sib(t, n, c).wait_send()
    for n in l_sends:
        remote(lgs.at[0], lgs.at[0], l_send.at[n], l_recv.at[0], sib).wait_send()
    for n in l_sibs:
        remote(lgs.at[0], lgs.at[0], lsib_send.at[n], l_recv.at[0], sib).wait_send()
    q_copy.wait_send()
    for way in range(4):
        for e in range(2):
            remote(
                kv[e].at[0], kv[e].at[0], kv_send.at[way, e], kv_recv.at[0, 0, 0], sib
            ).wait_send()
    for way, n, e, p in sends:
        piece = kv[e].at[0] if p is None else kv[e].at[0, 0]
        remote(piece, piece, kv_send.at[way, n], kv_recv.at[0, 0, 0], sib).wait_send()
    for (e, _, _), n in sib_number.items():
        remote(kv[e].at[0], kv[e].at[0], sib_send.at[n], kv_recv.at[0, 0, 0], sib).wait_send()


def on_device(
    tokens, norm_gain, w_query_one, w_query_two, w_key_one, w_key_two, w_value, mix_lambda,
    head_gain, w_ret_query, w_ret_key, w_ret_value, retain_log, init_state, w_out_diff, w_out_ret,
):
    vmem = pl.BlockSpec(memory_space=pltpu.VMEM)
    hbm = pl.BlockSpec(memory_space=pl.ANY)
    dma = pltpu.SemaphoreType.DMA
    return pl.pallas_call(
        kernel,
        out_shape=jax.ShapeDtypeStruct((128, 2048), BF16),
        in_specs=[vmem, vmem] + [hbm] * 5 + [vmem, vmem] + [hbm] * 3 + [vmem, vmem] + [hbm] * 2,
        out_specs=vmem,
        scratch_shapes=[
            pltpu.VMEM((4, 128, 2048), BF16),
            pltpu.VMEM((2048, 1280), BF16),
            pltpu.VMEM((5, 512, 256), BF16),
            pltpu.VMEM((32, 2, 256, 256), BF16),
            pltpu.VMEM((32, 2, 288, 256), BF16),
            pltpu.VMEM((4, 2, 256, 2048), BF16),
            pltpu.VMEM((32, 8, 128), F32),
            pltpu.VMEM((256, 256), BF16),
            pltpu.VMEM((2, 4, 256, 256), BF16),
            pltpu.VMEM((2, 4, 128, 256), F32),
            pltpu.VMEM((2, 4, 1, 256), F32),
            pltpu.VMEM((2, 4, 1, 256), F32),
            pltpu.VMEM((2, 256, 256), BF16),
            pltpu.VMEM((2, 2, 256, 128), F32),
            pltpu.VMEM((2, 256, 256), BF16),
            pltpu.VMEM((512, 256), BF16),
            pltpu.VMEM((2, 4, 128, 256), BF16),
            dma((10,)),
            dma((6,)),
            dma((4, 2)),
            dma((7,)),
            dma((4, 3)),
            dma((16,)),
            dma((32,)),
            dma((16,)),
            dma((4, 10)),
            dma((32, 2, 2)),
            dma((32,)),
            dma((2,)),
            dma((8,)),
            dma((2, 4)),
        ],
        compiler_params=pltpu.CompilerParams(
            collective_id=0, has_side_effects=True, vmem_limit_bytes=60 * 1024 * 1024
        ),
        cost_estimate=pl.CostEstimate(
            flops=20_000_000_000, bytes_accessed=10_000_000, transcendentals=17_000_000
        ),
        name="layer",
    )(
        tokens, norm_gain.reshape(1, -1), w_query_one, w_query_two, w_key_one, w_key_two, w_value,
        jnp.broadcast_to(mix_lambda[:, None], (2, 256)), head_gain.reshape(1, -1),
        w_ret_query, w_ret_key, w_ret_value, retain_log, init_state, w_out_diff, w_out_ret,
    )


def solution(mesh):
    both = ("sp", "tp")
    return jax.shard_map(
        on_device,
        mesh=mesh,
        in_specs=(
            P(both, None), P(), P(None, "tp"), P(None, "tp"), P(None, "tp"), P(None, "tp"),
            P(None, "tp"), P("tp"), P(), P(None, "tp"), P(None, "tp"), P(None, "tp"),
            P("tp", "sp"), P("tp", None, None), P("tp", None), P("tp", None),
        ),
        out_specs=P(both, None),
        check_vma=False,
    )
```

```python
import jax
import jax.numpy as jnp
from jax import lax
from jax.experimental import pallas as pl
from jax.experimental.pallas import tpu as pltpu
from jax.sharding import PartitionSpec as P

NORM_EPS = 1e-06
HEAD_EPS = 1e-05
DIFF_SCALE = 0.8
MESH = pl.DeviceIdType.MESH
F32 = jnp.float32
BF16 = jnp.bfloat16
HIGHEST = lax.Precision.HIGHEST
LOWEST = -3.0e38


SCHEDULE = (
    (((0, 0, 0), (-1, 0, 0), (0, -1, 0), (0, 1, 0), (1, 0, 0), (0, 0, 1), (2, 0, 0), (0, 2, 0), (1, -1, 0), (0, 1, 1), (0, 0, 2), (-1, -1, 0), (0, -1, 1), (1, 1, 0), (-1, 1, 0), (1, 0, 1), (0, -1, 2), (0, 1, 2), (0, 0, 3), (-1, 0, 1), (1, 2, 0), (0, 2, 1), (1, 1, 1)), (0, 0, 0)),
    (((-1, 2, 0), (1, 0, 2)), (0, 1, 0)),
    ((), (0, -1, 0)),
    (((1, -1, 1), (0, 2, 2)), (1, 0, 0)),
    (((-1, 0, 2),), (0, 0, 1)),
    (((1, 0, 3),), (-1, 0, 0)),
    (((0, -1, 3), (0, 1, 3), (2, -1, 0)), (0, 2, 0)),
    (((2, 0, 2),), (1, 1, 0)),
    ((), (1, -1, 0)),
    (((-1, -1, 1), (-1, 1, 1), (2, 1, 0)), (1, 0, 1)),
    (((2, 0, 3),), (0, -1, 1)),
    (((1, -1, 2), (1, 1, 2)), (0, 1, 1)),
    (((-1, 0, 3),), (-1, -1, 0)),
    ((), (-1, 1, 0)),
    (((1, 2, 1), (-1, 1, 2), (1, -1, 3)), (2, 0, 1)),
    (((2, 0, 1),), (-1, 0, 1)),
    (((-1, -1, 2),), (1, 2, 0)),
    (((0, 2, 3), (1, 1, 3), (2, 2, 0)), (1, -1, 1)),
    ((), (2, 0, 0)),
    (((2, -1, 2),), (0, 2, 1)),
    (((2, 1, 2), (2, -1, 3), (-1, -1, 3)), (1, 1, 1)),
    (((-1, 2, 1), (1, 2, 2)), (2, -1, 1)),
    ((), (-1, -1, 1)),
    (((1, 2, 3), (2, -1, 1), (-1, 1, 3)), (-1, 2, 0)),
    (((-1, 2, 2),), (1, 2, 1)),
    (((2, 1, 3),), (2, -1, 0)),
    (((-1, 2, 3), (2, 1, 1)), (-1, 1, 1)),
    (((2, 2, 1),), (2, 1, 1)),
    (((2, 2, 2),), (-1, 2, 1)),
    (((2, 2, 3),), (2, 1, 0)),
    ((), (2, 2, 0)),
    ((), (2, 2, 1)),
)
W_FIRST, W_LAST = 11, 22
PLUS_Y, MINUS_Y, PLUS_Z, MINUS_Z = range(4)
STEPS = ((0, 1), (0, -1), (1, 0), (-1, 0))
ALONG_Y_FIRST = (0, 3)
ONWARD_BY_PLUS = (0, 1)


def nt(a, b, precision=None):
    return lax.dot_general(
        a, b, (((1,), (1,)), ((), ())), preferred_element_type=F32, precision=precision
    )


def mm(a, b, precision=None):
    return jnp.dot(a, b, preferred_element_type=F32, precision=precision)


def head_norm(values, axis):
    return values * lax.rsqrt(jnp.mean(values * values, axis=axis, keepdims=True) + HEAD_EPS)


def routes(dz, dy, quarter):
    y_first = quarter in ALONG_Y_FIRST
    ways = ((PLUS_Y, MINUS_Y), (PLUS_Z, MINUS_Z))
    first, second = ways if y_first else ways[::-1]
    a, b = (dy, dz) if y_first else (dz, dy)
    by_plus = quarter in ONWARD_BY_PLUS
    if a == 0 and b == 0:
        return first + second
    line, at = (first, a) if b == 0 else (second, b)
    onward = ()
    if at == -1 and by_plus:
        onward = (line[0],)
    elif at == 1 and not by_plus:
        onward = (line[1],)
    return onward + (second if b == 0 else ())


def kernel(
    tokens, gain, wq1, wq2, wk1, wk2, wv, mix, hgain, wrq, wrk, wrv, logs, init, wod, wor,
    out,
    rows, weights, qt, qrecv, kv, states, retp, wout, qpad, acc, peak, denom, sbuf, pbuf, rgate,
    dsend, rsend, heads,
    load_sem, x_send, x_recv, w_send, w_recv, kv_send, kv_recv, pair_send, pair_recv,
    st_send, st_recv, st_pair_send, q_sem, o_send, o_recv, r_send, r_recv,
):
    sp = lax.axis_index("sp")
    t = lax.axis_index("tp")
    z, y, c = lax.div(sp, 8), lax.rem(lax.div(sp, 2), 4), lax.rem(sp, 2)
    partner = 31 - sp
    sib = (sp + 1 - 2 * c, t)
    left, right, far = lax.rem(t + 3, 4), lax.rem(t + 1, 4), lax.rem(t + 2, 4)

    def chip(dz, dy):
        return lax.rem(z + dz + 4, 4) * 4 + lax.rem(y + dy + 4, 4)

    near = [(chip(dz, dy) * 2 + c, t) for dz, dy in STEPS]

    loads = []
    sources = (
        (wk1, 256, 128), (wk2, 384, 128), (wv, 512, 256), (wq1, 0, 128), (wq2, 128, 128),
        (wrq, 768, 128), (wrk, 896, 128), (wrv, 1024, 256),
    )
    for k, (ref, at, width) in enumerate(sources):
        loads.append(pltpu.make_async_copy(ref, weights.at[:, pl.ds(at, width)], load_sem.at[k]))
    for k, ref in enumerate((wod, wor)):
        loads.append(pltpu.make_async_copy(ref, wout.at[t, k], load_sem.at[8 + k]))
    for load in loads:
        load.start()

    barrier = pltpu.get_barrier_semaphore()
    peers = [(sp, left), (sp, right), (sp, far), sib, *near] + [(partner, d) for d in range(4)]
    for peer in peers:
        pl.semaphore_signal(barrier, inc=1, device_id=peer, device_id_type=MESH)

    for chunk in range(2):
        floats = tokens[chunk * 64 : chunk * 64 + 64].astype(F32)
        scale = lax.rsqrt(jnp.mean(floats * floats, axis=-1, keepdims=True) + NORM_EPS)
        rows[t, chunk * 64 : chunk * 64 + 64] = (floats * scale * gain[...]).astype(BF16)
    lg = logs[...]

    pl.semaphore_wait(barrier, len(peers))

    def remote(src, dst, ssem, rsem, dev):
        return pltpu.make_async_remote_copy(
            src_ref=src, dst_ref=dst, send_sem=ssem, recv_sem=rsem, device_id=dev,
            device_id_type=MESH,
        )

    def x_copy(slot, chunk, to, n):
        piece = rows.at[slot, pl.ds(chunk * 64, 64)]
        return remote(piece, piece, x_send.at[n], x_recv.at[slot, chunk], (sp, to))

    def w_copy(slot, part, to, n):
        piece = wout.at[slot, c] if part is None else wout.at[slot, c, pl.ds(part * 128, 128)]
        rsem = w_recv.at[slot, 0 if part is None else part]
        return remote(piece, piece, w_send.at[n], rsem, (sp, to))

    def w_sib(slot, n, kind):
        piece = wout.at[slot, kind]
        return remote(piece, piece, w_send.at[4 + n], w_recv.at[slot, 2], sib)

    def kv_copy(j, q, way, n, dev):
        return remote(kv.at[j, q], kv.at[j, q], kv_send.at[way, n], kv_recv.at[j, q], dev)

    def st_copy(j, way, n, dev):
        return remote(states.at[j], states.at[j], st_send.at[way, n], st_recv.at[j], dev)

    def pair_copy(j, pair, n):
        piece = kv.at[j, pl.ds(2 * pair, 2)]
        return remote(piece, piece, pair_send.at[n], pair_recv.at[j, pair], sib)

    def st_pair_copy(j, n):
        return remote(states.at[j], states.at[j], st_pair_send.at[n], st_recv.at[j], sib)

    kv_used, st_used, pairs_used, st_pairs_used = [0] * 4, [0] * 4, [], []

    def pass_on(dz, dy, q):
        j = chip(dz, dy) * 2 + c
        for way in routes(dz, dy, q):
            kv_copy(j, q, way, kv_used[way], near[way]).start()
            kv_used[way] += 1

    def pass_state_on(dz, dy):
        j = chip(dz, dy) * 2 + c
        for way in routes(dz, dy, 3):
            st_copy(j, way, st_used[way], near[way]).start()
            st_used[way] += 1
        st_pair_copy(j, len(st_pairs_used)).start()
        st_pairs_used.append((dz, dy))

    arrived = set()

    def pair_to_sib(dz, dy, q):
        arrived.add((dz, dy, q))
        if (dz, dy, q ^ 1) in arrived:
            pair_copy(chip(dz, dy) * 2 + c, q // 2, len(pairs_used)).start()
            pairs_used.append((dz, dy, q // 2))

    def arrival(dz, dy, q):
        j = chip(dz, dy) * 2 + c
        kv_copy(j, q, 0, 0, sib).wait_recv()
        pass_on(dz, dy, q)
        if q == 3:
            st_copy(j, 0, 0, sib).wait_recv()
            pass_state_on(dz, dy)
        pair_to_sib(dz, dy, q)

    x_copy(t, 0, right, 0).start()
    x_copy(t, 1, left, 1).start()
    x_copy(t, 1, right, 2).start()
    x_copy(t, 0, left, 3).start()

    def times(lhs, n):
        return mm(lhs, weights[:, n * 256 : n * 256 + 256])

    spots = (
        ((0, t * 128, 128),),
        ((0, left * 128, 64), (64, right * 128 + 64, 64)),
        ((0, left * 128 + 64, 64), (64, right * 128, 64)),
        ((0, far * 128, 128),),
    )

    def own_quarter(q):
        if q == 0:
            for load in loads[:3]:
                load.wait()
            lhs = rows[t]
        elif q == 1:
            x_copy(left, 0, right, 0).wait_recv()
            x_copy(left, 0, right, 4).start()
            x_copy(right, 1, left, 0).wait_recv()
            x_copy(right, 1, left, 5).start()
            lhs = jnp.concatenate([rows[left, 0:64], rows[right, 64:128]], axis=0)
        elif q == 2:
            x_copy(left, 1, right, 0).wait_recv()
            x_copy(right, 0, left, 0).wait_recv()
            lhs = jnp.concatenate([rows[left, 64:128], rows[right, 0:64]], axis=0)
        else:
            x_copy(far, 0, right, 0).wait_recv()
            x_copy(far, 1, left, 0).wait_recv()
            lhs = rows[far]
        kv[sp, q, 0:128] = times(lhs, 1).astype(BF16)
        turned = times(lhs, 2).T.astype(BF16)
        kv[sp, q, 128:256] = jnp.concatenate([turned[0:128], turned[128:256]], axis=1)
        pass_on(0, 0, q)
        pair_to_sib(0, 0, q)
        if q == 0:
            for load in loads[3:8]:
                load.wait()
        at = q % 2 * 128
        qt[q // 2, :, at : at + 128] = times(lhs, 0).T.astype(BF16)
        for n in range(2):
            block = times(lhs, 3 + n).astype(BF16)
            for here, there, count in spots[q]:
                retp[n, pl.ds(pl.multiple_of(there, 64), count)] = block[here : here + count]
        if q == 1:
            q_copy.start()
            for load in loads[8:]:
                load.wait()
            w_copy(t, None, right, 0).start()
            w_copy(t, None, left, 1).start()

    q_copy = remote(qt.at[0], qrecv, q_sem.at[0], q_sem.at[1], (partner, t))
    row = lax.broadcasted_iota(jnp.int32, (256, 256), 0)
    col = lax.broadcasted_iota(jnp.int32, (256, 256), 1)
    lane = lax.broadcasted_iota(jnp.int32, (256, 128), 1)

    for event in SCHEDULE[0][0]:
        if event[:2] == (0, 0):
            own_quarter(event[2])
        else:
            arrival(*event)
        if event == (0, 0, 3):
            adds, fades, queries = retention_inside(lg, retp, rgate, states, sp, row, col, lane)
            pass_state_on(0, 0)

    def queries_of(half, block):
        big = block.astype(F32) * 0.125
        for hm in range(4):
            qpad[half, hm] = jnp.where(lax.div(row, 64) == hm, big, 0.0).astype(BF16)

    queries_of(0, qt[1])
    for half in range(2):
        for hm in range(4):
            peak[half, hm] = jnp.full((1, 256), LOWEST, F32)
            denom[half, hm] = jnp.zeros((1, 256), F32)
            acc[half, hm] = jnp.zeros((128, 256), F32)
    q_copy.wait_recv()
    queries_of(1, qrecv[...])

    def position(index, pair):
        early = jnp.where(
            index < 128, t * 128 + index,
            jnp.where(index < 192, left * 128 + index - 128, right * 128 + index - 128),
        )
        late = jnp.where(
            index < 64, left * 128 + 64 + index,
            jnp.where(index < 128, right * 128 + index - 64, far * 128 + index - 128),
        )
        return jnp.where(pair == 0, early, late)

    def attend(half, near_chip, pair, bound, masked):
        def keys(l):
            return jnp.concatenate([kv[near_chip * 2 + l, 2 * pair + p, 0:128] for p in range(2)], axis=0)

        def values(l, h):
            cut = slice(h * 128, h * 128 + 128)
            return jnp.concatenate(
                [kv[near_chip * 2 + l, 2 * pair + p, 128:256, cut] for p in range(2)], axis=1
            )

        if masked:
            late = position(col, 1 - half) - position(row, pair) + (bound - near_chip * 2) * 512
        for hm in range(4):
            for l in range(2):
                scores = mm(keys(l), qpad[half, hm])
                if masked:
                    scores = jnp.where(late >= l * 512, scores, -jnp.inf)
                sbuf[hm, l] = scores
        for hm in range(4):
            old = peak[half, hm]
            new = jnp.maximum(
                old, jnp.max(jnp.maximum(sbuf[hm, 0], sbuf[hm, 1]), axis=0, keepdims=True)
            )
            fade = jnp.exp(old - new)
            total = denom[half, hm] * fade
            for l in range(2):
                term = jnp.exp(sbuf[hm, l] - new)
                total = total + jnp.sum(term, axis=0, keepdims=True)
                pbuf[hm, l] = term.astype(BF16)
            denom[half, hm] = total
            peak[half, hm] = new
            acc[half, hm] = acc[half, hm] * fade + sum(
                mm(values(l, hm % 2), pbuf[hm, l]) for l in range(2)
            )

    def w_stage(stage):
        if stage == 1:
            w_copy(left, None, right, 0).wait_recv()
            w_copy(left, 0, right, 2).start()
            w_copy(right, None, left, 0).wait_recv()
            w_copy(right, 1, left, 3).start()
            w_sib(left, 0, c).start()
            w_sib(right, 1, c).start()
        else:
            w_copy(far, 0, right, 0).wait_recv()
            w_copy(far, 1, left, 0).wait_recv()
            w_sib(far, 2, c).start()

    def pick(values, s):
        chosen = jnp.int32(values[0])
        for k, value in enumerate(values[1:], 1):
            chosen = jnp.where(s == k, jnp.int32(value), chosen)
        return chosen

    codes = [(dz + 1) * 8 + (dy + 1) * 2 + pair for _, (dz, dy, pair) in SCHEDULE]

    def tick(s, carry):
        for k, (events, _) in enumerate(SCHEDULE):
            if k == 0 or not (events or k in (W_FIRST, W_LAST)):
                continue

            @pl.when(s == k)
            def _():
                for event in events:
                    arrival(*event)
                if k == W_FIRST:
                    w_stage(1)
                if k == W_LAST:
                    w_stage(2)

        code = pick(codes, s)
        near_chip = chip(lax.div(code, 8) - 1, lax.rem(lax.div(code, 2), 4) - 1)
        pair = lax.rem(code, 2)
        other = near_chip * 2 + 1 - c
        pair_copy(other, pair, 0).wait_recv()

        def one_half(half, carry):
            bound = jnp.where(half == 0, sp, partner)
            bound_chip = lax.div(bound, 2)

            @pl.when(near_chip < bound_chip)
            def _():
                attend(half, near_chip, pair, bound, False)

            @pl.when(near_chip == bound_chip)
            def _():
                attend(half, near_chip, pair, bound, True)

            return carry

        return lax.fori_loop(0, 2, one_half, carry)

    lax.fori_loop(0, len(SCHEDULE), tick, 0)
    assert kv_used == [15] * 4 and len(pairs_used) == 32 and len(st_pairs_used) == 16

    def o_copy(src, at, count, dev, n, sem):
        place = heads.at[0, t, pl.ds(at, count)]
        return remote(src, place, o_send.at[n], o_recv.at[t, sem], dev)

    def finish(half):
        sides = []
        for h in range(2):
            weight_two = mix[pl.ds(h, 1), :]
            first = acc[half, h] / denom[half, h]
            second = acc[half, 2 + h] / denom[half, 2 + h]
            attn = first - weight_two * second
            sides.append((head_norm(attn, 0) * DIFF_SCALE).T * hgain[...])
        dsend[half] = jnp.concatenate(sides, axis=1).astype(BF16)

    def o_copies(half):
        if half == 0:
            return [
                o_copy(dsend.at[0, pl.ds(0, 64)], 64, 64, (sp, left), 0, 1),
                o_copy(dsend.at[0, pl.ds(64, 64)], 0, 64, (sp, right), 1, 0),
                o_copy(dsend.at[0, pl.ds(128, 128)], 0, 128, (sp, far), 2, 0),
            ]
        return [
            o_copy(dsend.at[1, pl.ds(0, 128)], 0, 128, (partner, t), 3, 0),
            o_copy(dsend.at[1, pl.ds(128, 64)], 0, 64, (partner, left), 4, 0),
            o_copy(dsend.at[1, pl.ds(192, 64)], 64, 64, (partner, right), 5, 1),
        ]

    for half in range(2):
        finish(half)
        for copy in o_copies(half):
            copy.start()

    def chain(j, state):
        own = states[j].astype(F32)
        return state * jnp.exp(own[64:65] + own[65:66] + own[66:67]) + own[0:64]

    for dz, dy in st_pairs_used:
        st_copy(chip(dz, dy) * 2 + 1 - c, 0, 0, sib).wait_recv()
    state = lax.fori_loop(0, sp, chain, jnp.concatenate([init[0], init[1]], axis=1))
    state = jnp.concatenate([state[:, 0:128], state[:, 128:256]], axis=0)
    for b in range(2):
        for h in range(2):
            mine = (lane < 64) if h == 0 else (lane >= 64)
            older = mm(jnp.where(mine, queries[b], 0.0), state, HIGHEST)
            r = rgate[b, h] + older
            rsend[b * 256 : b * 256 + 256, h * 128 : h * 128 + 128] = head_norm(r, 1).astype(BF16)
        state = fades[b] * state + adds[b]

    def r_copy(slot, n):
        piece = rsend.at[pl.ds(pl.multiple_of(slot * 128, 128), 128)]
        return remote(piece, heads.at[1, t], r_send.at[n], r_recv.at[t], (sp, slot))

    others = (left, right, far)
    for n, slot in enumerate(others):
        r_copy(slot, n).start()
    heads[1, t] = rsend[pl.ds(pl.multiple_of(t * 128, 128), 128)]

    for slot in others:
        piece = wout.at[slot, 1 - c]
        remote(piece, piece, w_send.at[0], w_recv.at[slot, 2], sib).wait_recv()

    def o_wait(slot, at, count, sem):
        piece = heads.at[0, slot, pl.ds(at, count)]
        remote(piece, piece, o_send.at[0], o_recv.at[slot, sem], sib).wait_recv()

    o_wait(far, 0, 128, 0)
    o_wait(t, 0, 128, 0)
    for slot in (left, right):
        o_wait(slot, 0, 64, 0)
        o_wait(slot, 64, 64, 1)
    for slot in others:
        piece = heads.at[1, slot]
        remote(piece, piece, r_send.at[0], r_recv.at[slot], sib).wait_recv()

    def columns(n, carry):
        at = pl.ds(pl.multiple_of(n * 512, 512), 512)
        block = jnp.zeros((128, 512), F32)
        for slot in range(4):
            for kind in range(2):
                block += mm(heads[kind, slot], wout[slot, kind, :, at])
        out[:, at] = block.astype(BF16)
        return carry

    lax.fori_loop(0, 4, columns, 0)

    for n in range(6):
        x_copy(t, 0, right, n).wait_send()
    for n in range(2):
        w_copy(t, None, right, n).wait_send()
        w_copy(t, n, right, 2 + n).wait_send()
    for n in range(3):
        w_sib(t, n, c).wait_send()
        r_copy(t, n).wait_send()
    q_copy.wait_send()
    for way in range(4):
        for n in range(kv_used[way]):
            kv_copy(0, 0, way, n, sib).wait_send()
        for n in range(st_used[way]):
            st_copy(0, way, n, sib).wait_send()
    for n in range(len(pairs_used)):
        pair_copy(0, 0, n).wait_send()
    for n in range(len(st_pairs_used)):
        st_pair_copy(0, n).wait_send()
    for half in range(2):
        for copy in o_copies(half):
            copy.wait_send()


def retention_inside(lg, retp, rgate, states, sp, row, col, lane):
    state_row = lax.broadcasted_iota(jnp.int32, (128, 128), 0)
    upper = jnp.where(row <= col, 1.0, 0.0)
    adds, fades, queries, lasts_of = [], [], [], []
    for b in range(2):
        span = slice(b * 256, b * 256 + 256)
        lb = lg[:, span]
        cum_rows = mm(jnp.concatenate([lb, lb, lb, lb], axis=0), upper, HIGHEST)
        rq, rk = retp[0, span, 0:128], retp[0, span, 128:256]
        cols, lasts = [], []
        for h in range(2):
            cum_col = jnp.sum(jnp.where(col <= row, lb[h : h + 1], 0.0), axis=1, keepdims=True)
            cols.append(cum_col)
            lasts.append(jnp.sum(lb[h : h + 1], axis=1, keepdims=True))
            mine = (lane < 64) if h == 0 else (lane >= 64)
            raw = nt(jnp.where(mine, rq, jnp.zeros_like(rq)), rk)
            gap = jnp.where(col <= row, cum_col - cum_rows[h : h + 1], -jnp.inf)
            gate = (raw * 0.125 * jnp.exp(gap)).astype(BF16)
            rgate[b, h] = mm(gate, retp[1, span, h * 128 : h * 128 + 128])
        factor = jnp.where(lane < 64, jnp.exp(lasts[0] - cols[0]), jnp.exp(lasts[1] - cols[1]))
        keys = (rk.astype(F32) * 0.125 * factor).T.astype(BF16)
        both = mm(keys, retp[1, span])
        adds.append(jnp.where(state_row < 64, both[:, 0:128], both[:, 128:256]))
        fades.append(jnp.where(state_row < 64, jnp.exp(lasts[0]), jnp.exp(lasts[1])))
        grow = jnp.where(lane < 64, jnp.exp(cols[0]), jnp.exp(cols[1]))
        queries.append(rq.astype(F32) * grow)
        lasts_of.append(lasts)
    own = fades[1] * adds[0] + adds[1]
    states[sp, 0:64] = jnp.concatenate([own[0:64], own[64:128]], axis=1).astype(BF16)
    tile_lane = lax.broadcasted_iota(jnp.int32, (16, 256), 1)
    tile_row = lax.broadcasted_iota(jnp.int32, (16, 256), 0)
    total = jnp.where(
        tile_lane < 128, lasts_of[0][0] + lasts_of[1][0], lasts_of[0][1] + lasts_of[1][1]
    )
    high = total.astype(BF16).astype(F32)
    middle = (total - high).astype(BF16).astype(F32)
    low = total - high - middle
    tile = jnp.where(tile_row == 0, high, jnp.where(tile_row == 1, middle, low))
    states[sp, 64:80] = tile.astype(BF16)
    return adds, fades, queries


def on_device(
    tokens, norm_gain, w_query_one, w_query_two, w_key_one, w_key_two, w_value, mix_lambda,
    head_gain, w_ret_query, w_ret_key, w_ret_value, retain_log, init_state, w_out_diff, w_out_ret,
):
    vmem = pl.BlockSpec(memory_space=pltpu.VMEM)
    hbm = pl.BlockSpec(memory_space=pl.ANY)
    dma = pltpu.SemaphoreType.DMA
    return pl.pallas_call(
        kernel,
        out_shape=jax.ShapeDtypeStruct((128, 2048), BF16),
        in_specs=[vmem, vmem] + [hbm] * 5 + [vmem, vmem] + [hbm] * 3 + [vmem, vmem] + [hbm] * 2,
        out_specs=vmem,
        scratch_shapes=[
            pltpu.VMEM((4, 128, 2048), BF16),
            pltpu.VMEM((2048, 1280), BF16),
            pltpu.VMEM((2, 256, 256), BF16),
            pltpu.VMEM((256, 256), BF16),
            pltpu.VMEM((32, 4, 256, 256), BF16),
            pltpu.VMEM((32, 80, 256), BF16),
            pltpu.VMEM((2, 512, 256), BF16),
            pltpu.VMEM((4, 2, 256, 2048), BF16),
            pltpu.VMEM((2, 4, 256, 256), BF16),
            pltpu.VMEM((2, 4, 128, 256), F32),
            pltpu.VMEM((2, 4, 1, 256), F32),
            pltpu.VMEM((2, 4, 1, 256), F32),
            pltpu.VMEM((4, 2, 256, 256), F32),
            pltpu.VMEM((4, 2, 256, 256), BF16),
            pltpu.VMEM((2, 2, 256, 128), F32),
            pltpu.VMEM((2, 256, 256), BF16),
            pltpu.VMEM((512, 256), BF16),
            pltpu.VMEM((2, 4, 128, 256), BF16),
            dma((10,)),
            dma((6,)),
            dma((4, 2)),
            dma((7,)),
            dma((4, 3)),
            dma((4, 15)),
            dma((32, 4)),
            dma((32,)),
            dma((32, 2)),
            dma((4, 10)),
            dma((32,)),
            dma((16,)),
            dma((2,)),
            dma((6,)),
            dma((4, 2)),
            dma((3,)),
            dma((4,)),
        ],
        compiler_params=pltpu.CompilerParams(
            collective_id=0, has_side_effects=True, vmem_limit_bytes=60 * 1024 * 1024,
        ),
        cost_estimate=pl.CostEstimate(
            flops=20_000_000_000, bytes_accessed=10_000_000, transcendentals=17_000_000
        ),
        name="layer",
    )(
        tokens, norm_gain.reshape(1, -1), w_query_one, w_query_two, w_key_one, w_key_two, w_value,
        jnp.broadcast_to(mix_lambda[:, None], (2, 256)), head_gain.reshape(1, -1),
        w_ret_query, w_ret_key, w_ret_value, retain_log, init_state, w_out_diff, w_out_ret,
    )


def solution(mesh):
    both = ("sp", "tp")
    return jax.shard_map(
        on_device,
        mesh=mesh,
        in_specs=(
            P(both, None), P(), P(None, "tp"), P(None, "tp"), P(None, "tp"), P(None, "tp"),
            P(None, "tp"), P("tp"), P(), P(None, "tp"), P(None, "tp"), P(None, "tp"),
            P("tp", "sp"), P("tp", None, None), P("tp", None), P("tp", None),
        ),
        out_specs=P(both, None),
        check_vma=False,
    )
```

```python
import jax
import jax.numpy as jnp
from jax import lax
from jax.experimental import pallas as pl
from jax.experimental.pallas import tpu as pltpu
from jax.sharding import PartitionSpec as P

NORM_EPS = 1e-06
HEAD_EPS = 1e-05
DIFF_SCALE = 0.8
MESH = pl.DeviceIdType.MESH
F32 = jnp.float32
BF16 = jnp.bfloat16
HIGHEST = lax.Precision.HIGHEST
LOWEST = -3.0e38


SCHEDULE = (
    (((0, 0, 0), (-1, 0, 0), (0, -1, 0), (0, 1, 0), (1, 0, 0), (0, 0, 1), (2, 0, 0), (0, 2, 0), (1, -1, 0), (0, 0, 2), (0, 1, 1), (-1, -1, 0), (0, -1, 1), (1, 1, 0), (0, 0, 3), (-1, 1, 0), (1, 0, 1), (0, -1, 2), (0, 1, 2)), (0, 0, 0)),
    (((-1, 0, 1), (1, 2, 0), (0, 2, 1)), (0, 1, 0)),
    ((), (0, -1, 0)),
    (((-1, 2, 0), (1, 0, 2)), (0, 0, 1)),
    (((0, 1, 3), (0, -1, 3)), (1, 0, 0)),
    ((), (-1, 0, 0)),
    (((-1, 0, 2), (1, 0, 3), (1, 1, 1)), (0, 2, 0)),
    (((1, -1, 1),), (0, 1, 1)),
    (((2, -1, 0),), (0, -1, 1)),
    (((2, 0, 2), (0, 2, 2), (-1, -1, 1)), (1, 0, 1)),
    ((), (1, 1, 0)),
    (((-1, 0, 3), (-1, 1, 1)), (1, -1, 0)),
    (((1, -1, 2), (1, 1, 3)), (-1, -1, 0)),
    ((), (-1, 0, 1)),
    (((2, 1, 0), (1, 1, 2), (-1, -1, 2)), (-1, 1, 0)),
    (((1, -1, 3), (2, 0, 1)), (1, 1, 1)),
    (((1, 2, 1), (0, 2, 3)), (1, -1, 1)),
    (((2, 0, 3),), (2, 0, 0)),
    (((2, 2, 0), (2, -1, 2), (-1, 1, 2)), (1, 2, 0)),
    ((), (0, 2, 1)),
    ((), (2, 0, 1)),
    (((-1, 2, 1), (2, 1, 3), (-1, 1, 3), (2, 1, 2), (2, -1, 1)), (-1, 2, 0)),
    (((1, 2, 2), (2, -1, 3), (-1, -1, 3)), (-1, 1, 1)),
    ((), (2, 1, 1)),
    (((2, 1, 1),), (2, -1, 0)),
    (((1, 2, 3), (-1, 2, 3)), (2, -1, 1)),
    (((2, 2, 1), (-1, 2, 2)), (-1, -1, 1)),
    ((), (2, 1, 0)),
    ((), (1, 2, 1)),
    (((2, 2, 2),), (2, 2, 0)),
    ((), (-1, 2, 1)),
    (((2, 2, 3),), (2, 2, 1)),
)
W_FIRST, W_LAST, RETENTION = 11, 22, 31
PLUS_Y, MINUS_Y, PLUS_Z, MINUS_Z = range(4)
STEPS = ((0, 1), (0, -1), (1, 0), (-1, 0))
ALONG_Y_FIRST = (0, 3)
ONWARD_BY_PLUS = (0, 1)


def nt(a, b, precision=None):
    return lax.dot_general(
        a, b, (((1,), (1,)), ((), ())), preferred_element_type=F32, precision=precision
    )


def mm(a, b, precision=None):
    return jnp.dot(a, b, preferred_element_type=F32, precision=precision)


def head_norm(values, axis):
    return values * lax.rsqrt(jnp.mean(values * values, axis=axis, keepdims=True) + HEAD_EPS)


def routes(dz, dy, quarter):
    y_first = quarter in ALONG_Y_FIRST
    ways = ((PLUS_Y, MINUS_Y), (PLUS_Z, MINUS_Z))
    first, second = ways if y_first else ways[::-1]
    a, b = (dy, dz) if y_first else (dz, dy)
    by_plus = quarter in ONWARD_BY_PLUS
    if a == 0 and b == 0:
        return first + second
    line, at = (first, a) if b == 0 else (second, b)
    onward = ()
    if at == -1 and by_plus:
        onward = (line[0],)
    elif at == 1 and not by_plus:
        onward = (line[1],)
    return onward + (second if b == 0 else ())


def kernel(
    tokens, gain, wq1, wq2, wk1, wk2, wv, mix, hgain, wrq, wrk, wrv, logs, init, wod, wor,
    out,
    rows, weights, qt, qrecv, kv, states, retp, wout, qpad, acc, peak, denom, sbuf, pbuf, rgate, retq, retadd, retfade, osum,
    dsend, rsend, heads,
    load_sem, x_send, x_recv, w_send, w_recv, kv_send, kv_recv, pair_send, pair_recv,
    st_send, st_recv, st_pair_send, q_sem, o_send, o_recv, r_send, r_recv,
):
    sp = lax.axis_index("sp")
    t = lax.axis_index("tp")
    z, y, c = lax.div(sp, 8), lax.rem(lax.div(sp, 2), 4), lax.rem(sp, 2)
    partner = 31 - sp
    sib = (sp + 1 - 2 * c, t)
    left, right, far = lax.rem(t + 3, 4), lax.rem(t + 1, 4), lax.rem(t + 2, 4)

    def chip(dz, dy):
        return lax.rem(z + dz + 4, 4) * 4 + lax.rem(y + dy + 4, 4)

    near = [(chip(dz, dy) * 2 + c, t) for dz, dy in STEPS]

    loads = []
    sources = (
        (wk1, 256, 128), (wk2, 384, 128), (wv, 512, 256), (wq1, 0, 128), (wq2, 128, 128),
        (wrq, 768, 128), (wrk, 896, 128), (wrv, 1024, 256),
    )
    for k, (ref, at, width) in enumerate(sources):
        loads.append(pltpu.make_async_copy(ref, weights.at[:, pl.ds(at, width)], load_sem.at[k]))
    for k, ref in enumerate((wod, wor)):
        loads.append(pltpu.make_async_copy(ref, wout.at[t, k], load_sem.at[8 + k]))
    for load in loads:
        load.start()

    barrier = pltpu.get_barrier_semaphore()
    peers = [(sp, left), (sp, right), (sp, far), sib, *near] + [(partner, d) for d in range(4)]
    for peer in peers:
        pl.semaphore_signal(barrier, inc=1, device_id=peer, device_id_type=MESH)

    for chunk in range(2):
        floats = tokens[chunk * 64 : chunk * 64 + 64].astype(F32)
        scale = lax.rsqrt(jnp.mean(floats * floats, axis=-1, keepdims=True) + NORM_EPS)
        rows[t, chunk * 64 : chunk * 64 + 64] = (floats * scale * gain[...]).astype(BF16)
    lg = logs[...]

    pl.semaphore_wait(barrier, len(peers))

    def remote(src, dst, ssem, rsem, dev):
        return pltpu.make_async_remote_copy(
            src_ref=src, dst_ref=dst, send_sem=ssem, recv_sem=rsem, device_id=dev,
            device_id_type=MESH,
        )

    def x_copy(slot, chunk, to, n):
        piece = rows.at[slot, pl.ds(chunk * 64, 64)]
        return remote(piece, piece, x_send.at[n], x_recv.at[slot, chunk], (sp, to))

    def w_copy(slot, part, to, n):
        piece = wout.at[slot, c] if part is None else wout.at[slot, c, pl.ds(part * 128, 128)]
        rsem = w_recv.at[slot, 0 if part is None else part]
        return remote(piece, piece, w_send.at[n], rsem, (sp, to))

    def w_sib(slot, n, kind):
        piece = wout.at[slot, kind]
        return remote(piece, piece, w_send.at[4 + n], w_recv.at[slot, 2], sib)

    def kv_copy(j, q, way, n, dev):
        return remote(kv.at[j, q], kv.at[j, q], kv_send.at[way, n], kv_recv.at[j, q], dev)

    def st_copy(j, way, n, dev):
        return remote(states.at[j], states.at[j], st_send.at[way, n], st_recv.at[j], dev)

    def pair_copy(j, pair, n):
        piece = kv.at[j, pl.ds(2 * pair, 2)]
        return remote(piece, piece, pair_send.at[n], pair_recv.at[j, pair], sib)

    def st_pair_copy(j, n):
        return remote(states.at[j], states.at[j], st_pair_send.at[n], st_recv.at[j], sib)

    kv_used, st_used, pairs_used, st_pairs_used = [0] * 4, [0] * 4, [], []

    def pass_on(dz, dy, q):
        j = chip(dz, dy) * 2 + c
        for way in routes(dz, dy, q):
            kv_copy(j, q, way, kv_used[way], near[way]).start()
            kv_used[way] += 1

    def pass_state_on(dz, dy):
        j = chip(dz, dy) * 2 + c
        for way in routes(dz, dy, 3):
            st_copy(j, way, st_used[way], near[way]).start()
            st_used[way] += 1
        st_pair_copy(j, len(st_pairs_used)).start()
        st_pairs_used.append((dz, dy))

    arrived = set()

    def pair_to_sib(dz, dy, q):
        arrived.add((dz, dy, q))
        if (dz, dy, q ^ 1) in arrived:
            pair_copy(chip(dz, dy) * 2 + c, q // 2, len(pairs_used)).start()
            pairs_used.append((dz, dy, q // 2))

    def arrival(dz, dy, q):
        j = chip(dz, dy) * 2 + c
        kv_copy(j, q, 0, 0, sib).wait_recv()
        pass_on(dz, dy, q)
        if q == 3:
            st_copy(j, 0, 0, sib).wait_recv()
            pass_state_on(dz, dy)
        pair_to_sib(dz, dy, q)

    x_copy(t, 0, right, 0).start()
    x_copy(t, 1, left, 1).start()
    x_copy(t, 1, right, 2).start()
    x_copy(t, 0, left, 3).start()

    def times(lhs, n):
        return mm(lhs, weights[:, n * 256 : n * 256 + 256])

    spots = (
        ((0, t * 128, 128),),
        ((0, left * 128, 64), (64, right * 128 + 64, 64)),
        ((0, left * 128 + 64, 64), (64, right * 128, 64)),
        ((0, far * 128, 128),),
    )

    def own_quarter(q):
        if q == 0:
            for load in loads[:3]:
                load.wait()
            lhs = rows[t]
        elif q == 1:
            x_copy(left, 0, right, 0).wait_recv()
            x_copy(left, 0, right, 4).start()
            x_copy(right, 1, left, 0).wait_recv()
            x_copy(right, 1, left, 5).start()
            lhs = jnp.concatenate([rows[left, 0:64], rows[right, 64:128]], axis=0)
        elif q == 2:
            x_copy(left, 1, right, 0).wait_recv()
            x_copy(right, 0, left, 0).wait_recv()
            lhs = jnp.concatenate([rows[left, 64:128], rows[right, 0:64]], axis=0)
        else:
            x_copy(far, 0, right, 0).wait_recv()
            x_copy(far, 1, left, 0).wait_recv()
            lhs = rows[far]
        kv[sp, q, 0:128] = times(lhs, 1).astype(BF16)
        turned = times(lhs, 2).T.astype(BF16)
        kv[sp, q, 128:256] = jnp.concatenate([turned[0:128], turned[128:256]], axis=1)
        pass_on(0, 0, q)
        pair_to_sib(0, 0, q)
        if q == 0:
            for load in loads[3:8]:
                load.wait()
        at = q % 2 * 128
        qt[q // 2, :, at : at + 128] = times(lhs, 0).T.astype(BF16)
        for n in range(2):
            block = times(lhs, 3 + n).astype(BF16)
            for here, there, count in spots[q]:
                retp[n, pl.ds(pl.multiple_of(there, 64), count)] = block[here : here + count]
        if q == 1:
            q_copy.start()
            for load in loads[8:]:
                load.wait()
            w_copy(t, None, right, 0).start()
            w_copy(t, None, left, 1).start()

    q_copy = remote(qt.at[0], qrecv, q_sem.at[0], q_sem.at[1], (partner, t))
    row = lax.broadcasted_iota(jnp.int32, (256, 256), 0)
    col = lax.broadcasted_iota(jnp.int32, (256, 256), 1)
    lane = lax.broadcasted_iota(jnp.int32, (256, 128), 1)

    for event in SCHEDULE[0][0]:
        if event[:2] == (0, 0):
            own_quarter(event[2])
        else:
            arrival(*event)
        if event == (0, 0, 3):
            retention_inside(lg, retp, rgate, retq, retadd, retfade, states, sp, row, col, lane)
            pass_state_on(0, 0)

    def queries_of(half, block):
        big = block.astype(F32) * 0.125
        for hm in range(4):
            qpad[half, hm] = jnp.where(lax.div(row, 64) == hm, big, 0.0).astype(BF16)

    queries_of(0, qt[1])
    for half in range(2):
        for hm in range(4):
            peak[half, hm] = jnp.full((1, 256), LOWEST, F32)
            denom[half, hm] = jnp.zeros((1, 256), F32)
            acc[half, hm] = jnp.zeros((128, 256), F32)
    q_copy.wait_recv()
    queries_of(1, qrecv[...])

    def position(index, pair):
        early = jnp.where(
            index < 128, t * 128 + index,
            jnp.where(index < 192, left * 128 + index - 128, right * 128 + index - 128),
        )
        late = jnp.where(
            index < 64, left * 128 + 64 + index,
            jnp.where(index < 128, right * 128 + index - 64, far * 128 + index - 128),
        )
        return jnp.where(pair == 0, early, late)

    def attend(half, near_chip, pair, bound, masked):
        def keys(l):
            return jnp.concatenate([kv[near_chip * 2 + l, 2 * pair + p, 0:128] for p in range(2)], axis=0)

        def values(l, h):
            cut = slice(h * 128, h * 128 + 128)
            return jnp.concatenate(
                [kv[near_chip * 2 + l, 2 * pair + p, 128:256, cut] for p in range(2)], axis=1
            )

        if masked:
            late = position(col, 1 - half) - position(row, pair) + (bound - near_chip * 2) * 512
        for hm in range(4):
            for l in range(2):
                scores = mm(keys(l), qpad[half, hm])
                if masked:
                    scores = jnp.where(late >= l * 512, scores, -jnp.inf)
                sbuf[hm, l] = scores
        for hm in range(4):
            old = peak[half, hm]
            new = jnp.maximum(
                old, jnp.max(jnp.maximum(sbuf[hm, 0], sbuf[hm, 1]), axis=0, keepdims=True)
            )
            fade = jnp.exp(old - new)
            total = denom[half, hm] * fade
            for l in range(2):
                term = jnp.exp(sbuf[hm, l] - new)
                total = total + jnp.sum(term, axis=0, keepdims=True)
                pbuf[hm, l] = term.astype(BF16)
            denom[half, hm] = total
            peak[half, hm] = new
            acc[half, hm] = acc[half, hm] * fade + sum(
                mm(values(l, hm % 2), pbuf[hm, l]) for l in range(2)
            )

    def w_stage(stage):
        if stage == 1:
            w_copy(left, None, right, 0).wait_recv()
            w_copy(left, 0, right, 2).start()
            w_copy(right, None, left, 0).wait_recv()
            w_copy(right, 1, left, 3).start()
            w_sib(left, 0, c).start()
            w_sib(right, 1, c).start()
        else:
            w_copy(far, 0, right, 0).wait_recv()
            w_copy(far, 1, left, 0).wait_recv()
            w_sib(far, 2, c).start()

    others = (left, right, far)

    def r_copy(slot, n):
        piece = rsend.at[pl.ds(pl.multiple_of(slot * 128, 128), 128)]
        return remote(piece, heads.at[1, t], r_send.at[n], r_recv.at[t], (sp, slot))

    def chain(j, state):
        own = states[j].astype(F32)
        return state * jnp.exp(own[64:65] + own[65:66] + own[66:67]) + own[0:64]

    def retention_end():
        for dz in (0, 1, 2, -1):
            for dy in (0, 1, 2, -1):
                st_copy(chip(dz, dy) * 2 + 1 - c, 0, 0, sib).wait_recv()
        state = lax.fori_loop(0, sp, chain, jnp.concatenate([init[0], init[1]], axis=1))
        state = jnp.concatenate([state[:, 0:128], state[:, 128:256]], axis=0)
        for b in range(2):
            for h in range(2):
                mine = (lane < 64) if h == 0 else (lane >= 64)
                older = mm(jnp.where(mine, retq[b], 0.0), state, HIGHEST)
                r = rgate[b, h] + older
                rsend[b * 256 : b * 256 + 256, h * 128 : h * 128 + 128] = head_norm(r, 1).astype(BF16)
            state = retfade[b] * state + retadd[b]
        for n, slot in enumerate(others):
            r_copy(slot, n).start()
        heads[1, t] = rsend[pl.ds(pl.multiple_of(t * 128, 128), 128)]

    codes = [(dz + 1) * 8 + (dy + 1) * 2 + pair for _, (dz, dy, pair) in SCHEDULE]

    def handled(s, low, high):
        if high - low > 1:
            middle = (low + high) // 2
            return lax.cond(
                s < middle, lambda: handled(s, low, middle), lambda: handled(s, middle, high)
            )
        if low > 0:
            for event in SCHEDULE[low][0]:
                arrival(*event)
        if low == W_FIRST:
            w_stage(1)
        if low == W_LAST:
            w_stage(2)
        if low == RETENTION:
            retention_end()
        return jnp.int32(codes[low])

    def tick(s, carry):
        code = handled(s, 0, len(SCHEDULE))
        near_chip = chip(lax.div(code, 8) - 1, lax.rem(lax.div(code, 2), 4) - 1)
        pair = lax.rem(code, 2)
        other = near_chip * 2 + 1 - c
        pair_copy(other, pair, 0).wait_recv()

        def one_half(half, carry):
            bound = jnp.where(half == 0, sp, partner)
            bound_chip = lax.div(bound, 2)

            @pl.when(near_chip < bound_chip)
            def _():
                attend(half, near_chip, pair, bound, False)

            @pl.when(near_chip == bound_chip)
            def _():
                attend(half, near_chip, pair, bound, True)

            return carry

        return lax.fori_loop(0, 2, one_half, carry)

    lax.fori_loop(0, len(SCHEDULE), tick, 0)
    assert kv_used == [15] * 4 and len(pairs_used) == 32 and len(st_pairs_used) == 16

    def o_copy(src, at, count, dev, n, sem):
        place = heads.at[0, t, pl.ds(at, count)]
        return remote(src, place, o_send.at[n], o_recv.at[t, sem], dev)

    def finish(half):
        sides = []
        for h in range(2):
            weight_two = mix[:, h : h + 1]
            first = acc[half, h] / denom[half, h]
            second = acc[half, 2 + h] / denom[half, 2 + h]
            attn = first - weight_two * second
            sides.append((head_norm(attn, 0) * DIFF_SCALE).T * hgain[...])
        dsend[half] = jnp.concatenate(sides, axis=1).astype(BF16)

    def o_copies(half):
        if half == 0:
            return [
                o_copy(dsend.at[0, pl.ds(0, 64)], 64, 64, (sp, left), 0, 1),
                o_copy(dsend.at[0, pl.ds(64, 64)], 0, 64, (sp, right), 1, 0),
                o_copy(dsend.at[0, pl.ds(128, 128)], 0, 128, (sp, far), 2, 0),
            ]
        return [
            o_copy(dsend.at[1, pl.ds(0, 128)], 0, 128, (partner, t), 3, 0),
            o_copy(dsend.at[1, pl.ds(128, 64)], 0, 64, (partner, left), 4, 0),
            o_copy(dsend.at[1, pl.ds(192, 64)], 64, 64, (partner, right), 5, 1),
        ]

    for half in range(2):
        finish(half)
        for copy in o_copies(half):
            copy.start()

    def product(kind, last):
        def columns(n, carry):
            at = pl.ds(pl.multiple_of(n * 512, 512), 512)
            block = osum[:, at] if last else jnp.zeros((128, 512), F32)
            for slot in range(4):
                block += mm(heads[kind, slot], wout[slot, kind, :, at])
            if last:
                out[:, at] = block.astype(BF16)
            else:
                osum[:, at] = block
            return carry

        lax.fori_loop(0, 4, columns, 0)

    for slot in others:
        piece = wout.at[slot, 1 - c]
        remote(piece, piece, w_send.at[0], w_recv.at[slot, 2], sib).wait_recv()
    for slot in others:
        piece = heads.at[1, slot]
        remote(piece, piece, r_send.at[0], r_recv.at[slot], sib).wait_recv()
    product(1, False)

    def o_wait(slot, at, count, sem):
        piece = heads.at[0, slot, pl.ds(at, count)]
        remote(piece, piece, o_send.at[0], o_recv.at[slot, sem], sib).wait_recv()

    o_wait(far, 0, 128, 0)
    o_wait(t, 0, 128, 0)
    for slot in (left, right):
        o_wait(slot, 0, 64, 0)
        o_wait(slot, 64, 64, 1)
    product(0, True)

    for n in range(6):
        x_copy(t, 0, right, n).wait_send()
    for n in range(2):
        w_copy(t, None, right, n).wait_send()
        w_copy(t, n, right, 2 + n).wait_send()
    for n in range(3):
        w_sib(t, n, c).wait_send()
        r_copy(t, n).wait_send()
    q_copy.wait_send()
    for way in range(4):
        for n in range(kv_used[way]):
            kv_copy(0, 0, way, n, sib).wait_send()
        for n in range(st_used[way]):
            st_copy(0, way, n, sib).wait_send()
    for n in range(len(pairs_used)):
        pair_copy(0, 0, n).wait_send()
    for n in range(len(st_pairs_used)):
        st_pair_copy(0, n).wait_send()
    for half in range(2):
        for copy in o_copies(half):
            copy.wait_send()


def retention_inside(lg, retp, rgate, retq, retadd, retfade, states, sp, row, col, lane):
    state_row = lax.broadcasted_iota(jnp.int32, (128, 128), 0)
    upper = jnp.where(row <= col, 1.0, 0.0)
    adds, fades, lasts_of = [], [], []
    for b in range(2):
        span = slice(b * 256, b * 256 + 256)
        lb = lg[:, span]
        cum_rows = mm(jnp.concatenate([lb, lb, lb, lb], axis=0), upper, HIGHEST)
        rq, rk = retp[0, span, 0:128], retp[0, span, 128:256]
        cols, lasts = [], []
        for h in range(2):
            cum_col = jnp.sum(jnp.where(col <= row, lb[h : h + 1], 0.0), axis=1, keepdims=True)
            cols.append(cum_col)
            lasts.append(jnp.sum(lb[h : h + 1], axis=1, keepdims=True))
            mine = (lane < 64) if h == 0 else (lane >= 64)
            raw = nt(jnp.where(mine, rq, jnp.zeros_like(rq)), rk)
            gap = jnp.where(col <= row, cum_col - cum_rows[h : h + 1], -jnp.inf)
            gate = (raw * 0.125 * jnp.exp(gap)).astype(BF16)
            rgate[b, h] = mm(gate, retp[1, span, h * 128 : h * 128 + 128])
        factor = jnp.where(lane < 64, jnp.exp(lasts[0] - cols[0]), jnp.exp(lasts[1] - cols[1]))
        keys = (rk.astype(F32) * 0.125 * factor).T.astype(BF16)
        both = mm(keys, retp[1, span])
        adds.append(jnp.where(state_row < 64, both[:, 0:128], both[:, 128:256]))
        fades.append(jnp.where(state_row < 64, jnp.exp(lasts[0]), jnp.exp(lasts[1])))
        grow = jnp.where(lane < 64, jnp.exp(cols[0]), jnp.exp(cols[1]))
        retq[b] = rq.astype(F32) * grow
        retadd[b] = adds[b]
        retfade[b] = fades[b]
        lasts_of.append(lasts)
    own = fades[1] * adds[0] + adds[1]
    states[sp, 0:64] = jnp.concatenate([own[0:64], own[64:128]], axis=1).astype(BF16)
    tile_lane = lax.broadcasted_iota(jnp.int32, (16, 256), 1)
    tile_row = lax.broadcasted_iota(jnp.int32, (16, 256), 0)
    total = jnp.where(
        tile_lane < 128, lasts_of[0][0] + lasts_of[1][0], lasts_of[0][1] + lasts_of[1][1]
    )
    high = total.astype(BF16).astype(F32)
    middle = (total - high).astype(BF16).astype(F32)
    low = total - high - middle
    tile = jnp.where(tile_row == 0, high, jnp.where(tile_row == 1, middle, low))
    states[sp, 64:80] = tile.astype(BF16)


def on_device(
    tokens, norm_gain, w_query_one, w_query_two, w_key_one, w_key_two, w_value, mix_lambda,
    head_gain, w_ret_query, w_ret_key, w_ret_value, retain_log, init_state, w_out_diff, w_out_ret,
):
    vmem = pl.BlockSpec(memory_space=pltpu.VMEM)
    hbm = pl.BlockSpec(memory_space=pl.ANY)
    dma = pltpu.SemaphoreType.DMA
    return pl.pallas_call(
        kernel,
        out_shape=jax.ShapeDtypeStruct((128, 2048), BF16),
        in_specs=[vmem, vmem] + [hbm] * 5 + [vmem, vmem] + [hbm] * 3 + [vmem, vmem] + [hbm] * 2,
        out_specs=vmem,
        scratch_shapes=[
            pltpu.VMEM((4, 128, 2048), BF16),
            pltpu.VMEM((2048, 1280), BF16),
            pltpu.VMEM((2, 256, 256), BF16),
            pltpu.VMEM((256, 256), BF16),
            pltpu.VMEM((32, 4, 256, 256), BF16),
            pltpu.VMEM((32, 80, 256), BF16),
            pltpu.VMEM((2, 512, 256), BF16),
            pltpu.VMEM((4, 2, 256, 2048), BF16),
            pltpu.VMEM((2, 4, 256, 256), BF16),
            pltpu.VMEM((2, 4, 128, 256), F32),
            pltpu.VMEM((2, 4, 1, 256), F32),
            pltpu.VMEM((2, 4, 1, 256), F32),
            pltpu.VMEM((4, 2, 256, 256), F32),
            pltpu.VMEM((4, 2, 256, 256), BF16),
            pltpu.VMEM((2, 2, 256, 128), F32),
            pltpu.VMEM((2, 256, 128), F32),
            pltpu.VMEM((2, 128, 128), F32),
            pltpu.VMEM((2, 128, 128), F32),
            pltpu.VMEM((128, 2048), F32),
            pltpu.VMEM((2, 256, 256), BF16),
            pltpu.VMEM((512, 256), BF16),
            pltpu.VMEM((2, 4, 128, 256), BF16),
            dma((10,)),
            dma((6,)),
            dma((4, 2)),
            dma((7,)),
            dma((4, 3)),
            dma((4, 15)),
            dma((32, 4)),
            dma((32,)),
            dma((32, 2)),
            dma((4, 10)),
            dma((32,)),
            dma((16,)),
            dma((2,)),
            dma((6,)),
            dma((4, 2)),
            dma((3,)),
            dma((4,)),
        ],
        compiler_params=pltpu.CompilerParams(
            collective_id=0, has_side_effects=True, vmem_limit_bytes=60 * 1024 * 1024,
        ),
        cost_estimate=pl.CostEstimate(
            flops=20_000_000_000, bytes_accessed=10_000_000, transcendentals=17_000_000
        ),
        name="layer",
    )(
        tokens, norm_gain.reshape(1, -1), w_query_one, w_query_two, w_key_one, w_key_two, w_value,
        mix_lambda.reshape(1, -1), head_gain.reshape(1, -1),
        w_ret_query, w_ret_key, w_ret_value, retain_log, init_state, w_out_diff, w_out_ret,
    )


def solution(mesh):
    both = ("sp", "tp")
    return jax.shard_map(
        on_device,
        mesh=mesh,
        in_specs=(
            P(both, None), P(), P(None, "tp"), P(None, "tp"), P(None, "tp"), P(None, "tp"),
            P(None, "tp"), P("tp"), P(), P(None, "tp"), P(None, "tp"), P(None, "tp"),
            P("tp", "sp"), P("tp", None, None), P("tp", None), P("tp", None),
        ),
        out_specs=P(both, None),
        check_vma=False,
    )
```

```python
import jax
import jax.numpy as jnp
from jax import lax
from jax.experimental import pallas as pl
from jax.experimental.pallas import tpu as pltpu
from jax.sharding import PartitionSpec as P

NORM_EPS = 1e-06
HEAD_EPS = 1e-05
DIFF_SCALE = 0.8
MESH = pl.DeviceIdType.MESH
F32 = jnp.float32
BF16 = jnp.bfloat16
HIGHEST = lax.Precision.HIGHEST
LOWEST = -3.0e38


W_NEAR, W_FAR, RETENTION = range(3)
SCHEDULE = (
    (((0, 0, 0), (0, 1, 0), (-1, 0, 0), (0, 0, 1), (0, -1, 0), (0, 0, 2), (1, 0, 1), (2, 0, 0), (1, 1, 0), (1, -1, 0), (-1, 1, 0), (0, -1, 1), (-1, 0, 1), (0, 2, 0), (1, 0, 0), (0, 0, 3), (0, 0, 4)), (0, 0, 0)),
    (((1, 0, 2), (0, -1, 2)), (0, 0, 1)),
    ((), (-1, 0, 0)),
    (((0, 1, 1), (-1, -1, 0)), (1, 0, 0)),
    (((1, -1, 1), (1, 0, 3)), (0, -1, 0)),
    (((0, 2, 1),), (0, 1, 0)),
    (((0, 1, 2), (0, 1, 3), (-1, 1, 1)), (1, 0, 1)),
    (((2, 0, 1), (1, 1, 1)), (0, 2, 0)),
    ((), (0, 1, 1)),
    (((0, -1, 3),), (-1, 1, 0)),
    (((0, -1, 4),), (1, -1, 0)),
    (((-1, 0, 2),), (1, 1, 0)),
    (((0, 1, 4), (1, -1, 2), (1, 1, 3), (-1, 0, 3)), (2, 0, 0)),
    (((1, 1, 2), (-1, -1, 1)), (0, -1, 1)),
    (((1, 2, 1), (0, 2, 3), (2, 0, 2)), (-1, 0, 1)),
    (((1, 2, 0),), (-1, -1, 0)),
    (((2, 0, 3), (2, 1, 1), (1, -1, 4), (0, 2, 2)), (1, 1, 1)),
    (((1, -1, 3), (2, 1, 0)), (1, 2, 0)),
    (((2, -1, 1), W_NEAR), (0, 2, 1)),
    (((-1, 1, 2), (-1, 1, 3), (-1, -1, 3)), (2, 1, 0)),
    (((0, 2, 4), (2, 1, 3), (-1, -1, 2), (-1, 2, 0)), (1, -1, 1)),
    (((2, -1, 0), (1, 2, 3)), (-1, 1, 1)),
    (((-1, -1, 4), (1, 0, 4), (-1, 2, 1)), (2, 0, 1)),
    (((-1, 2, 3), (2, 1, 2), (-1, 0, 4), (1, 2, 2)), (-1, -1, 1)),
    (((-1, 2, 4),), (2, -1, 0)),
    (((2, -1, 3), (2, -1, 2), (1, 2, 4), (1, 1, 4), (-1, 1, 4)), (-1, 2, 0)),
    (((2, 2, 3), (2, 2, 0), (-1, 2, 2), (2, 2, 1)), (2, 1, 1)),
    (((2, -1, 4),), (2, -1, 1)),
    ((), (2, 2, 0)),
    (((2, 2, 2), W_FAR, (2, 0, 4), (2, 2, 4), (2, 1, 4)), (1, 2, 1)),
    ((), (-1, 2, 1)),
    ((RETENTION,), (2, 2, 1)),
)
LAST = ()
PLUS_Y, MINUS_Y, PLUS_Z, MINUS_Z = range(4)
STEPS = ((0, 1), (0, -1), (1, 0), (-1, 0))
ALONG_Y_FIRST = (0, 3, 4)
ONWARD_BY_PLUS = (0, 1, 4)


def nt(a, b, precision=None):
    return lax.dot_general(
        a, b, (((1,), (1,)), ((), ())), preferred_element_type=F32, precision=precision
    )


def mm(a, b, precision=None):
    return jnp.dot(a, b, preferred_element_type=F32, precision=precision)


def head_norm(values, axis):
    return values * lax.rsqrt(jnp.mean(values * values, axis=axis, keepdims=True) + HEAD_EPS)


def routes(dz, dy, quarter):
    y_first = quarter in ALONG_Y_FIRST
    ways = ((PLUS_Y, MINUS_Y), (PLUS_Z, MINUS_Z))
    first, second = ways if y_first else ways[::-1]
    a, b = (dy, dz) if y_first else (dz, dy)
    by_plus = quarter in ONWARD_BY_PLUS
    if a == 0 and b == 0:
        return first + second
    line, at = (first, a) if b == 0 else (second, b)
    onward = ()
    if at == -1 and by_plus:
        onward = (line[0],)
    elif at == 1 and not by_plus:
        onward = (line[1],)
    return onward + (second if b == 0 else ())


def kernel(
    tokens, gain, wq1, wq2, wk1, wk2, wv, mix, hgain, wrq, wrk, wrv, logs, init, wod, wor,
    out,
    rows, weights, qt, qrecv, kv, states, retp, wout, qpad, acc, peak, denom, sbuf, pbuf, rgate, retq, retadd, retfade, osum,
    dsend, rsend, heads,
    load_sem, x_send, x_recv, w_send, w_recv, kv_send, kv_recv, pair_send, pair_recv,
    st_send, st_recv, st_pair_send, q_sem, o_send, o_recv, r_send, r_recv,
):
    sp = lax.axis_index("sp")
    t = lax.axis_index("tp")
    z, y, c = lax.div(sp, 8), lax.rem(lax.div(sp, 2), 4), lax.rem(sp, 2)
    partner = 31 - sp
    sib = (sp + 1 - 2 * c, t)
    left, right, far = lax.rem(t + 3, 4), lax.rem(t + 1, 4), lax.rem(t + 2, 4)

    def chip(dz, dy):
        return lax.rem(z + dz + 4, 4) * 4 + lax.rem(y + dy + 4, 4)

    near = [(chip(dz, dy) * 2 + c, t) for dz, dy in STEPS]

    loads = []
    sources = (
        (wk1, 256, 128), (wk2, 384, 128), (wv, 512, 256), (wq1, 0, 128), (wq2, 128, 128),
        (wrq, 768, 128), (wrk, 896, 128), (wrv, 1024, 256),
    )
    for k, (ref, at, width) in enumerate(sources):
        loads.append(pltpu.make_async_copy(ref, weights.at[:, pl.ds(at, width)], load_sem.at[k]))
    for k, ref in enumerate((wod, wor)):
        loads.append(pltpu.make_async_copy(ref, wout.at[t, k], load_sem.at[8 + k]))
    for load in loads:
        load.start()

    barrier = pltpu.get_barrier_semaphore()
    peers = [(sp, left), (sp, right), (sp, far), sib, *near] + [(partner, d) for d in range(4)]
    for peer in peers:
        pl.semaphore_signal(barrier, inc=1, device_id=peer, device_id_type=MESH)

    for chunk in range(2):
        floats = tokens[chunk * 64 : chunk * 64 + 64].astype(F32)
        scale = lax.rsqrt(jnp.mean(floats * floats, axis=-1, keepdims=True) + NORM_EPS)
        rows[t, chunk * 64 : chunk * 64 + 64] = (floats * scale * gain[...]).astype(BF16)
    lg = logs[...]

    pl.semaphore_wait(barrier, len(peers))

    def remote(src, dst, ssem, rsem, dev):
        return pltpu.make_async_remote_copy(
            src_ref=src, dst_ref=dst, send_sem=ssem, recv_sem=rsem, device_id=dev,
            device_id_type=MESH,
        )

    def x_copy(slot, chunk, to, n):
        piece = rows.at[slot, pl.ds(chunk * 64, 64)]
        return remote(piece, piece, x_send.at[n], x_recv.at[slot, chunk], (sp, to))

    def w_copy(slot, part, to, n):
        piece = wout.at[slot, c] if part is None else wout.at[slot, c, pl.ds(part * 128, 128)]
        rsem = w_recv.at[slot, 0 if part is None else part]
        return remote(piece, piece, w_send.at[n], rsem, (sp, to))

    def w_sib(slot, n, kind):
        piece = wout.at[slot, kind]
        return remote(piece, piece, w_send.at[4 + n], w_recv.at[slot, 2], sib)

    def kv_copy(j, q, way, n, dev):
        return remote(kv.at[j, q], kv.at[j, q], kv_send.at[way, n], kv_recv.at[j, q], dev)

    def st_copy(j, way, n, dev):
        return remote(states.at[j], states.at[j], st_send.at[way, n], st_recv.at[j], dev)

    def pair_copy(j, pair, n):
        piece = kv.at[j, pl.ds(2 * pair, 2)]
        return remote(piece, piece, pair_send.at[n], pair_recv.at[j, pair], sib)

    def st_pair_copy(j, n):
        return remote(states.at[j], states.at[j], st_pair_send.at[n], st_recv.at[j], sib)

    kv_used, st_used, pairs_used, st_pairs_used = [0] * 4, [0] * 4, [], []

    def pass_on(dz, dy, q):
        j = chip(dz, dy) * 2 + c
        for way in routes(dz, dy, q):
            kv_copy(j, q, way, kv_used[way], near[way]).start()
            kv_used[way] += 1

    def pass_state_on(dz, dy):
        j = chip(dz, dy) * 2 + c
        for way in routes(dz, dy, 4):
            st_copy(j, way, st_used[way], near[way]).start()
            st_used[way] += 1
        st_pair_copy(j, len(st_pairs_used)).start()
        st_pairs_used.append((dz, dy))

    arrived = set()

    def pair_to_sib(dz, dy, q):
        arrived.add((dz, dy, q))
        if (dz, dy, q ^ 1) in arrived:
            pair_copy(chip(dz, dy) * 2 + c, q // 2, len(pairs_used)).start()
            pairs_used.append((dz, dy, q // 2))

    def arrival(dz, dy, q):
        j = chip(dz, dy) * 2 + c
        if q == 4:
            st_copy(j, 0, 0, sib).wait_recv()
            pass_state_on(dz, dy)
        else:
            kv_copy(j, q, 0, 0, sib).wait_recv()
            pass_on(dz, dy, q)
            pair_to_sib(dz, dy, q)

    x_copy(t, 0, right, 0).start()
    x_copy(t, 1, left, 1).start()
    x_copy(t, 1, right, 2).start()
    x_copy(t, 0, left, 3).start()

    def times(lhs, n):
        return mm(lhs, weights[:, n * 256 : n * 256 + 256])

    spots = (
        ((0, t * 128, 128),),
        ((0, left * 128, 64), (64, right * 128 + 64, 64)),
        ((0, left * 128 + 64, 64), (64, right * 128, 64)),
        ((0, far * 128, 128),),
    )

    def own_quarter(q):
        if q == 0:
            for load in loads[:3]:
                load.wait()
            lhs = rows[t]
        elif q == 1:
            x_copy(left, 0, right, 0).wait_recv()
            x_copy(left, 0, right, 4).start()
            x_copy(right, 1, left, 0).wait_recv()
            x_copy(right, 1, left, 5).start()
            lhs = jnp.concatenate([rows[left, 0:64], rows[right, 64:128]], axis=0)
        elif q == 2:
            x_copy(left, 1, right, 0).wait_recv()
            x_copy(right, 0, left, 0).wait_recv()
            lhs = jnp.concatenate([rows[left, 64:128], rows[right, 0:64]], axis=0)
        else:
            x_copy(far, 0, right, 0).wait_recv()
            x_copy(far, 1, left, 0).wait_recv()
            lhs = rows[far]
        kv[sp, q, 0:128] = times(lhs, 1).astype(BF16)
        turned = times(lhs, 2).T.astype(BF16)
        kv[sp, q, 128:256] = jnp.concatenate([turned[0:128], turned[128:256]], axis=1)
        pass_on(0, 0, q)
        pair_to_sib(0, 0, q)
        if q == 0:
            for load in loads[3:8]:
                load.wait()
        at = q % 2 * 128
        qt[q // 2, :, at : at + 128] = times(lhs, 0).T.astype(BF16)
        for n in range(2):
            block = times(lhs, 3 + n).astype(BF16)
            for here, there, count in spots[q]:
                retp[n, pl.ds(pl.multiple_of(there, 64), count)] = block[here : here + count]
        if q == 1:
            q_copy.start()
            for load in loads[8:]:
                load.wait()
            w_copy(t, None, right, 0).start()
            w_copy(t, None, left, 1).start()

    q_copy = remote(qt.at[0], qrecv, q_sem.at[0], q_sem.at[1], (partner, t))
    row = lax.broadcasted_iota(jnp.int32, (256, 256), 0)
    col = lax.broadcasted_iota(jnp.int32, (256, 256), 1)
    lane = lax.broadcasted_iota(jnp.int32, (256, 128), 1)

    for event in SCHEDULE[0][0]:
        if event == (0, 0, 4):
            retention_inside(lg, retp, rgate, retq, retadd, retfade, states, sp, row, col, lane)
            pass_state_on(0, 0)
        elif event[:2] == (0, 0):
            own_quarter(event[2])
        else:
            arrival(*event)

    def queries_of(half, block):
        big = block.astype(F32) * 0.125
        for hm in range(4):
            qpad[half, hm] = jnp.where(lax.div(row, 64) == hm, big, 0.0).astype(BF16)

    queries_of(0, qt[1])
    for half in range(2):
        for hm in range(4):
            peak[half, hm] = jnp.full((1, 256), LOWEST, F32)
            denom[half, hm] = jnp.zeros((1, 256), F32)
            acc[half, hm] = jnp.zeros((128, 256), F32)
    q_copy.wait_recv()
    queries_of(1, qrecv[...])

    def position(index, pair):
        early = jnp.where(
            index < 128, t * 128 + index,
            jnp.where(index < 192, left * 128 + index - 128, right * 128 + index - 128),
        )
        late = jnp.where(
            index < 64, left * 128 + 64 + index,
            jnp.where(index < 128, right * 128 + index - 64, far * 128 + index - 128),
        )
        return jnp.where(pair == 0, early, late)

    def attend(half, near_chip, pair, bound, masked):
        def keys(l):
            return jnp.concatenate([kv[near_chip * 2 + l, 2 * pair + p, 0:128] for p in range(2)], axis=0)

        def values(l, h):
            cut = slice(h * 128, h * 128 + 128)
            return jnp.concatenate(
                [kv[near_chip * 2 + l, 2 * pair + p, 128:256, cut] for p in range(2)], axis=1
            )

        if masked:
            late = position(col, 1 - half) - position(row, pair) + (bound - near_chip * 2) * 512
        for hm in range(4):
            for l in range(2):
                scores = mm(keys(l), qpad[half, hm])
                if masked:
                    scores = jnp.where(late >= l * 512, scores, -jnp.inf)
                sbuf[hm, l] = scores
        for hm in range(4):
            old = peak[half, hm]
            new = jnp.maximum(
                old, jnp.max(jnp.maximum(sbuf[hm, 0], sbuf[hm, 1]), axis=0, keepdims=True)
            )
            fade = jnp.exp(old - new)
            total = denom[half, hm] * fade
            for l in range(2):
                term = jnp.exp(sbuf[hm, l] - new)
                total = total + jnp.sum(term, axis=0, keepdims=True)
                pbuf[hm, l] = term.astype(BF16)
            denom[half, hm] = total
            peak[half, hm] = new
            acc[half, hm] = acc[half, hm] * fade + sum(
                mm(values(l, hm % 2), pbuf[hm, l]) for l in range(2)
            )

    def w_stage(stage):
        if stage == W_NEAR:
            w_copy(left, None, right, 0).wait_recv()
            w_copy(left, 0, right, 2).start()
            w_copy(right, None, left, 0).wait_recv()
            w_copy(right, 1, left, 3).start()
            w_sib(left, 0, c).start()
            w_sib(right, 1, c).start()
        else:
            w_copy(far, 0, right, 0).wait_recv()
            w_copy(far, 1, left, 0).wait_recv()
            w_sib(far, 2, c).start()

    others = (left, right, far)

    def r_copy(slot, n):
        piece = rsend.at[pl.ds(pl.multiple_of(slot * 128, 128), 128)]
        return remote(piece, heads.at[1, t], r_send.at[n], r_recv.at[t], (sp, slot))

    def chain(j, state):
        own = states[j].astype(F32)
        return state * jnp.exp(own[64:65] + own[65:66] + own[66:67]) + own[0:64]

    def retention_end():
        for dz in (0, 1, 2, -1):
            for dy in (0, 1, 2, -1):
                st_copy(chip(dz, dy) * 2 + 1 - c, 0, 0, sib).wait_recv()
        state = lax.fori_loop(0, sp, chain, jnp.concatenate([init[0], init[1]], axis=1))
        state = jnp.concatenate([state[:, 0:128], state[:, 128:256]], axis=0)
        for b in range(2):
            for h in range(2):
                mine = (lane < 64) if h == 0 else (lane >= 64)
                older = mm(jnp.where(mine, retq[b], 0.0), state, HIGHEST)
                r = rgate[b, h] + older
                rsend[b * 256 : b * 256 + 256, h * 128 : h * 128 + 128] = head_norm(r, 1).astype(BF16)
            state = retfade[b] * state + retadd[b]
        for n, slot in enumerate(others):
            r_copy(slot, n).start()
        heads[1, t] = rsend[pl.ds(pl.multiple_of(t * 128, 128), 128)]

    codes = [(dz + 1) * 8 + (dy + 1) * 2 + pair for _, (dz, dy, pair) in SCHEDULE]

    def happen(events):
        for event in events:
            if event == RETENTION:
                retention_end()
            elif event in (W_NEAR, W_FAR):
                w_stage(event)
            else:
                arrival(*event)

    def handled(s, low, high):
        if high - low > 1:
            middle = (low + high) // 2
            return lax.cond(
                s < middle, lambda: handled(s, low, middle), lambda: handled(s, middle, high)
            )
        if low > 0:
            happen(SCHEDULE[low][0])
        return jnp.int32(codes[low])

    def tick(s, carry):
        code = handled(s, 0, len(SCHEDULE))
        near_chip = chip(lax.div(code, 8) - 1, lax.rem(lax.div(code, 2), 4) - 1)
        pair = lax.rem(code, 2)
        other = near_chip * 2 + 1 - c
        pair_copy(other, pair, 0).wait_recv()

        def one_half(half, carry):
            bound = jnp.where(half == 0, sp, partner)
            bound_chip = lax.div(bound, 2)

            @pl.when(near_chip < bound_chip)
            def _():
                attend(half, near_chip, pair, bound, False)

            @pl.when(near_chip == bound_chip)
            def _():
                attend(half, near_chip, pair, bound, True)

            return carry

        return lax.fori_loop(0, 2, one_half, carry)

    lax.fori_loop(0, len(SCHEDULE), tick, 0)
    happen(LAST)
    assert kv_used == [15] * 4 and len(pairs_used) == 32 and len(st_pairs_used) == 16

    def o_copy(src, at, count, dev, n, sem):
        place = heads.at[0, t, pl.ds(at, count)]
        return remote(src, place, o_send.at[n], o_recv.at[t, sem], dev)

    def finish(half):
        sides = []
        for h in range(2):
            weight_two = mix[:, h : h + 1]
            first = acc[half, h] / denom[half, h]
            second = acc[half, 2 + h] / denom[half, 2 + h]
            attn = first - weight_two * second
            sides.append((head_norm(attn, 0) * DIFF_SCALE).T * hgain[...])
        dsend[half] = jnp.concatenate(sides, axis=1).astype(BF16)

    def o_copies(half):
        if half == 0:
            return [
                o_copy(dsend.at[0, pl.ds(0, 64)], 64, 64, (sp, left), 0, 1),
                o_copy(dsend.at[0, pl.ds(64, 64)], 0, 64, (sp, right), 1, 0),
                o_copy(dsend.at[0, pl.ds(128, 128)], 0, 128, (sp, far), 2, 0),
            ]
        return [
            o_copy(dsend.at[1, pl.ds(0, 128)], 0, 128, (partner, t), 3, 0),
            o_copy(dsend.at[1, pl.ds(128, 64)], 0, 64, (partner, left), 4, 0),
            o_copy(dsend.at[1, pl.ds(192, 64)], 64, 64, (partner, right), 5, 1),
        ]

    for half in range(2):
        finish(half)
        for copy in o_copies(half):
            copy.start()

    def product(kind, last):
        def columns(n, carry):
            at = pl.ds(pl.multiple_of(n * 512, 512), 512)
            block = osum[:, at] if last else jnp.zeros((128, 512), F32)
            for slot in range(4):
                block += mm(heads[kind, slot], wout[slot, kind, :, at])
            if last:
                out[:, at] = block.astype(BF16)
            else:
                osum[:, at] = block
            return carry

        lax.fori_loop(0, 4, columns, 0)

    for slot in others:
        piece = wout.at[slot, 1 - c]
        remote(piece, piece, w_send.at[0], w_recv.at[slot, 2], sib).wait_recv()
    for slot in others:
        piece = heads.at[1, slot]
        remote(piece, piece, r_send.at[0], r_recv.at[slot], sib).wait_recv()
    product(1, False)

    def o_wait(slot, at, count, sem):
        piece = heads.at[0, slot, pl.ds(at, count)]
        remote(piece, piece, o_send.at[0], o_recv.at[slot, sem], sib).wait_recv()

    o_wait(far, 0, 128, 0)
    o_wait(t, 0, 128, 0)
    for slot in (left, right):
        o_wait(slot, 0, 64, 0)
        o_wait(slot, 64, 64, 1)
    product(0, True)

    for n in range(6):
        x_copy(t, 0, right, n).wait_send()
    for n in range(2):
        w_copy(t, None, right, n).wait_send()
        w_copy(t, n, right, 2 + n).wait_send()
    for n in range(3):
        w_sib(t, n, c).wait_send()
        r_copy(t, n).wait_send()
    q_copy.wait_send()
    for way in range(4):
        for n in range(kv_used[way]):
            kv_copy(0, 0, way, n, sib).wait_send()
        for n in range(st_used[way]):
            st_copy(0, way, n, sib).wait_send()
    for n in range(len(pairs_used)):
        pair_copy(0, 0, n).wait_send()
    for n in range(len(st_pairs_used)):
        st_pair_copy(0, n).wait_send()
    for half in range(2):
        for copy in o_copies(half):
            copy.wait_send()


def retention_inside(lg, retp, rgate, retq, retadd, retfade, states, sp, row, col, lane):
    state_row = lax.broadcasted_iota(jnp.int32, (128, 128), 0)
    upper = jnp.where(row <= col, 1.0, 0.0)
    adds, fades, lasts_of = [], [], []
    for b in range(2):
        span = slice(b * 256, b * 256 + 256)
        lb = lg[:, span]
        cum_rows = mm(jnp.concatenate([lb, lb, lb, lb], axis=0), upper, HIGHEST)
        rq, rk = retp[0, span, 0:128], retp[0, span, 128:256]
        cols, lasts = [], []
        for h in range(2):
            cum_col = jnp.sum(jnp.where(col <= row, lb[h : h + 1], 0.0), axis=1, keepdims=True)
            cols.append(cum_col)
            lasts.append(jnp.sum(lb[h : h + 1], axis=1, keepdims=True))
            mine = (lane < 64) if h == 0 else (lane >= 64)
            raw = nt(jnp.where(mine, rq, jnp.zeros_like(rq)), rk)
            gap = jnp.where(col <= row, cum_col - cum_rows[h : h + 1], -jnp.inf)
            gate = (raw * 0.125 * jnp.exp(gap)).astype(BF16)
            rgate[b, h] = mm(gate, retp[1, span, h * 128 : h * 128 + 128])
        factor = jnp.where(lane < 64, jnp.exp(lasts[0] - cols[0]), jnp.exp(lasts[1] - cols[1]))
        keys = (rk.astype(F32) * 0.125 * factor).T.astype(BF16)
        both = mm(keys, retp[1, span])
        adds.append(jnp.where(state_row < 64, both[:, 0:128], both[:, 128:256]))
        fades.append(jnp.where(state_row < 64, jnp.exp(lasts[0]), jnp.exp(lasts[1])))
        grow = jnp.where(lane < 64, jnp.exp(cols[0]), jnp.exp(cols[1]))
        retq[b] = rq.astype(F32) * grow
        retadd[b] = adds[b]
        retfade[b] = fades[b]
        lasts_of.append(lasts)
    own = fades[1] * adds[0] + adds[1]
    states[sp, 0:64] = jnp.concatenate([own[0:64], own[64:128]], axis=1).astype(BF16)
    tile_lane = lax.broadcasted_iota(jnp.int32, (16, 256), 1)
    tile_row = lax.broadcasted_iota(jnp.int32, (16, 256), 0)
    total = jnp.where(
        tile_lane < 128, lasts_of[0][0] + lasts_of[1][0], lasts_of[0][1] + lasts_of[1][1]
    )
    high = total.astype(BF16).astype(F32)
    middle = (total - high).astype(BF16).astype(F32)
    low = total - high - middle
    tile = jnp.where(tile_row == 0, high, jnp.where(tile_row == 1, middle, low))
    states[sp, 64:80] = tile.astype(BF16)


def on_device(
    tokens, norm_gain, w_query_one, w_query_two, w_key_one, w_key_two, w_value, mix_lambda,
    head_gain, w_ret_query, w_ret_key, w_ret_value, retain_log, init_state, w_out_diff, w_out_ret,
):
    vmem = pl.BlockSpec(memory_space=pltpu.VMEM)
    hbm = pl.BlockSpec(memory_space=pl.ANY)
    dma = pltpu.SemaphoreType.DMA
    return pl.pallas_call(
        kernel,
        out_shape=jax.ShapeDtypeStruct((128, 2048), BF16),
        in_specs=[vmem, vmem] + [hbm] * 5 + [vmem, vmem] + [hbm] * 3 + [vmem, vmem] + [hbm] * 2,
        out_specs=vmem,
        scratch_shapes=[
            pltpu.VMEM((4, 128, 2048), BF16),
            pltpu.VMEM((2048, 1280), BF16),
            pltpu.VMEM((2, 256, 256), BF16),
            pltpu.VMEM((256, 256), BF16),
            pltpu.VMEM((32, 4, 256, 256), BF16),
            pltpu.VMEM((32, 80, 256), BF16),
            pltpu.VMEM((2, 512, 256), BF16),
            pltpu.VMEM((4, 2, 256, 2048), BF16),
            pltpu.VMEM((2, 4, 256, 256), BF16),
            pltpu.VMEM((2, 4, 128, 256), F32),
            pltpu.VMEM((2, 4, 1, 256), F32),
            pltpu.VMEM((2, 4, 1, 256), F32),
            pltpu.VMEM((4, 2, 256, 256), F32),
            pltpu.VMEM((4, 2, 256, 256), BF16),
            pltpu.VMEM((2, 2, 256, 128), F32),
            pltpu.VMEM((2, 256, 128), F32),
            pltpu.VMEM((2, 128, 128), F32),
            pltpu.VMEM((2, 128, 128), F32),
            pltpu.VMEM((128, 2048), F32),
            pltpu.VMEM((2, 256, 256), BF16),
            pltpu.VMEM((512, 256), BF16),
            pltpu.VMEM((2, 4, 128, 256), BF16),
            dma((10,)),
            dma((6,)),
            dma((4, 2)),
            dma((7,)),
            dma((4, 3)),
            dma((4, 15)),
            dma((32, 4)),
            dma((32,)),
            dma((32, 2)),
            dma((4, 10)),
            dma((32,)),
            dma((16,)),
            dma((2,)),
            dma((6,)),
            dma((4, 2)),
            dma((3,)),
            dma((4,)),
        ],
        compiler_params=pltpu.CompilerParams(
            collective_id=0, has_side_effects=True, vmem_limit_bytes=60 * 1024 * 1024,
        ),
        cost_estimate=pl.CostEstimate(
            flops=20_000_000_000, bytes_accessed=10_000_000, transcendentals=17_000_000
        ),
        name="layer",
    )(
        tokens, norm_gain.reshape(1, -1), w_query_one, w_query_two, w_key_one, w_key_two, w_value,
        mix_lambda.reshape(1, -1), head_gain.reshape(1, -1),
        w_ret_query, w_ret_key, w_ret_value, retain_log, init_state, w_out_diff, w_out_ret,
    )


def solution(mesh):
    both = ("sp", "tp")
    return jax.shard_map(
        on_device,
        mesh=mesh,
        in_specs=(
            P(both, None), P(), P(None, "tp"), P(None, "tp"), P(None, "tp"), P(None, "tp"),
            P(None, "tp"), P("tp"), P(), P(None, "tp"), P(None, "tp"), P(None, "tp"),
            P("tp", "sp"), P("tp", None, None), P("tp", None), P("tp", None),
        ),
        out_specs=P(both, None),
        check_vma=False,
    )
```

```python
import jax
import jax.numpy as jnp
from jax import lax
from jax.experimental import pallas as pl
from jax.experimental.pallas import tpu as pltpu
from jax.sharding import PartitionSpec as P

NORM_EPS = 1e-06
HEAD_EPS = 1e-05
DIFF_SCALE = 0.8
MESH = pl.DeviceIdType.MESH
F32 = jnp.float32
BF16 = jnp.bfloat16
HIGHEST = lax.Precision.HIGHEST
LOWEST = -3.0e38


W_NEAR, W_FAR, RETENTION = range(3)
SCHEDULE = (
    (((0, 0, 0), (-1, 0, 0), (0, 0, 1), (0, -1, 0), (0, 0, 2), (-1, 0, 1), (0, 1, 0), (0, 1, 1), (2, 0, 0), (1, 0, 0), (0, 0, 3), (0, 0, 4), (1, 0, 2), (0, -1, 2), (1, 0, 1)), (-1, 0, 0)),
    ((), (0, 0, 0)),
    (((-1, -1, 0),), (0, 1, 0)),
    (((2, 0, 1), (1, 0, 3), (-1, 1, 0), (-1, 1, 1), (0, 1, 4), (-1, 0, 2)), (0, 0, 1)),
    ((), (1, 0, 1)),
    (((0, 1, 2), (0, -1, 4), (-1, 0, 3), (0, -1, 3)), (-1, 1, 0)),
    (((1, -1, 0), (0, 1, 3)), (1, 0, 0)),
    ((), (0, -1, 1)),
    (((0, -1, 1), (1, 1, 0), (2, 0, 2), (-1, -1, 1), (1, -1, 1)), (-1, 0, 1)),
    ((), (2, 0, 0)),
    (((2, 0, 3), (2, -1, 1), (1, 1, 1), (0, 2, 0)), (0, 1, 1)),
    ((), (0, -1, 0)),
    (((1, -1, 4), (2, 1, 1), (1, -1, 2), (2, 1, 0)), (-1, -1, 0)),
    (((1, -1, 3), (-1, -1, 2), (2, -1, 0)), (1, -1, 0)),
    (((1, 1, 4), (0, 2, 4)), (1, 1, 0)),
    ((), (2, 1, 0)),
    (((0, 2, 2), (-1, 1, 2), (1, 1, 2), (-1, 1, 4)), (2, -1, 0)),
    (((-1, -1, 4), W_NEAR, (-1, 0, 4), (-1, -1, 3), (0, 2, 3)), (2, 0, 1)),
    (((1, 2, 0), (1, 1, 3), (-1, 1, 3)), (1, -1, 1)),
    (((1, 0, 4), (2, -1, 3), (2, -1, 2)), (-1, -1, 1)),
    (((2, 1, 2), (-1, 2, 4)), (-1, 1, 1)),
    (((2, 1, 4), (1, 2, 4), (-1, 2, 1)), (2, -1, 1)),
    (((1, 2, 1), (-1, 2, 0), (1, 2, 3), (-1, 2, 2)), (1, 1, 1)),
    (((0, 2, 1), (2, -1, 4)), (0, 2, 1)),
    (((2, 2, 1), (1, 2, 2), (2, 0, 4), (-1, 2, 3), (2, 2, 4)), (-1, 2, 0)),
    ((), (1, 2, 0)),
    (((2, 2, 2), (2, 1, 3), RETENTION, (2, 2, 0), (2, 2, 3)), (0, 2, 0)),
    ((W_FAR,), (-1, 2, 1)),
    ((), (1, 2, 1)),
    ((), (2, 1, 1)),
    ((), (2, 2, 0)),
    ((), (2, 2, 1)),
)
LAST = ()
PLUS_Y, MINUS_Y, PLUS_Z, MINUS_Z = range(4)
STEPS = ((0, 1), (0, -1), (1, 0), (-1, 0))
ALONG_Y_FIRST = (0, 3, 4)
ONWARD_BY_PLUS = (0, 1, 4)


def nt(a, b, precision=None):
    return lax.dot_general(
        a, b, (((1,), (1,)), ((), ())), preferred_element_type=F32, precision=precision
    )


def mm(a, b, precision=None):
    return jnp.dot(a, b, preferred_element_type=F32, precision=precision)


def head_norm(values, axis):
    return values * lax.rsqrt(jnp.mean(values * values, axis=axis, keepdims=True) + HEAD_EPS)


def routes(dz, dy, quarter):
    y_first = quarter in ALONG_Y_FIRST
    ways = ((PLUS_Y, MINUS_Y), (PLUS_Z, MINUS_Z))
    first, second = ways if y_first else ways[::-1]
    a, b = (dy, dz) if y_first else (dz, dy)
    by_plus = quarter in ONWARD_BY_PLUS
    if a == 0 and b == 0:
        return first + second
    line, at = (first, a) if b == 0 else (second, b)
    onward = ()
    if at == -1 and by_plus:
        onward = (line[0],)
    elif at == 1 and not by_plus:
        onward = (line[1],)
    return onward + (second if b == 0 else ())


def kernel(
    tokens, gain, wq1, wq2, wk1, wk2, wv, mix, hgain, wrq, wrk, wrv, logs, init, wod, wor,
    out,
    rows, weights, qt, qrecv, kv, states, retp, wout, qpad, acc, peak, denom, sbuf, pbuf, rgate, retq, retadd, retfade, osum,
    dsend, rsend, heads,
    load_sem, x_send, x_recv, w_send, w_recv, kv_send, kv_recv, pair_send, pair_recv,
    st_send, st_recv, st_pair_send, q_sem, o_send, o_recv, r_send, r_recv,
):
    sp = lax.axis_index("sp")
    t = lax.axis_index("tp")
    z, y, c = lax.div(sp, 8), lax.rem(lax.div(sp, 2), 4), lax.rem(sp, 2)
    partner = 31 - sp
    sib = (sp + 1 - 2 * c, t)
    left, right, far = lax.rem(t + 3, 4), lax.rem(t + 1, 4), lax.rem(t + 2, 4)

    def chip(dz, dy):
        return lax.rem(z + dz + 4, 4) * 4 + lax.rem(y + dy + 4, 4)

    near = [(chip(dz, dy) * 2 + c, t) for dz, dy in STEPS]

    loads = []
    sources = (
        (wk1, 256, 128), (wk2, 384, 128), (wv, 512, 256), (wq1, 0, 128), (wq2, 128, 128),
        (wrq, 768, 128), (wrk, 896, 128), (wrv, 1024, 256),
    )
    for k, (ref, at, width) in enumerate(sources):
        loads.append(pltpu.make_async_copy(ref, weights.at[:, pl.ds(at, width)], load_sem.at[k]))
    for k, ref in enumerate((wod, wor)):
        loads.append(pltpu.make_async_copy(ref, wout.at[t, k], load_sem.at[8 + k]))
    for load in loads:
        load.start()

    barrier = pltpu.get_barrier_semaphore()
    peers = [(sp, left), (sp, right), (sp, far), sib, *near] + [(partner, d) for d in range(4)]
    for peer in peers:
        pl.semaphore_signal(barrier, inc=1, device_id=peer, device_id_type=MESH)

    for chunk in range(2):
        floats = tokens[chunk * 64 : chunk * 64 + 64].astype(F32)
        scale = lax.rsqrt(jnp.mean(floats * floats, axis=-1, keepdims=True) + NORM_EPS)
        rows[t, chunk * 64 : chunk * 64 + 64] = (floats * scale * gain[...]).astype(BF16)
    lg = logs[...]

    pl.semaphore_wait(barrier, len(peers))

    def remote(src, dst, ssem, rsem, dev):
        return pltpu.make_async_remote_copy(
            src_ref=src, dst_ref=dst, send_sem=ssem, recv_sem=rsem, device_id=dev,
            device_id_type=MESH,
        )

    def x_copy(slot, chunk, to, n):
        piece = rows.at[slot, pl.ds(chunk * 64, 64)]
        return remote(piece, piece, x_send.at[n], x_recv.at[slot, chunk], (sp, to))

    def w_copy(slot, part, to, n):
        piece = wout.at[slot, c] if part is None else wout.at[slot, c, pl.ds(part * 128, 128)]
        rsem = w_recv.at[slot, 0 if part is None else part]
        return remote(piece, piece, w_send.at[n], rsem, (sp, to))

    def w_sib(slot, n, kind):
        piece = wout.at[slot, kind]
        return remote(piece, piece, w_send.at[4 + n], w_recv.at[slot, 2], sib)

    def kv_copy(j, q, way, n, dev):
        return remote(kv.at[j, q], kv.at[j, q], kv_send.at[way, n], kv_recv.at[j, q], dev)

    def st_copy(j, way, n, dev):
        return remote(states.at[j], states.at[j], st_send.at[way, n], st_recv.at[j], dev)

    def pair_copy(j, pair, n):
        piece = kv.at[j, pl.ds(2 * pair, 2)]
        return remote(piece, piece, pair_send.at[n], pair_recv.at[j, pair], sib)

    def st_pair_copy(j, n):
        return remote(states.at[j], states.at[j], st_pair_send.at[n], st_recv.at[j], sib)

    kv_used, st_used, pairs_used, st_pairs_used = [0] * 4, [0] * 4, [], []

    def pass_on(dz, dy, q):
        j = chip(dz, dy) * 2 + c
        for way in routes(dz, dy, q):
            kv_copy(j, q, way, kv_used[way], near[way]).start()
            kv_used[way] += 1

    def pass_state_on(dz, dy):
        j = chip(dz, dy) * 2 + c
        for way in routes(dz, dy, 4):
            st_copy(j, way, st_used[way], near[way]).start()
            st_used[way] += 1
        st_pair_copy(j, len(st_pairs_used)).start()
        st_pairs_used.append((dz, dy))

    arrived = set()

    def pair_to_sib(dz, dy, q):
        arrived.add((dz, dy, q))
        if (dz, dy, q ^ 1) in arrived:
            pair_copy(chip(dz, dy) * 2 + c, q // 2, len(pairs_used)).start()
            pairs_used.append((dz, dy, q // 2))

    def arrival(dz, dy, q):
        j = chip(dz, dy) * 2 + c
        if q == 4:
            st_copy(j, 0, 0, sib).wait_recv()
            pass_state_on(dz, dy)
        else:
            kv_copy(j, q, 0, 0, sib).wait_recv()
            pass_on(dz, dy, q)
            pair_to_sib(dz, dy, q)

    x_copy(t, 0, right, 0).start()
    x_copy(t, 1, left, 1).start()
    x_copy(t, 1, right, 2).start()
    x_copy(t, 0, left, 3).start()

    def times(lhs, n):
        return mm(lhs, weights[:, n * 256 : n * 256 + 256])

    spots = (
        ((0, t * 128, 128),),
        ((0, left * 128, 64), (64, right * 128 + 64, 64)),
        ((0, left * 128 + 64, 64), (64, right * 128, 64)),
        ((0, far * 128, 128),),
    )

    def own_quarter(q):
        if q == 0:
            for load in loads[:3]:
                load.wait()
            lhs = rows[t]
        elif q == 1:
            x_copy(left, 0, right, 0).wait_recv()
            x_copy(left, 0, right, 4).start()
            x_copy(right, 1, left, 0).wait_recv()
            x_copy(right, 1, left, 5).start()
            lhs = jnp.concatenate([rows[left, 0:64], rows[right, 64:128]], axis=0)
        elif q == 2:
            x_copy(left, 1, right, 0).wait_recv()
            x_copy(right, 0, left, 0).wait_recv()
            lhs = jnp.concatenate([rows[left, 64:128], rows[right, 0:64]], axis=0)
        else:
            x_copy(far, 0, right, 0).wait_recv()
            x_copy(far, 1, left, 0).wait_recv()
            lhs = rows[far]
        kv[sp, q, 0:128] = times(lhs, 1).astype(BF16)
        turned = times(lhs, 2).T.astype(BF16)
        kv[sp, q, 128:256] = jnp.concatenate([turned[0:128], turned[128:256]], axis=1)
        pass_on(0, 0, q)
        pair_to_sib(0, 0, q)
        if q == 0:
            for load in loads[3:8]:
                load.wait()
        at = q % 2 * 128
        qt[q // 2, :, at : at + 128] = times(lhs, 0).T.astype(BF16)
        for n in range(2):
            block = times(lhs, 3 + n).astype(BF16)
            for here, there, count in spots[q]:
                retp[n, pl.ds(pl.multiple_of(there, 64), count)] = block[here : here + count]
        if q == 1:
            q_copy.start()
            for load in loads[8:]:
                load.wait()
            w_copy(t, None, right, 0).start()
            w_copy(t, None, left, 1).start()

    q_copy = remote(qt.at[0], qrecv, q_sem.at[0], q_sem.at[1], (partner, t))
    row = lax.broadcasted_iota(jnp.int32, (256, 256), 0)
    col = lax.broadcasted_iota(jnp.int32, (256, 256), 1)
    lane = lax.broadcasted_iota(jnp.int32, (256, 128), 1)

    for event in SCHEDULE[0][0]:
        if event == (0, 0, 4):
            retention_inside(lg, retp, rgate, retq, retadd, retfade, states, sp, row, col, lane)
            pass_state_on(0, 0)
        elif event[:2] == (0, 0):
            own_quarter(event[2])
        else:
            arrival(*event)

    def queries_of(half, block):
        big = block.astype(F32) * 0.125
        for hm in range(4):
            qpad[half, hm] = jnp.where(lax.div(row, 64) == hm, big, 0.0).astype(BF16)

    queries_of(0, qt[1])
    for half in range(2):
        for hm in range(4):
            peak[half, hm] = jnp.full((1, 256), LOWEST, F32)
            denom[half, hm] = jnp.zeros((1, 256), F32)
            acc[half, hm] = jnp.zeros((128, 256), F32)
    q_copy.wait_recv()
    queries_of(1, qrecv[...])

    def position(index, pair):
        early = jnp.where(
            index < 128, t * 128 + index,
            jnp.where(index < 192, left * 128 + index - 128, right * 128 + index - 128),
        )
        late = jnp.where(
            index < 64, left * 128 + 64 + index,
            jnp.where(index < 128, right * 128 + index - 64, far * 128 + index - 128),
        )
        return jnp.where(pair == 0, early, late)

    def attend(halves, near_chip, pair, bound=None):
        def keys(l):
            return jnp.concatenate([kv[near_chip * 2 + l, 2 * pair + p, 0:128] for p in range(2)], axis=0)

        def values(l, h):
            cut = slice(h * 128, h * 128 + 128)
            return jnp.concatenate(
                [kv[near_chip * 2 + l, 2 * pair + p, 128:256, cut] for p in range(2)], axis=1
            )

        if bound is not None:
            late = position(col, 1 - halves[0]) - position(row, pair) + (bound - near_chip * 2) * 512
        chains = [(n * 4 + hm, half, hm) for n, half in enumerate(halves) for hm in range(4)]
        for at, half, hm in chains:
            for l in range(2):
                scores = mm(keys(l), qpad[half, hm])
                if bound is not None:
                    scores = jnp.where(late >= l * 512, scores, -jnp.inf)
                sbuf[at, l] = scores
        fades = []
        for at, half, hm in chains:
            old = peak[half, hm]
            new = jnp.maximum(
                old, jnp.max(jnp.maximum(sbuf[at, 0], sbuf[at, 1]), axis=0, keepdims=True)
            )
            fade = jnp.exp(old - new)
            total = denom[half, hm] * fade
            for l in range(2):
                term = jnp.exp(sbuf[at, l] - new)
                total = total + jnp.sum(term, axis=0, keepdims=True)
                pbuf[at, l] = term.astype(BF16)
            denom[half, hm] = total
            peak[half, hm] = new
            fades.append(fade)
        for at, half, hm in chains:
            acc[half, hm] = acc[half, hm] * fades[at] + sum(
                mm(values(l, hm % 2), pbuf[at, l]) for l in range(2)
            )

    def w_stage(stage):
        if stage == W_NEAR:
            w_copy(left, None, right, 0).wait_recv()
            w_copy(left, 0, right, 2).start()
            w_copy(right, None, left, 0).wait_recv()
            w_copy(right, 1, left, 3).start()
            w_sib(left, 0, c).start()
            w_sib(right, 1, c).start()
        else:
            w_copy(far, 0, right, 0).wait_recv()
            w_copy(far, 1, left, 0).wait_recv()
            w_sib(far, 2, c).start()

    others = (left, right, far)

    def r_copy(slot, n):
        piece = rsend.at[pl.ds(pl.multiple_of(slot * 128, 128), 128)]
        return remote(piece, heads.at[1, t], r_send.at[n], r_recv.at[t], (sp, slot))

    def chain(j, state):
        own = states[j].astype(F32)
        return state * jnp.exp(own[64:65] + own[65:66] + own[66:67]) + own[0:64]

    def retention_end():
        for dz in (0, 1, 2, -1):
            for dy in (0, 1, 2, -1):
                st_copy(chip(dz, dy) * 2 + 1 - c, 0, 0, sib).wait_recv()
        state = lax.fori_loop(0, sp, chain, jnp.concatenate([init[0], init[1]], axis=1))
        state = jnp.concatenate([state[:, 0:128], state[:, 128:256]], axis=0)
        for b in range(2):
            for h in range(2):
                mine = (lane < 64) if h == 0 else (lane >= 64)
                older = mm(jnp.where(mine, retq[b], 0.0), state, HIGHEST)
                r = rgate[b, h] + older
                rsend[b * 256 : b * 256 + 256, h * 128 : h * 128 + 128] = head_norm(r, 1).astype(BF16)
            state = retfade[b] * state + retadd[b]
        for n, slot in enumerate(others):
            r_copy(slot, n).start()
        heads[1, t] = rsend[pl.ds(pl.multiple_of(t * 128, 128), 128)]

    codes = [(dz + 1) * 8 + (dy + 1) * 2 + pair for _, (dz, dy, pair) in SCHEDULE]

    def happen(events):
        for event in events:
            if event == RETENTION:
                retention_end()
            elif event in (W_NEAR, W_FAR):
                w_stage(event)
            else:
                arrival(*event)

    own_chip = lax.div(sp, 2)
    low, high = jnp.minimum(own_chip, 15 - own_chip), jnp.maximum(own_chip, 15 - own_chip)

    def handled(s, low, high):
        if high - low > 1:
            middle = (low + high) // 2
            return lax.cond(
                s < middle, lambda: handled(s, low, middle), lambda: handled(s, middle, high)
            )
        if low > 0:
            happen(SCHEDULE[low][0])
        return jnp.int32(codes[low])

    def tick(s, carry):
        code = handled(s, 0, len(SCHEDULE))
        near_chip = chip(lax.div(code, 8) - 1, lax.rem(lax.div(code, 2), 4) - 1)
        pair = lax.rem(code, 2)
        other = near_chip * 2 + 1 - c
        pair_copy(other, pair, 0).wait_recv()

        @pl.when(near_chip < low)
        def _():
            attend((0, 1), near_chip, pair)

        @pl.when(jnp.logical_and(near_chip >= low, near_chip < high))
        def _():
            attend((jnp.where(own_chip == high, 0, 1),), near_chip, pair)

        @pl.when(jnp.logical_or(near_chip == low, near_chip == high))
        def _():
            half = jnp.where(near_chip == own_chip, 0, 1)
            attend((half,), near_chip, pair, jnp.where(half == 0, sp, partner))

        return carry

    lax.fori_loop(0, len(SCHEDULE), tick, 0)
    happen(LAST)
    assert kv_used == [15] * 4 and len(pairs_used) == 32 and len(st_pairs_used) == 16

    def o_copy(src, at, count, dev, n, sem):
        place = heads.at[0, t, pl.ds(at, count)]
        return remote(src, place, o_send.at[n], o_recv.at[t, sem], dev)

    def finish(half):
        sides = []
        for h in range(2):
            weight_two = mix[:, h : h + 1]
            first = acc[half, h] / denom[half, h]
            second = acc[half, 2 + h] / denom[half, 2 + h]
            attn = first - weight_two * second
            sides.append((head_norm(attn, 0) * DIFF_SCALE).T * hgain[...])
        dsend[half] = jnp.concatenate(sides, axis=1).astype(BF16)

    def o_copies(half):
        if half == 0:
            return [
                o_copy(dsend.at[0, pl.ds(0, 64)], 64, 64, (sp, left), 0, 1),
                o_copy(dsend.at[0, pl.ds(64, 64)], 0, 64, (sp, right), 1, 0),
                o_copy(dsend.at[0, pl.ds(128, 128)], 0, 128, (sp, far), 2, 0),
            ]
        return [
            o_copy(dsend.at[1, pl.ds(0, 128)], 0, 128, (partner, t), 3, 0),
            o_copy(dsend.at[1, pl.ds(128, 64)], 0, 64, (partner, left), 4, 0),
            o_copy(dsend.at[1, pl.ds(192, 64)], 64, 64, (partner, right), 5, 1),
        ]

    for half in range(2):
        finish(half)
        for copy in o_copies(half):
            copy.start()

    def product(kind, last):
        def columns(n, carry):
            at = pl.ds(pl.multiple_of(n * 512, 512), 512)
            block = osum[:, at] if last else jnp.zeros((128, 512), F32)
            for slot in range(4):
                block += mm(heads[kind, slot], wout[slot, kind, :, at])
            if last:
                out[:, at] = block.astype(BF16)
            else:
                osum[:, at] = block
            return carry

        lax.fori_loop(0, 4, columns, 0)

    for slot in others:
        piece = wout.at[slot, 1 - c]
        remote(piece, piece, w_send.at[0], w_recv.at[slot, 2], sib).wait_recv()
    for slot in others:
        piece = heads.at[1, slot]
        remote(piece, piece, r_send.at[0], r_recv.at[slot], sib).wait_recv()
    product(1, False)

    def o_wait(slot, at, count, sem):
        piece = heads.at[0, slot, pl.ds(at, count)]
        remote(piece, piece, o_send.at[0], o_recv.at[slot, sem], sib).wait_recv()

    o_wait(far, 0, 128, 0)
    o_wait(t, 0, 128, 0)
    for slot in (left, right):
        o_wait(slot, 0, 64, 0)
        o_wait(slot, 64, 64, 1)
    product(0, True)

    for n in range(6):
        x_copy(t, 0, right, n).wait_send()
    for n in range(2):
        w_copy(t, None, right, n).wait_send()
        w_copy(t, n, right, 2 + n).wait_send()
    for n in range(3):
        w_sib(t, n, c).wait_send()
        r_copy(t, n).wait_send()
    q_copy.wait_send()
    for way in range(4):
        for n in range(kv_used[way]):
            kv_copy(0, 0, way, n, sib).wait_send()
        for n in range(st_used[way]):
            st_copy(0, way, n, sib).wait_send()
    for n in range(len(pairs_used)):
        pair_copy(0, 0, n).wait_send()
    for n in range(len(st_pairs_used)):
        st_pair_copy(0, n).wait_send()
    for half in range(2):
        for copy in o_copies(half):
            copy.wait_send()


def retention_inside(lg, retp, rgate, retq, retadd, retfade, states, sp, row, col, lane):
    state_row = lax.broadcasted_iota(jnp.int32, (128, 128), 0)
    upper = jnp.where(row <= col, 1.0, 0.0)
    adds, fades, lasts_of = [], [], []
    for b in range(2):
        span = slice(b * 256, b * 256 + 256)
        lb = lg[:, span]
        cum_rows = mm(jnp.concatenate([lb, lb, lb, lb], axis=0), upper, HIGHEST)
        rq, rk = retp[0, span, 0:128], retp[0, span, 128:256]
        cols, lasts = [], []
        for h in range(2):
            cum_col = jnp.sum(jnp.where(col <= row, lb[h : h + 1], 0.0), axis=1, keepdims=True)
            cols.append(cum_col)
            lasts.append(jnp.sum(lb[h : h + 1], axis=1, keepdims=True))
            mine = (lane < 64) if h == 0 else (lane >= 64)
            raw = nt(jnp.where(mine, rq, jnp.zeros_like(rq)), rk)
            gap = jnp.where(col <= row, cum_col - cum_rows[h : h + 1], -jnp.inf)
            gate = (raw * 0.125 * jnp.exp(gap)).astype(BF16)
            rgate[b, h] = mm(gate, retp[1, span, h * 128 : h * 128 + 128])
        factor = jnp.where(lane < 64, jnp.exp(lasts[0] - cols[0]), jnp.exp(lasts[1] - cols[1]))
        keys = (rk.astype(F32) * 0.125 * factor).T.astype(BF16)
        both = mm(keys, retp[1, span])
        adds.append(jnp.where(state_row < 64, both[:, 0:128], both[:, 128:256]))
        fades.append(jnp.where(state_row < 64, jnp.exp(lasts[0]), jnp.exp(lasts[1])))
        grow = jnp.where(lane < 64, jnp.exp(cols[0]), jnp.exp(cols[1]))
        retq[b] = rq.astype(F32) * grow
        retadd[b] = adds[b]
        retfade[b] = fades[b]
        lasts_of.append(lasts)
    own = fades[1] * adds[0] + adds[1]
    states[sp, 0:64] = jnp.concatenate([own[0:64], own[64:128]], axis=1).astype(BF16)
    tile_lane = lax.broadcasted_iota(jnp.int32, (16, 256), 1)
    tile_row = lax.broadcasted_iota(jnp.int32, (16, 256), 0)
    total = jnp.where(
        tile_lane < 128, lasts_of[0][0] + lasts_of[1][0], lasts_of[0][1] + lasts_of[1][1]
    )
    high = total.astype(BF16).astype(F32)
    middle = (total - high).astype(BF16).astype(F32)
    low = total - high - middle
    tile = jnp.where(tile_row == 0, high, jnp.where(tile_row == 1, middle, low))
    states[sp, 64:80] = tile.astype(BF16)


def on_device(
    tokens, norm_gain, w_query_one, w_query_two, w_key_one, w_key_two, w_value, mix_lambda,
    head_gain, w_ret_query, w_ret_key, w_ret_value, retain_log, init_state, w_out_diff, w_out_ret,
):
    vmem = pl.BlockSpec(memory_space=pltpu.VMEM)
    hbm = pl.BlockSpec(memory_space=pl.ANY)
    dma = pltpu.SemaphoreType.DMA
    return pl.pallas_call(
        kernel,
        out_shape=jax.ShapeDtypeStruct((128, 2048), BF16),
        in_specs=[vmem, vmem] + [hbm] * 5 + [vmem, vmem] + [hbm] * 3 + [vmem, vmem] + [hbm] * 2,
        out_specs=vmem,
        scratch_shapes=[
            pltpu.VMEM((4, 128, 2048), BF16),
            pltpu.VMEM((2048, 1280), BF16),
            pltpu.VMEM((2, 256, 256), BF16),
            pltpu.VMEM((256, 256), BF16),
            pltpu.VMEM((32, 4, 256, 256), BF16),
            pltpu.VMEM((32, 80, 256), BF16),
            pltpu.VMEM((2, 512, 256), BF16),
            pltpu.VMEM((4, 2, 256, 2048), BF16),
            pltpu.VMEM((2, 4, 256, 256), BF16),
            pltpu.VMEM((2, 4, 128, 256), F32),
            pltpu.VMEM((2, 4, 1, 256), F32),
            pltpu.VMEM((2, 4, 1, 256), F32),
            pltpu.VMEM((8, 2, 256, 256), F32),
            pltpu.VMEM((8, 2, 256, 256), BF16),
            pltpu.VMEM((2, 2, 256, 128), F32),
            pltpu.VMEM((2, 256, 128), F32),
            pltpu.VMEM((2, 128, 128), F32),
            pltpu.VMEM((2, 128, 128), F32),
            pltpu.VMEM((128, 2048), F32),
            pltpu.VMEM((2, 256, 256), BF16),
            pltpu.VMEM((512, 256), BF16),
            pltpu.VMEM((2, 4, 128, 256), BF16),
            dma((10,)),
            dma((6,)),
            dma((4, 2)),
            dma((7,)),
            dma((4, 3)),
            dma((4, 15)),
            dma((32, 4)),
            dma((32,)),
            dma((32, 2)),
            dma((4, 10)),
            dma((32,)),
            dma((16,)),
            dma((2,)),
            dma((6,)),
            dma((4, 2)),
            dma((3,)),
            dma((4,)),
        ],
        compiler_params=pltpu.CompilerParams(
            collective_id=0, has_side_effects=True, vmem_limit_bytes=53 * 1024 * 1024,
        ),
        cost_estimate=pl.CostEstimate(
            flops=20_000_000_000, bytes_accessed=10_000_000, transcendentals=17_000_000
        ),
        name="layer",
    )(
        tokens, norm_gain.reshape(1, -1), w_query_one, w_query_two, w_key_one, w_key_two, w_value,
        mix_lambda.reshape(1, -1), head_gain.reshape(1, -1),
        w_ret_query, w_ret_key, w_ret_value, retain_log, init_state, w_out_diff, w_out_ret,
    )


def solution(mesh):
    both = ("sp", "tp")
    return jax.shard_map(
        on_device,
        mesh=mesh,
        in_specs=(
            P(both, None), P(), P(None, "tp"), P(None, "tp"), P(None, "tp"), P(None, "tp"),
            P(None, "tp"), P("tp"), P(), P(None, "tp"), P(None, "tp"), P(None, "tp"),
            P("tp", "sp"), P("tp", None, None), P("tp", None), P("tp", None),
        ),
        out_specs=P(both, None),
        check_vma=False,
    )
```

```python
import jax
import jax.numpy as jnp
from jax import lax
from jax.experimental import pallas as pl
from jax.experimental.pallas import tpu as pltpu
from jax.sharding import PartitionSpec as P

NORM_EPS = 1e-06
HEAD_EPS = 1e-05
DIFF_SCALE = 0.8
MESH = pl.DeviceIdType.MESH
F32 = jnp.float32
BF16 = jnp.bfloat16
HIGHEST = lax.Precision.HIGHEST
LOWEST = -3.0e38


W_NEAR, W_FAR, RETENTION = range(3)
SCHEDULE = (
    (((0, 0, 0), (-1, 0, 0), (0, 0, 1), (0, -1, 0), (0, 0, 2), (-1, 0, 1), (0, 1, 0), (0, 1, 1), (2, 0, 0), (1, 0, 0), (0, 0, 3), (0, 0, 4), (1, 0, 2), (0, -1, 2), (1, 0, 1)), (-1, 0, 0)),
    ((), (0, 0, 0)),
    (((-1, -1, 0),), (0, 1, 0)),
    (((2, 0, 1), (1, 0, 3), (-1, 1, 0), (-1, 1, 1), (0, 1, 4), (-1, 0, 2)), (0, 0, 1)),
    ((), (1, 0, 1)),
    (((0, 1, 2), (0, -1, 4), (-1, 0, 3), (0, -1, 3)), (-1, 1, 0)),
    (((1, -1, 0), (0, 1, 3)), (1, 0, 0)),
    ((), (0, -1, 1)),
    (((0, -1, 1), (1, 1, 0), (2, 0, 2), (-1, -1, 1), (1, -1, 1)), (-1, 0, 1)),
    ((), (2, 0, 0)),
    (((2, 0, 3), (2, -1, 1), (1, 1, 1), (0, 2, 0)), (0, 1, 1)),
    ((), (0, -1, 0)),
    (((1, -1, 4), (2, 1, 1), (1, -1, 2), (2, 1, 0)), (-1, -1, 0)),
    (((1, -1, 3), (-1, -1, 2), (2, -1, 0)), (1, -1, 0)),
    (((1, 1, 4), (0, 2, 4)), (1, 1, 0)),
    ((), (2, 1, 0)),
    (((0, 2, 2), (-1, 1, 2), (1, 1, 2), (-1, 1, 4)), (2, -1, 0)),
    (((-1, -1, 4), W_NEAR, (-1, 0, 4), (-1, -1, 3), (0, 2, 3)), (2, 0, 1)),
    (((1, 2, 0), (1, 1, 3), (-1, 1, 3)), (1, -1, 1)),
    (((1, 0, 4), (2, -1, 3), (2, -1, 2)), (-1, -1, 1)),
    (((2, 1, 2), (-1, 2, 4)), (-1, 1, 1)),
    (((2, 1, 4), (1, 2, 4), (-1, 2, 1)), (2, -1, 1)),
    (((1, 2, 1), (-1, 2, 0), (1, 2, 3), (-1, 2, 2)), (1, 1, 1)),
    (((0, 2, 1), (2, -1, 4)), (0, 2, 1)),
    (((2, 2, 1), (1, 2, 2), (2, 0, 4), (-1, 2, 3), (2, 2, 4)), (-1, 2, 0)),
    ((), (1, 2, 0)),
    (((2, 2, 2), (2, 1, 3), RETENTION, (2, 2, 0), (2, 2, 3)), (0, 2, 0)),
    ((W_FAR,), (-1, 2, 1)),
    ((), (1, 2, 1)),
    ((), (2, 1, 1)),
    ((), (2, 2, 0)),
    ((), (2, 2, 1)),
)
LAST = ()
PLUS_Y, MINUS_Y, PLUS_Z, MINUS_Z = range(4)
STEPS = ((0, 1), (0, -1), (1, 0), (-1, 0))
ALONG_Y_FIRST = (0, 3, 4)
ONWARD_BY_PLUS = (0, 1, 4)


def nt(a, b, precision=None):
    return lax.dot_general(
        a, b, (((1,), (1,)), ((), ())), preferred_element_type=F32, precision=precision
    )


def mm(a, b, precision=None):
    return jnp.dot(a, b, preferred_element_type=F32, precision=precision)


def head_norm(values, axis):
    return values * lax.rsqrt(jnp.mean(values * values, axis=axis, keepdims=True) + HEAD_EPS)


def routes(dz, dy, quarter):
    y_first = quarter in ALONG_Y_FIRST
    ways = ((PLUS_Y, MINUS_Y), (PLUS_Z, MINUS_Z))
    first, second = ways if y_first else ways[::-1]
    a, b = (dy, dz) if y_first else (dz, dy)
    by_plus = quarter in ONWARD_BY_PLUS
    if a == 0 and b == 0:
        return first + second
    line, at = (first, a) if b == 0 else (second, b)
    onward = ()
    if at == -1 and by_plus:
        onward = (line[0],)
    elif at == 1 and not by_plus:
        onward = (line[1],)
    return onward + (second if b == 0 else ())


def kernel(
    tokens, gain, wq1, wq2, wk1, wk2, wv, mix, hgain, wrq, wrk, wrv, logs, init, wod, wor,
    out,
    rows, weights, qt, qrecv, kv, states, retp, wout, qpad, acc, peak, denom, sbuf, pbuf, rgate, retq, retadd, retfade, osum,
    dsend, rsend, heads,
    load_sem, x_send, x_recv, w_send, w_recv, kv_send, kv_recv, pair_send, pair_recv,
    st_send, st_recv, st_pair_send, q_sem, o_send, o_recv, r_send, r_recv,
):
    sp = lax.axis_index("sp")
    t = lax.axis_index("tp")
    z, y, c = lax.div(sp, 8), lax.rem(lax.div(sp, 2), 4), lax.rem(sp, 2)
    partner = 31 - sp
    sib = (sp + 1 - 2 * c, t)
    left, right, far = lax.rem(t + 3, 4), lax.rem(t + 1, 4), lax.rem(t + 2, 4)

    def chip(dz, dy):
        return lax.rem(z + dz + 4, 4) * 4 + lax.rem(y + dy + 4, 4)

    near = [(chip(dz, dy) * 2 + c, t) for dz, dy in STEPS]

    loads = []
    sources = (
        (wk1, 256, 128), (wk2, 384, 128), (wv, 512, 256), (wq1, 0, 128), (wq2, 128, 128),
        (wrq, 768, 128), (wrk, 896, 128), (wrv, 1024, 256),
    )
    for k, (ref, at, width) in enumerate(sources):
        group = load_sem.at[0 if k < 3 else 1]
        loads.append(pltpu.make_async_copy(ref, weights.at[:, pl.ds(at, width)], group))
    for k, ref in enumerate((wod, wor)):
        loads.append(pltpu.make_async_copy(ref, wout.at[t, k], load_sem.at[2]))
    for load in loads:
        load.start()

    def drain(piece, sem):
        pltpu.make_async_copy(piece, piece, sem).wait()

    barrier = pltpu.get_barrier_semaphore()
    peers = [(sp, left), (sp, right), (sp, far), sib, *near] + [(partner, d) for d in range(4)]
    for peer in peers:
        pl.semaphore_signal(barrier, inc=1, device_id=peer, device_id_type=MESH)

    for chunk in range(2):
        floats = tokens[chunk * 64 : chunk * 64 + 64].astype(F32)
        scale = lax.rsqrt(jnp.mean(floats * floats, axis=-1, keepdims=True) + NORM_EPS)
        rows[t, chunk * 64 : chunk * 64 + 64] = (floats * scale * gain[...]).astype(BF16)
    lg = logs[...]

    pl.semaphore_wait(barrier, len(peers))

    def remote(src, dst, ssem, rsem, dev):
        return pltpu.make_async_remote_copy(
            src_ref=src, dst_ref=dst, send_sem=ssem, recv_sem=rsem, device_id=dev,
            device_id_type=MESH,
        )

    def x_copy(slot, chunk, to, n):
        piece = rows.at[slot, pl.ds(chunk * 64, 64)]
        return remote(piece, piece, x_send, x_recv.at[slot, chunk], (sp, to))

    def w_copy(slot, part, to, n):
        piece = wout.at[slot, c] if part is None else wout.at[slot, c, pl.ds(part * 128, 128)]
        rsem = w_recv.at[slot, 0 if part is None else part]
        return remote(piece, piece, w_send, rsem, (sp, to))

    def w_sib(slot, n, kind):
        piece = wout.at[slot, kind]
        return remote(piece, piece, w_send, w_recv.at[slot, 2], sib)

    def kv_copy(j, q, way, n, dev):
        return remote(kv.at[j, q], kv.at[j, q], kv_send.at[way], kv_recv.at[lax.div(j, 2), q], dev)

    def st_copy(j, way, n, dev):
        return remote(states.at[j], states.at[j], st_send.at[way], st_recv.at[j], dev)

    def pair_copy(j, pair, n):
        piece = kv.at[j, pl.ds(2 * pair, 2)]
        return remote(piece, piece, pair_send, pair_recv.at[lax.div(j, 2), pair], sib)

    def st_pair_copy(j, n):
        return remote(states.at[j], states.at[j], st_pair_send, st_recv.at[j], sib)

    kv_used, st_used, pairs_used, st_pairs_used = [0] * 4, [0] * 4, [], []

    def pass_on(dz, dy, q):
        j = chip(dz, dy) * 2 + c
        for way in routes(dz, dy, q):
            kv_copy(j, q, way, kv_used[way], near[way]).start()
            kv_used[way] += 1

    def pass_state_on(dz, dy):
        j = chip(dz, dy) * 2 + c
        for way in routes(dz, dy, 4):
            st_copy(j, way, st_used[way], near[way]).start()
            st_used[way] += 1
        st_pair_copy(j, len(st_pairs_used)).start()
        st_pairs_used.append((dz, dy))

    arrived = set()

    def pair_to_sib(dz, dy, q):
        arrived.add((dz, dy, q))
        if (dz, dy, q ^ 1) in arrived:
            pair_copy(chip(dz, dy) * 2 + c, q // 2, len(pairs_used)).start()
            pairs_used.append((dz, dy, q // 2))

    def arrival(dz, dy, q):
        j = chip(dz, dy) * 2 + c
        if q == 4:
            st_copy(j, 0, 0, sib).wait_recv()
            pass_state_on(dz, dy)
        else:
            kv_copy(j, q, 0, 0, sib).wait_recv()
            pass_on(dz, dy, q)
            pair_to_sib(dz, dy, q)

    x_copy(t, 0, right, 0).start()
    x_copy(t, 1, left, 1).start()
    x_copy(t, 1, right, 2).start()
    x_copy(t, 0, left, 3).start()

    def times(lhs, n):
        return mm(lhs, weights[:, n * 256 : n * 256 + 256])

    spots = (
        ((0, t * 128, 128),),
        ((0, left * 128, 64), (64, right * 128 + 64, 64)),
        ((0, left * 128 + 64, 64), (64, right * 128, 64)),
        ((0, far * 128, 128),),
    )

    def own_quarter(q):
        if q == 0:
            drain(weights.at[:, pl.ds(256, 512)], load_sem.at[0])
            lhs = rows[t]
        elif q == 1:
            x_copy(left, 0, right, 0).wait_recv()
            x_copy(left, 0, right, 4).start()
            x_copy(right, 1, left, 0).wait_recv()
            x_copy(right, 1, left, 5).start()
            lhs = jnp.concatenate([rows[left, 0:64], rows[right, 64:128]], axis=0)
        elif q == 2:
            x_copy(left, 1, right, 0).wait_recv()
            x_copy(right, 0, left, 0).wait_recv()
            lhs = jnp.concatenate([rows[left, 64:128], rows[right, 0:64]], axis=0)
        else:
            x_copy(far, 0, right, 0).wait_recv()
            x_copy(far, 1, left, 0).wait_recv()
            lhs = rows[far]
        kv[sp, q, 0:128] = times(lhs, 1).astype(BF16)
        turned = times(lhs, 2).T.astype(BF16)
        kv[sp, q, 128:256] = jnp.concatenate([turned[0:128], turned[128:256]], axis=1)
        pass_on(0, 0, q)
        pair_to_sib(0, 0, q)
        if q == 0:
            drain(weights.at[:, pl.ds(0, 768)], load_sem.at[1])
        at = q % 2 * 128
        qt[q // 2, :, at : at + 128] = times(lhs, 0).T.astype(BF16)
        for n in range(2):
            block = times(lhs, 3 + n).astype(BF16)
            for here, there, count in spots[q]:
                retp[n, pl.ds(pl.multiple_of(there, 64), count)] = block[here : here + count]
        if q == 1:
            q_copy.start()
            drain(wout.at[t], load_sem.at[2])
            w_copy(t, None, right, 0).start()
            w_copy(t, None, left, 1).start()

    q_copy = remote(qt.at[0], qrecv, q_sem.at[0], q_sem.at[1], (partner, t))
    row = lax.broadcasted_iota(jnp.int32, (256, 256), 0)
    col = lax.broadcasted_iota(jnp.int32, (256, 256), 1)
    lane = lax.broadcasted_iota(jnp.int32, (256, 128), 1)

    for event in SCHEDULE[0][0]:
        if event == (0, 0, 4):
            retention_inside(lg, retp, rgate, retq, retadd, retfade, states, sp, row, col, lane)
            pass_state_on(0, 0)
        elif event[:2] == (0, 0):
            own_quarter(event[2])
        else:
            arrival(*event)

    def queries_of(half, block):
        big = block.astype(F32) * 0.125
        for hm in range(4):
            qpad[half, hm] = jnp.where(lax.div(row, 64) == hm, big, 0.0).astype(BF16)

    queries_of(0, qt[1])
    for half in range(2):
        for hm in range(4):
            peak[half, hm] = jnp.full((1, 256), LOWEST, F32)
            denom[half, hm] = jnp.zeros((1, 256), F32)
            acc[half, hm] = jnp.zeros((128, 256), F32)
    q_copy.wait_recv()
    queries_of(1, qrecv[...])

    def position(index, pair):
        early = jnp.where(
            index < 128, t * 128 + index,
            jnp.where(index < 192, left * 128 + index - 128, right * 128 + index - 128),
        )
        late = jnp.where(
            index < 64, left * 128 + 64 + index,
            jnp.where(index < 128, right * 128 + index - 64, far * 128 + index - 128),
        )
        return jnp.where(pair == 0, early, late)

    def attend(halves, near_chip, pair, bound=None):
        def keys(l):
            return jnp.concatenate([kv[near_chip * 2 + l, 2 * pair + p, 0:128] for p in range(2)], axis=0)

        def values(l, h):
            cut = slice(h * 128, h * 128 + 128)
            return jnp.concatenate(
                [kv[near_chip * 2 + l, 2 * pair + p, 128:256, cut] for p in range(2)], axis=1
            )

        if bound is not None:
            late = position(col, 1 - halves[0]) - position(row, pair) + (bound - near_chip * 2) * 512
        chains = [(n * 4 + hm, half, hm) for n, half in enumerate(halves) for hm in range(4)]
        for at, half, hm in chains:
            for l in range(2):
                scores = mm(keys(l), qpad[half, hm])
                if bound is not None:
                    scores = jnp.where(late >= l * 512, scores, -jnp.inf)
                sbuf[at, l] = scores
        fades = []
        for at, half, hm in chains:
            old = peak[half, hm]
            new = jnp.maximum(
                old, jnp.max(jnp.maximum(sbuf[at, 0], sbuf[at, 1]), axis=0, keepdims=True)
            )
            fade = jnp.exp(old - new)
            total = denom[half, hm] * fade
            for l in range(2):
                term = jnp.exp(sbuf[at, l] - new)
                total = total + jnp.sum(term, axis=0, keepdims=True)
                pbuf[at, l] = term.astype(BF16)
            denom[half, hm] = total
            peak[half, hm] = new
            fades.append(fade)
        for at, half, hm in chains:
            acc[half, hm] = acc[half, hm] * fades[at] + sum(
                mm(values(l, hm % 2), pbuf[at, l]) for l in range(2)
            )

    def w_stage(stage):
        if stage == W_NEAR:
            w_copy(left, None, right, 0).wait_recv()
            w_copy(left, 0, right, 2).start()
            w_copy(right, None, left, 0).wait_recv()
            w_copy(right, 1, left, 3).start()
            w_sib(left, 0, c).start()
            w_sib(right, 1, c).start()
        else:
            w_copy(far, 0, right, 0).wait_recv()
            w_copy(far, 1, left, 0).wait_recv()
            w_sib(far, 2, c).start()

    others = (left, right, far)

    def r_copy(slot, n):
        piece = rsend.at[pl.ds(pl.multiple_of(slot * 128, 128), 128)]
        return remote(piece, heads.at[1, t], r_send, r_recv.at[t], (sp, slot))

    def chain(j, state):
        own = states[j].astype(F32)
        return state * jnp.exp(own[64:65] + own[65:66] + own[66:67]) + own[0:64]

    def retention_end():
        for dz in (0, 1, 2, -1):
            for dy in (0, 1, 2, -1):
                st_copy(chip(dz, dy) * 2 + 1 - c, 0, 0, sib).wait_recv()
        state = lax.fori_loop(0, sp, chain, jnp.concatenate([init[0], init[1]], axis=1))
        state = jnp.concatenate([state[:, 0:128], state[:, 128:256]], axis=0)
        for b in range(2):
            for h in range(2):
                mine = (lane < 64) if h == 0 else (lane >= 64)
                older = mm(jnp.where(mine, retq[b], 0.0), state, HIGHEST)
                r = rgate[b, h] + older
                rsend[b * 256 : b * 256 + 256, h * 128 : h * 128 + 128] = head_norm(r, 1).astype(BF16)
            state = retfade[b] * state + retadd[b]
        for n, slot in enumerate(others):
            r_copy(slot, n).start()
        heads[1, t] = rsend[pl.ds(pl.multiple_of(t * 128, 128), 128)]

    codes = [(dz + 1) * 8 + (dy + 1) * 2 + pair for _, (dz, dy, pair) in SCHEDULE]

    def happen(events):
        for event in events:
            if event == RETENTION:
                retention_end()
            elif event in (W_NEAR, W_FAR):
                w_stage(event)
            else:
                arrival(*event)

    own_chip = lax.div(sp, 2)
    low, high = jnp.minimum(own_chip, 15 - own_chip), jnp.maximum(own_chip, 15 - own_chip)

    def handled(s, low, high):
        if high - low > 1:
            middle = (low + high) // 2
            return lax.cond(
                s < middle, lambda: handled(s, low, middle), lambda: handled(s, middle, high)
            )
        if low > 0:
            happen(SCHEDULE[low][0])
        return jnp.int32(codes[low])

    def tick(s, carry):
        code = handled(s, 0, len(SCHEDULE))
        near_chip = chip(lax.div(code, 8) - 1, lax.rem(lax.div(code, 2), 4) - 1)
        pair = lax.rem(code, 2)
        other = near_chip * 2 + 1 - c
        pair_copy(other, pair, 0).wait_recv()

        @pl.when(near_chip < low)
        def _():
            attend((0, 1), near_chip, pair)

        @pl.when(jnp.logical_and(near_chip >= low, near_chip < high))
        def _():
            attend((jnp.where(own_chip == high, 0, 1),), near_chip, pair)

        @pl.when(jnp.logical_or(near_chip == low, near_chip == high))
        def _():
            half = jnp.where(near_chip == own_chip, 0, 1)
            attend((half,), near_chip, pair, jnp.where(half == 0, sp, partner))

        return carry

    lax.fori_loop(0, len(SCHEDULE), tick, 0)
    happen(LAST)
    assert kv_used == [15] * 4 and len(pairs_used) == 32 and len(st_pairs_used) == 16

    def o_copy(src, at, count, dev, n, sem):
        place = heads.at[0, t, pl.ds(at, count)]
        return remote(src, place, o_send, o_recv.at[t, sem], dev)

    def finish(half):
        sides = []
        for h in range(2):
            weight_two = mix[:, h : h + 1]
            first = acc[half, h] / denom[half, h]
            second = acc[half, 2 + h] / denom[half, 2 + h]
            attn = first - weight_two * second
            sides.append((head_norm(attn, 0) * DIFF_SCALE).T * hgain[...])
        dsend[half] = jnp.concatenate(sides, axis=1).astype(BF16)

    def o_copies(half):
        if half == 0:
            return [
                o_copy(dsend.at[0, pl.ds(0, 64)], 64, 64, (sp, left), 0, 1),
                o_copy(dsend.at[0, pl.ds(64, 64)], 0, 64, (sp, right), 1, 0),
                o_copy(dsend.at[0, pl.ds(128, 128)], 0, 128, (sp, far), 2, 0),
            ]
        return [
            o_copy(dsend.at[1, pl.ds(0, 128)], 0, 128, (partner, t), 3, 0),
            o_copy(dsend.at[1, pl.ds(128, 64)], 0, 64, (partner, left), 4, 0),
            o_copy(dsend.at[1, pl.ds(192, 64)], 64, 64, (partner, right), 5, 1),
        ]

    for half in range(2):
        finish(half)
        for copy in o_copies(half):
            copy.start()

    def product(kind, last):
        def columns(n, carry):
            at = pl.ds(pl.multiple_of(n * 512, 512), 512)
            block = osum[:, at] if last else jnp.zeros((128, 512), F32)
            for slot in range(4):
                block += mm(heads[kind, slot], wout[slot, kind, :, at])
            if last:
                out[:, at] = block.astype(BF16)
            else:
                osum[:, at] = block
            return carry

        lax.fori_loop(0, 4, columns, 0)

    for slot in others:
        piece = wout.at[slot, 1 - c]
        remote(piece, piece, w_send, w_recv.at[slot, 2], sib).wait_recv()
    for slot in others:
        piece = heads.at[1, slot]
        remote(piece, piece, r_send, r_recv.at[slot], sib).wait_recv()
    product(1, False)

    def o_wait(slot, at, count, sem):
        piece = heads.at[0, slot, pl.ds(at, count)]
        remote(piece, piece, o_send, o_recv.at[slot, sem], sib).wait_recv()

    o_wait(far, 0, 128, 0)
    o_wait(t, 0, 128, 0)
    for slot in (left, right):
        o_wait(slot, 0, 64, 0)
        o_wait(slot, 64, 64, 1)
    product(0, True)

    drain(rows.at[pl.ds(0, 3)], x_send)
    drain(wout.at[pl.ds(0, 3)], w_send)
    drain(rsend.at[pl.ds(0, 384)], r_send)
    drain(dsend, o_send)
    q_copy.wait_send()
    for way in range(4):
        drain(kv.at[pl.ds(0, kv_used[way]), 0], kv_send.at[way])
        drain(states.at[pl.ds(0, st_used[way])], st_send.at[way])
    drain(kv.at[:, pl.ds(0, 2)], pair_send)
    drain(states.at[pl.ds(0, 16)], st_pair_send)


def retention_inside(lg, retp, rgate, retq, retadd, retfade, states, sp, row, col, lane):
    state_row = lax.broadcasted_iota(jnp.int32, (128, 128), 0)
    upper = jnp.where(row <= col, 1.0, 0.0)
    adds, fades, lasts_of = [], [], []
    for b in range(2):
        span = slice(b * 256, b * 256 + 256)
        lb = lg[:, span]
        cum_rows = mm(jnp.concatenate([lb, lb, lb, lb], axis=0), upper, HIGHEST)
        rq, rk = retp[0, span, 0:128], retp[0, span, 128:256]
        cols, lasts = [], []
        for h in range(2):
            cum_col = jnp.sum(jnp.where(col <= row, lb[h : h + 1], 0.0), axis=1, keepdims=True)
            cols.append(cum_col)
            lasts.append(jnp.sum(lb[h : h + 1], axis=1, keepdims=True))
            mine = (lane < 64) if h == 0 else (lane >= 64)
            raw = nt(jnp.where(mine, rq, jnp.zeros_like(rq)), rk)
            gap = jnp.where(col <= row, cum_col - cum_rows[h : h + 1], -jnp.inf)
            gate = (raw * 0.125 * jnp.exp(gap)).astype(BF16)
            rgate[b, h] = mm(gate, retp[1, span, h * 128 : h * 128 + 128])
        factor = jnp.where(lane < 64, jnp.exp(lasts[0] - cols[0]), jnp.exp(lasts[1] - cols[1]))
        keys = (rk.astype(F32) * 0.125 * factor).T.astype(BF16)
        both = mm(keys, retp[1, span])
        adds.append(jnp.where(state_row < 64, both[:, 0:128], both[:, 128:256]))
        fades.append(jnp.where(state_row < 64, jnp.exp(lasts[0]), jnp.exp(lasts[1])))
        grow = jnp.where(lane < 64, jnp.exp(cols[0]), jnp.exp(cols[1]))
        retq[b] = rq.astype(F32) * grow
        retadd[b] = adds[b]
        retfade[b] = fades[b]
        lasts_of.append(lasts)
    own = fades[1] * adds[0] + adds[1]
    states[sp, 0:64] = jnp.concatenate([own[0:64], own[64:128]], axis=1).astype(BF16)
    tile_lane = lax.broadcasted_iota(jnp.int32, (16, 256), 1)
    tile_row = lax.broadcasted_iota(jnp.int32, (16, 256), 0)
    total = jnp.where(
        tile_lane < 128, lasts_of[0][0] + lasts_of[1][0], lasts_of[0][1] + lasts_of[1][1]
    )
    high = total.astype(BF16).astype(F32)
    middle = (total - high).astype(BF16).astype(F32)
    low = total - high - middle
    tile = jnp.where(tile_row == 0, high, jnp.where(tile_row == 1, middle, low))
    states[sp, 64:80] = tile.astype(BF16)


def on_device(
    tokens, norm_gain, w_query_one, w_query_two, w_key_one, w_key_two, w_value, mix_lambda,
    head_gain, w_ret_query, w_ret_key, w_ret_value, retain_log, init_state, w_out_diff, w_out_ret,
):
    vmem = pl.BlockSpec(memory_space=pltpu.VMEM)
    hbm = pl.BlockSpec(memory_space=pl.ANY)
    dma = pltpu.SemaphoreType.DMA
    return pl.pallas_call(
        kernel,
        out_shape=jax.ShapeDtypeStruct((128, 2048), BF16),
        in_specs=[vmem, vmem] + [hbm] * 5 + [vmem, vmem] + [hbm] * 3 + [vmem, vmem] + [hbm] * 2,
        out_specs=vmem,
        scratch_shapes=[
            pltpu.VMEM((4, 128, 2048), BF16),
            pltpu.VMEM((2048, 1280), BF16),
            pltpu.VMEM((2, 256, 256), BF16),
            pltpu.VMEM((256, 256), BF16),
            pltpu.VMEM((32, 4, 256, 256), BF16),
            pltpu.VMEM((32, 80, 256), BF16),
            pltpu.VMEM((2, 512, 256), BF16),
            pltpu.VMEM((4, 2, 256, 2048), BF16),
            pltpu.VMEM((2, 4, 256, 256), BF16),
            pltpu.VMEM((2, 4, 128, 256), F32),
            pltpu.VMEM((2, 4, 1, 256), F32),
            pltpu.VMEM((2, 4, 1, 256), F32),
            pltpu.VMEM((8, 2, 256, 256), F32),
            pltpu.VMEM((8, 2, 256, 256), BF16),
            pltpu.VMEM((2, 2, 256, 128), F32),
            pltpu.VMEM((2, 256, 128), F32),
            pltpu.VMEM((2, 128, 128), F32),
            pltpu.VMEM((2, 128, 128), F32),
            pltpu.VMEM((128, 2048), F32),
            pltpu.VMEM((2, 256, 256), BF16),
            pltpu.VMEM((512, 256), BF16),
            pltpu.VMEM((2, 4, 128, 256), BF16),
            dma((3,)),
            dma,
            dma((4, 2)),
            dma,
            dma((4, 3)),
            dma((4,)),
            dma((16, 4)),
            dma,
            dma((16, 2)),
            dma((4,)),
            dma((32,)),
            dma,
            dma((2,)),
            dma,
            dma((4, 2)),
            dma,
            dma((4,)),
        ],
        compiler_params=pltpu.CompilerParams(
            collective_id=0, has_side_effects=True, vmem_limit_bytes=53 * 1024 * 1024,
        ),
        cost_estimate=pl.CostEstimate(
            flops=20_000_000_000, bytes_accessed=10_000_000, transcendentals=17_000_000
        ),
        name="layer",
    )(
        tokens, norm_gain.reshape(1, -1), w_query_one, w_query_two, w_key_one, w_key_two, w_value,
        mix_lambda.reshape(1, -1), head_gain.reshape(1, -1),
        w_ret_query, w_ret_key, w_ret_value, retain_log, init_state, w_out_diff, w_out_ret,
    )


def solution(mesh):
    both = ("sp", "tp")
    return jax.shard_map(
        on_device,
        mesh=mesh,
        in_specs=(
            P(both, None), P(), P(None, "tp"), P(None, "tp"), P(None, "tp"), P(None, "tp"),
            P(None, "tp"), P("tp"), P(), P(None, "tp"), P(None, "tp"), P(None, "tp"),
            P("tp", "sp"), P("tp", None, None), P("tp", None), P("tp", None),
        ),
        out_specs=P(both, None),
        check_vma=False,
    )
```

```python
import jax
import jax.numpy as jnp
from jax import lax
from jax.experimental import pallas as pl
from jax.experimental.pallas import tpu as pltpu
from jax.sharding import PartitionSpec as P

NORM_EPS = 1e-06
HEAD_EPS = 1e-05
DIFF_SCALE = 0.8
MESH = pl.DeviceIdType.MESH
F32 = jnp.float32
BF16 = jnp.bfloat16
HIGHEST = lax.Precision.HIGHEST
LOWEST = -3.0e38


W_NEAR, W_FAR, RETENTION = range(3)
SCHEDULE = (
    (((0, 0, 0), (0, -1, 0), (0, 0, 1), (-1, 0, 0), (0, 1, 0), (0, 0, 2), (1, -1, 0), (-1, 0, 1), (0, 1, 1), (0, 0, 3), (1, 0, 0), (0, 0, 4), (0, -1, 1), (0, 1, 2), (1, 0, 2), (0, -1, 2)), (-1, 0, 0), (0, 0, 0)),
    (((1, 0, 3), (2, 0, 0), (0, 1, 3), (0, -1, 4), (-1, 1, 1), (0, -1, 3), (0, 1, 4)), (0, 0, 1), (1, 0, 1)),
    (((-1, 0, 2), (1, 0, 1)), (0, 1, 0), (0, -1, 0)),
    (((2, 0, 1), (-1, 0, 3), (0, 2, 2), (-1, -1, 0), (-1, -1, 1), (-1, 1, 0), (1, 1, 0), (2, 0, 3)), (0, -1, 1), (1, 0, 0)),
    (((2, 0, 2),), (-1, 0, 1), (-1, 1, 0)),
    (((0, 2, 4), (1, -1, 2), (0, 2, 1), (0, 2, 0), (1, 0, 4)), (2, 0, 0), (-1, -1, 0)),
    (((-1, -1, 3), (-1, 1, 3), (1, 1, 3), (1, -1, 1), (-1, 1, 4), (-1, -1, 2), (-1, 1, 2), (1, 1, 4)), (2, 0, 1), (0, 2, 0)),
    ((W_NEAR, (-1, -1, 4), (0, 2, 3), (1, -1, 3), (1, 1, 2), (-1, 0, 4)), (-1, -1, 1), (-1, 1, 1)),
    (((2, -1, 0), (2, -1, 1), (1, 1, 1), (2, 1, 1)), (1, -1, 1), (0, 2, 1)),
    (((1, 2, 0), (-1, 2, 4), (2, 1, 2)), (1, 1, 0), (1, 1, 1)),
    (((-1, 2, 1), (2, -1, 2), (2, 1, 0), (2, 1, 3), (-1, 2, 0)), (2, -1, 0), (1, -1, 0)),
    ((), (2, 1, 1), (2, 1, 0)),
    (((-1, 2, 2), (1, 2, 1), (1, -1, 4), (2, 1, 4), (2, -1, 4), (2, -1, 3), (1, 2, 4), (2, 0, 4), (2, 2, 4), (1, 2, 3)), (0, 1, 1), (-1, 2, 0)),
    (((-1, 2, 3), RETENTION, (2, 2, 1), (1, 2, 2), (2, 2, 0)), (1, 2, 0), (2, -1, 1)),
    (((2, 2, 3), (2, 2, 2), W_FAR), (-1, 2, 1), (2, 2, 0)),
    ((), (1, 2, 1), (2, 2, 1)),
)
LAST = ()
PLUS_Y, MINUS_Y, PLUS_Z, MINUS_Z = range(4)
STEPS = ((0, 1), (0, -1), (1, 0), (-1, 0))
ALONG_Y_FIRST = (0, 3, 4)
ONWARD_BY_PLUS = (0, 1, 4)


def nt(a, b, precision=None):
    return lax.dot_general(
        a, b, (((1,), (1,)), ((), ())), preferred_element_type=F32, precision=precision
    )


def mm(a, b, precision=None):
    return jnp.dot(a, b, preferred_element_type=F32, precision=precision)


def head_norm(values, axis):
    return values * lax.rsqrt(jnp.mean(values * values, axis=axis, keepdims=True) + HEAD_EPS)


def routes(dz, dy, quarter):
    y_first = quarter in ALONG_Y_FIRST
    ways = ((PLUS_Y, MINUS_Y), (PLUS_Z, MINUS_Z))
    first, second = ways if y_first else ways[::-1]
    a, b = (dy, dz) if y_first else (dz, dy)
    by_plus = quarter in ONWARD_BY_PLUS
    if a == 0 and b == 0:
        return first + second
    line, at = (first, a) if b == 0 else (second, b)
    onward = ()
    if at == -1 and by_plus:
        onward = (line[0],)
    elif at == 1 and not by_plus:
        onward = (line[1],)
    return onward + (second if b == 0 else ())


def kernel(
    tokens, gain, wq1, wq2, wk1, wk2, wv, mix, hgain, wrq, wrk, wrv, logs, init, wod, wor,
    out,
    rows, weights, qt, qrecv, kv, states, retp, wout, qpad, acc, peak, denom, sbuf, pbuf, rgate, retq, retadd, retfade, osum,
    dsend, rsend, heads,
    load_sem, x_send, x_recv, w_send, w_recv, kv_send, kv_recv, pair_send, pair_recv,
    st_send, st_recv, st_pair_send, st_pair_recv, q_sem, o_send, o_recv, r_send, r_recv,
):
    sp = lax.axis_index("sp")
    t = lax.axis_index("tp")
    z, y, c = lax.div(sp, 8), lax.rem(lax.div(sp, 2), 4), lax.rem(sp, 2)
    partner = 31 - sp
    sib = (sp + 1 - 2 * c, t)
    left, right, far = lax.rem(t + 3, 4), lax.rem(t + 1, 4), lax.rem(t + 2, 4)

    def chip(dz, dy):
        return lax.rem(z + dz + 4, 4) * 4 + lax.rem(y + dy + 4, 4)

    near = [(chip(dz, dy) * 2 + c, t) for dz, dy in STEPS]

    loads = []
    sources = (
        (wk1, 256, 128), (wk2, 384, 128), (wv, 512, 256), (wq1, 0, 128), (wq2, 128, 128),
        (wrq, 768, 128), (wrk, 896, 128), (wrv, 1024, 256),
    )
    for k, (ref, at, width) in enumerate(sources):
        group = load_sem.at[0 if k < 3 else 1]
        loads.append(pltpu.make_async_copy(ref, weights.at[:, pl.ds(at, width)], group))
    for k, ref in enumerate((wod, wor)):
        loads.append(pltpu.make_async_copy(ref, wout.at[t, k], load_sem.at[2]))
    for load in loads:
        load.start()

    def drain(piece, sem):
        pltpu.make_async_copy(piece, piece, sem).wait()

    barrier = pltpu.get_barrier_semaphore()
    peers = [(sp, left), (sp, right), (sp, far), sib, *near] + [(partner, d) for d in range(4)]
    for peer in peers:
        pl.semaphore_signal(barrier, inc=1, device_id=peer, device_id_type=MESH)

    for chunk in range(2):
        floats = tokens[chunk * 64 : chunk * 64 + 64].astype(F32)
        scale = lax.rsqrt(jnp.mean(floats * floats, axis=-1, keepdims=True) + NORM_EPS)
        rows[t, chunk * 64 : chunk * 64 + 64] = (floats * scale * gain[...]).astype(BF16)
    lg = logs[...]

    pl.semaphore_wait(barrier, len(peers))

    def remote(src, dst, ssem, rsem, dev):
        return pltpu.make_async_remote_copy(
            src_ref=src, dst_ref=dst, send_sem=ssem, recv_sem=rsem, device_id=dev,
            device_id_type=MESH,
        )

    def x_copy(slot, chunk, to, n):
        piece = rows.at[slot, pl.ds(chunk * 64, 64)]
        return remote(piece, piece, x_send, x_recv.at[n // 2], (sp, to))

    def w_copy(slot, part, to, n):
        piece = wout.at[slot, c] if part is None else wout.at[slot, c, pl.ds(part * 128, 128)]
        rsem = w_recv.at[0 if part is None else 1]
        return remote(piece, piece, w_send, rsem, (sp, to))

    def w_sib(slot, n, kind):
        piece = wout.at[slot, kind]
        return remote(piece, piece, w_send, w_recv.at[2], sib)

    def kv_copy(j, q, way, n, dev):
        return remote(kv.at[j, q], kv.at[j, q], kv_send.at[way], kv_recv.at[lax.div(j, 2), q], dev)

    def st_copy(j, way, n, dev):
        return remote(states.at[j], states.at[j], st_send.at[way], st_recv.at[lax.div(j, 2)], dev)

    def pair_copy(j, pair, n):
        piece = kv.at[j, pl.ds(2 * pair, 2)]
        return remote(piece, piece, pair_send, pair_recv.at[lax.div(j, 2), pair], sib)

    def st_pair_copy(j, n):
        return remote(states.at[j], states.at[j], st_pair_send, st_pair_recv, sib)

    kv_used, st_used, pairs_used, st_pairs_used = [0] * 4, [0] * 4, [], []

    def pass_on(dz, dy, q):
        j = chip(dz, dy) * 2 + c
        for way in routes(dz, dy, q):
            kv_copy(j, q, way, kv_used[way], near[way]).start()
            kv_used[way] += 1

    def pass_state_on(dz, dy):
        j = chip(dz, dy) * 2 + c
        for way in routes(dz, dy, 4):
            st_copy(j, way, st_used[way], near[way]).start()
            st_used[way] += 1
        st_pair_copy(j, len(st_pairs_used)).start()
        st_pairs_used.append((dz, dy))

    arrived = set()

    def pair_to_sib(dz, dy, q):
        arrived.add((dz, dy, q))
        if (dz, dy, q ^ 1) in arrived:
            pair_copy(chip(dz, dy) * 2 + c, q // 2, len(pairs_used)).start()
            pairs_used.append((dz, dy, q // 2))

    def arrival(dz, dy, q):
        j = chip(dz, dy) * 2 + c
        if q == 4:
            st_copy(j, 0, 0, sib).wait_recv()
            pass_state_on(dz, dy)
        else:
            kv_copy(j, q, 0, 0, sib).wait_recv()
            pass_on(dz, dy, q)
            pair_to_sib(dz, dy, q)

    x_copy(t, 0, right, 0).start()
    x_copy(t, 1, left, 1).start()
    x_copy(t, 1, right, 2).start()
    x_copy(t, 0, left, 3).start()

    def times(lhs, n):
        return mm(lhs, weights[:, n * 256 : n * 256 + 256])

    spots = (
        ((0, t * 128, 128),),
        ((0, left * 128, 64), (64, right * 128 + 64, 64)),
        ((0, left * 128 + 64, 64), (64, right * 128, 64)),
        ((0, far * 128, 128),),
    )

    def own_quarter(q):
        if q == 0:
            drain(weights.at[:, pl.ds(256, 512)], load_sem.at[0])
            lhs = rows[t]
        elif q == 1:
            drain(rows.at[0], x_recv.at[0])
            x_copy(left, 0, right, 4).start()
            x_copy(right, 1, left, 5).start()
            lhs = jnp.concatenate([rows[left, 0:64], rows[right, 64:128]], axis=0)
        elif q == 2:
            drain(rows.at[0], x_recv.at[1])
            lhs = jnp.concatenate([rows[left, 64:128], rows[right, 0:64]], axis=0)
        else:
            drain(rows.at[0], x_recv.at[2])
            lhs = rows[far]
        kv[sp, q, 0:128] = times(lhs, 1).astype(BF16)
        turned = times(lhs, 2).T.astype(BF16)
        kv[sp, q, 128:256] = jnp.concatenate([turned[0:128], turned[128:256]], axis=1)
        pass_on(0, 0, q)
        pair_to_sib(0, 0, q)
        if q == 0:
            drain(weights.at[:, pl.ds(0, 768)], load_sem.at[1])
        at = q % 2 * 128
        qt[q // 2, :, at : at + 128] = times(lhs, 0).T.astype(BF16)
        for n in range(2):
            block = times(lhs, 3 + n).astype(BF16)
            for here, there, count in spots[q]:
                retp[n, pl.ds(pl.multiple_of(there, 64), count)] = block[here : here + count]
        if q == 1:
            q_copy.start()
            drain(wout.at[t], load_sem.at[2])
            w_copy(t, None, right, 0).start()
            w_copy(t, None, left, 1).start()

    q_copy = remote(qt.at[0], qrecv, q_sem.at[0], q_sem.at[1], (partner, t))
    row = lax.broadcasted_iota(jnp.int32, (256, 256), 0)
    col = lax.broadcasted_iota(jnp.int32, (256, 256), 1)
    lane = lax.broadcasted_iota(jnp.int32, (256, 128), 1)

    for event in SCHEDULE[0][0]:
        if event == (0, 0, 4):
            retention_inside(lg, retp, rgate, retq, retadd, retfade, states, sp, row, col, lane)
            pass_state_on(0, 0)
        elif event[:2] == (0, 0):
            own_quarter(event[2])
        else:
            arrival(*event)

    def queries_of(half, block):
        big = block.astype(F32) * 0.125
        for hm in range(4):
            qpad[half, hm] = jnp.where(lax.div(row, 64) == hm, big, 0.0).astype(BF16)

    queries_of(0, qt[1])
    for half in range(2):
        for hm in range(4):
            peak[half, hm] = jnp.full((1, 256), LOWEST, F32)
            denom[half, hm] = jnp.zeros((1, 256), F32)
            acc[half, hm] = jnp.zeros((128, 256), F32)
    q_copy.wait_recv()
    queries_of(1, qrecv[...])

    def position(index, pair):
        early = jnp.where(
            index < 128, t * 128 + index,
            jnp.where(index < 192, left * 128 + index - 128, right * 128 + index - 128),
        )
        late = jnp.where(
            index < 64, left * 128 + 64 + index,
            jnp.where(index < 128, right * 128 + index - 64, far * 128 + index - 128),
        )
        return jnp.where(pair == 0, early, late)

    def attend(half, units, bound=None):
        def keys(near_chip, pair, l):
            return jnp.concatenate([kv[near_chip * 2 + l, 2 * pair + p, 0:128] for p in range(2)], axis=0)

        def values(near_chip, pair, l, h):
            cut = slice(h * 128, h * 128 + 128)
            return jnp.concatenate(
                [kv[near_chip * 2 + l, 2 * pair + p, 128:256, cut] for p in range(2)], axis=1
            )

        chains = [(n * 4 + hm, hm, *unit) for n, unit in enumerate(units) for hm in range(4)]
        for at, hm, near_chip, pair in chains:
            if bound is not None and hm == 0:
                late = position(col, 1 - half) - position(row, pair) + (bound - near_chip * 2) * 512
            for l in range(2):
                scores = mm(keys(near_chip, pair, l), qpad[half, hm])
                if bound is not None:
                    scores = jnp.where(late >= l * 512, scores, -jnp.inf)
                sbuf[at, l] = scores
        fades = []
        for at, hm, _, _ in chains:
            old = peak[half, hm]
            new = jnp.maximum(
                old, jnp.max(jnp.maximum(sbuf[at, 0], sbuf[at, 1]), axis=0, keepdims=True)
            )
            fade = jnp.exp(old - new)
            total = denom[half, hm] * fade
            for l in range(2):
                term = jnp.exp(sbuf[at, l] - new)
                total = total + jnp.sum(term, axis=0, keepdims=True)
                pbuf[at, l] = term.astype(BF16)
            denom[half, hm] = total
            peak[half, hm] = new
            fades.append(fade)
        for at, hm, near_chip, pair in chains:
            acc[half, hm] = acc[half, hm] * fades[at] + sum(
                mm(values(near_chip, pair, l, hm % 2), pbuf[at, l]) for l in range(2)
            )

    def w_stage(stage):
        if stage == W_NEAR:
            drain(wout.at[0], w_recv.at[0])
            w_copy(left, 0, right, 2).start()
            w_copy(right, 1, left, 3).start()
            w_sib(left, 0, c).start()
            w_sib(right, 1, c).start()
        else:
            drain(wout.at[0, 0], w_recv.at[1])
            w_sib(far, 2, c).start()

    others = (left, right, far)

    def r_copy(slot, n):
        piece = rsend.at[pl.ds(pl.multiple_of(slot * 128, 128), 128)]
        return remote(piece, heads.at[1, t], r_send, r_recv, (sp, slot))

    def chain(j, state):
        own = states[j].astype(F32)
        return state * jnp.exp(own[64:65] + own[65:66] + own[66:67]) + own[0:64]

    def retention_end():
        drain(states.at[pl.ds(0, 16)], st_pair_recv)
        state = lax.fori_loop(0, sp, chain, jnp.concatenate([init[0], init[1]], axis=1))
        state = jnp.concatenate([state[:, 0:128], state[:, 128:256]], axis=0)
        for b in range(2):
            for h in range(2):
                mine = (lane < 64) if h == 0 else (lane >= 64)
                older = mm(jnp.where(mine, retq[b], 0.0), state, HIGHEST)
                r = rgate[b, h] + older
                rsend[b * 256 : b * 256 + 256, h * 128 : h * 128 + 128] = head_norm(r, 1).astype(BF16)
            state = retfade[b] * state + retadd[b]
        for n, slot in enumerate(others):
            r_copy(slot, n).start()
        heads[1, t] = rsend[pl.ds(pl.multiple_of(t * 128, 128), 128)]

    codes = [
        sum(((dz + 1) * 8 + (dy + 1) * 2 + pair) * scale for scale, (dz, dy, pair) in zip((1, 32), units))
        for _, *units in SCHEDULE
    ]

    def happen(events):
        for event in events:
            if event == RETENTION:
                retention_end()
            elif event in (W_NEAR, W_FAR):
                w_stage(event)
            else:
                arrival(*event)

    def handled(s, low, high):
        if high - low > 1:
            middle = (low + high) // 2
            return lax.cond(
                s < middle, lambda: handled(s, low, middle), lambda: handled(s, middle, high)
            )
        if low > 0:
            happen(SCHEDULE[low][0])
        return jnp.int32(codes[low])

    def tick(s, carry):
        code = handled(s, 0, len(SCHEDULE))
        units = []
        for part in (lax.rem(code, 32), lax.div(code, 32)):
            near_chip = chip(lax.div(part, 8) - 1, lax.rem(lax.div(part, 2), 4) - 1)
            pair = lax.rem(part, 2)
            pair_copy(near_chip * 2 + 1 - c, pair, 0).wait_recv()
            units.append((near_chip, pair))
        (chip_a, pair_a), (chip_b, pair_b) = units

        def one_half(half, carry):
            bound = jnp.where(half == 0, sp, partner)
            last = lax.div(bound, 2)
            early_a, early_b = chip_a < last, chip_b < last

            @pl.when(jnp.logical_and(early_a, early_b))
            def _():
                attend(half, units)

            @pl.when(jnp.logical_xor(early_a, early_b))
            def _():
                attend(half, [(jnp.where(early_a, chip_a, chip_b), jnp.where(early_a, pair_a, pair_b))])

            def one_edge(n, carry):
                near_chip = jnp.where(n == 0, chip_a, chip_b)

                @pl.when(near_chip == last)
                def _():
                    attend(half, [(near_chip, jnp.where(n == 0, pair_a, pair_b))], bound)

                return carry

            @pl.when(jnp.logical_or(chip_a == last, chip_b == last))
            def _():
                lax.fori_loop(0, 2, one_edge, 0)

            return carry

        return lax.fori_loop(0, 2, one_half, carry)

    lax.fori_loop(0, len(SCHEDULE), tick, 0)
    happen(LAST)
    assert kv_used == [15] * 4 and len(pairs_used) == 32 and len(st_pairs_used) == 16

    def o_copy(src, at, count, dev, n, sem):
        place = heads.at[0, t, pl.ds(at, count)]
        return remote(src, place, o_send, o_recv, dev)

    def finish(half):
        sides = []
        for h in range(2):
            weight_two = mix[:, h : h + 1]
            first = acc[half, h] / denom[half, h]
            second = acc[half, 2 + h] / denom[half, 2 + h]
            attn = first - weight_two * second
            sides.append((head_norm(attn, 0) * DIFF_SCALE).T * hgain[...])
        dsend[half] = jnp.concatenate(sides, axis=1).astype(BF16)

    def o_copies(half):
        if half == 0:
            return [
                o_copy(dsend.at[0, pl.ds(0, 64)], 64, 64, (sp, left), 0, 1),
                o_copy(dsend.at[0, pl.ds(64, 64)], 0, 64, (sp, right), 1, 0),
                o_copy(dsend.at[0, pl.ds(128, 128)], 0, 128, (sp, far), 2, 0),
            ]
        return [
            o_copy(dsend.at[1, pl.ds(0, 128)], 0, 128, (partner, t), 3, 0),
            o_copy(dsend.at[1, pl.ds(128, 64)], 0, 64, (partner, left), 4, 0),
            o_copy(dsend.at[1, pl.ds(192, 64)], 64, 64, (partner, right), 5, 1),
        ]

    for half in range(2):
        finish(half)
        for copy in o_copies(half):
            copy.start()

    def product(kind, last):
        def columns(n, carry):
            at = pl.ds(pl.multiple_of(n * 512, 512), 512)
            block = osum[:, at] if last else jnp.zeros((128, 512), F32)
            for slot in range(4):
                block += mm(heads[kind, slot], wout[slot, kind, :, at])
            if last:
                out[:, at] = block.astype(BF16)
            else:
                osum[:, at] = block
            return carry

        lax.fori_loop(0, 4, columns, 0)

    drain(wout.at[pl.ds(0, 3), 0], w_recv.at[2])
    drain(rsend.at[pl.ds(0, 384)], r_recv)
    product(1, False)

    drain(dsend, o_recv)
    product(0, True)

    drain(rows.at[pl.ds(0, 3)], x_send)
    drain(wout.at[pl.ds(0, 3)], w_send)
    drain(rsend.at[pl.ds(0, 384)], r_send)
    drain(dsend, o_send)
    q_copy.wait_send()
    for way in range(4):
        drain(kv.at[pl.ds(0, kv_used[way]), 0], kv_send.at[way])
        drain(states.at[pl.ds(0, st_used[way])], st_send.at[way])
    drain(kv.at[:, pl.ds(0, 2)], pair_send)
    drain(states.at[pl.ds(0, 16)], st_pair_send)


def retention_inside(lg, retp, rgate, retq, retadd, retfade, states, sp, row, col, lane):
    state_row = lax.broadcasted_iota(jnp.int32, (128, 128), 0)
    upper = jnp.where(row <= col, 1.0, 0.0)
    adds, fades, lasts_of = [], [], []
    for b in range(2):
        span = slice(b * 256, b * 256 + 256)
        lb = lg[:, span]
        cum_rows = mm(jnp.concatenate([lb, lb, lb, lb], axis=0), upper, HIGHEST)
        rq, rk = retp[0, span, 0:128], retp[0, span, 128:256]
        cols, lasts = [], []
        for h in range(2):
            cum_col = jnp.sum(jnp.where(col <= row, lb[h : h + 1], 0.0), axis=1, keepdims=True)
            cols.append(cum_col)
            lasts.append(jnp.sum(lb[h : h + 1], axis=1, keepdims=True))
            mine = (lane < 64) if h == 0 else (lane >= 64)
            raw = nt(jnp.where(mine, rq, jnp.zeros_like(rq)), rk)
            gap = jnp.where(col <= row, cum_col - cum_rows[h : h + 1], -jnp.inf)
            gate = (raw * 0.125 * jnp.exp(gap)).astype(BF16)
            rgate[b, h] = mm(gate, retp[1, span, h * 128 : h * 128 + 128])
        factor = jnp.where(lane < 64, jnp.exp(lasts[0] - cols[0]), jnp.exp(lasts[1] - cols[1]))
        keys = (rk.astype(F32) * 0.125 * factor).T.astype(BF16)
        both = mm(keys, retp[1, span])
        adds.append(jnp.where(state_row < 64, both[:, 0:128], both[:, 128:256]))
        fades.append(jnp.where(state_row < 64, jnp.exp(lasts[0]), jnp.exp(lasts[1])))
        grow = jnp.where(lane < 64, jnp.exp(cols[0]), jnp.exp(cols[1]))
        retq[b] = rq.astype(F32) * grow
        retadd[b] = adds[b]
        retfade[b] = fades[b]
        lasts_of.append(lasts)
    own = fades[1] * adds[0] + adds[1]
    states[sp, 0:64] = jnp.concatenate([own[0:64], own[64:128]], axis=1).astype(BF16)
    tile_lane = lax.broadcasted_iota(jnp.int32, (16, 256), 1)
    tile_row = lax.broadcasted_iota(jnp.int32, (16, 256), 0)
    total = jnp.where(
        tile_lane < 128, lasts_of[0][0] + lasts_of[1][0], lasts_of[0][1] + lasts_of[1][1]
    )
    high = total.astype(BF16).astype(F32)
    middle = (total - high).astype(BF16).astype(F32)
    low = total - high - middle
    tile = jnp.where(tile_row == 0, high, jnp.where(tile_row == 1, middle, low))
    states[sp, 64:80] = tile.astype(BF16)


def on_device(
    tokens, norm_gain, w_query_one, w_query_two, w_key_one, w_key_two, w_value, mix_lambda,
    head_gain, w_ret_query, w_ret_key, w_ret_value, retain_log, init_state, w_out_diff, w_out_ret,
):
    vmem = pl.BlockSpec(memory_space=pltpu.VMEM)
    hbm = pl.BlockSpec(memory_space=pl.ANY)
    dma = pltpu.SemaphoreType.DMA
    return pl.pallas_call(
        kernel,
        out_shape=jax.ShapeDtypeStruct((128, 2048), BF16),
        in_specs=[vmem, vmem] + [hbm] * 5 + [vmem, vmem] + [hbm] * 3 + [vmem, vmem] + [hbm] * 2,
        out_specs=vmem,
        scratch_shapes=[
            pltpu.VMEM((4, 128, 2048), BF16),
            pltpu.VMEM((2048, 1280), BF16),
            pltpu.VMEM((2, 256, 256), BF16),
            pltpu.VMEM((256, 256), BF16),
            pltpu.VMEM((32, 4, 256, 256), BF16),
            pltpu.VMEM((32, 80, 256), BF16),
            pltpu.VMEM((2, 512, 256), BF16),
            pltpu.VMEM((4, 2, 256, 2048), BF16),
            pltpu.VMEM((2, 4, 256, 256), BF16),
            pltpu.VMEM((2, 4, 128, 256), F32),
            pltpu.VMEM((2, 4, 1, 256), F32),
            pltpu.VMEM((2, 4, 1, 256), F32),
            pltpu.VMEM((8, 2, 256, 256), F32),
            pltpu.VMEM((8, 2, 256, 256), BF16),
            pltpu.VMEM((2, 2, 256, 128), F32),
            pltpu.VMEM((2, 256, 128), F32),
            pltpu.VMEM((2, 128, 128), F32),
            pltpu.VMEM((2, 128, 128), F32),
            pltpu.VMEM((128, 2048), F32),
            pltpu.VMEM((2, 256, 256), BF16),
            pltpu.VMEM((512, 256), BF16),
            pltpu.VMEM((2, 4, 128, 256), BF16),
            dma((3,)),
            dma,
            dma((3,)),
            dma,
            dma((3,)),
            dma((4,)),
            dma((16, 4)),
            dma,
            dma((16, 2)),
            dma((4,)),
            dma((16,)),
            dma,
            dma,
            dma((2,)),
            dma,
            dma,
            dma,
            dma,
        ],
        compiler_params=pltpu.CompilerParams(
            collective_id=0, has_side_effects=True, vmem_limit_bytes=53 * 1024 * 1024,
        ),
        cost_estimate=pl.CostEstimate(
            flops=20_000_000_000, bytes_accessed=10_000_000, transcendentals=17_000_000
        ),
        name="layer",
    )(
        tokens, norm_gain.reshape(1, -1), w_query_one, w_query_two, w_key_one, w_key_two, w_value,
        mix_lambda.reshape(1, -1), head_gain.reshape(1, -1),
        w_ret_query, w_ret_key, w_ret_value, retain_log, init_state, w_out_diff, w_out_ret,
    )


def solution(mesh):
    both = ("sp", "tp")
    return jax.shard_map(
        on_device,
        mesh=mesh,
        in_specs=(
            P(both, None), P(), P(None, "tp"), P(None, "tp"), P(None, "tp"), P(None, "tp"),
            P(None, "tp"), P("tp"), P(), P(None, "tp"), P(None, "tp"), P(None, "tp"),
            P("tp", "sp"), P("tp", None, None), P("tp", None), P("tp", None),
        ),
        out_specs=P(both, None),
        check_vma=False,
    )
```

```python
import jax
import jax.numpy as jnp
from jax import lax
from jax.experimental import pallas as pl
from jax.experimental.pallas import tpu as pltpu
from jax.sharding import PartitionSpec as P

NORM_EPS = 1e-06
HEAD_EPS = 1e-05
DIFF_SCALE = 0.8
MESH = pl.DeviceIdType.MESH
F32 = jnp.float32
BF16 = jnp.bfloat16
HIGHEST = lax.Precision.HIGHEST
LOWEST = -3.0e38


W_NEAR, W_FAR, RETENTION = range(3)
SCHEDULE = (
    (((0, 0, 0), (0, -1, 0), (0, 0, 1), (-1, 0, 0), (0, 1, 0), (0, 0, 2), (1, -1, 0), (-1, 0, 1), (0, 1, 1), (0, 0, 3), (1, 0, 0), (0, 0, 4), (0, -1, 1), (0, 1, 2), (1, 0, 2), (0, -1, 2)), (-1, 0, 0), (0, 0, 0)),
    (((1, 0, 3), (2, 0, 0), (0, 1, 3), (0, -1, 4), (-1, 1, 1), (0, -1, 3), (0, 1, 4)), (0, 0, 1), (1, 0, 1)),
    (((-1, 0, 2), (1, 0, 1)), (0, 1, 0), (0, -1, 0)),
    (((2, 0, 1), (-1, 0, 3), (0, 2, 2), (-1, -1, 0), (-1, -1, 1), (-1, 1, 0), (1, 1, 0), (2, 0, 3)), (0, -1, 1), (1, 0, 0)),
    (((2, 0, 2),), (-1, 0, 1), (-1, 1, 0)),
    (((0, 2, 4), (1, -1, 2), (0, 2, 1), (0, 2, 0), (1, 0, 4)), (2, 0, 0), (-1, -1, 0)),
    (((-1, -1, 3), (-1, 1, 3), (1, 1, 3), (1, -1, 1), (-1, 1, 4), (-1, -1, 2), (-1, 1, 2), (1, 1, 4)), (2, 0, 1), (0, 2, 0)),
    ((W_NEAR, (-1, -1, 4), (0, 2, 3), (1, -1, 3), (1, 1, 2), (-1, 0, 4)), (-1, -1, 1), (-1, 1, 1)),
    (((2, -1, 0), (2, -1, 1), (1, 1, 1), (2, 1, 1)), (1, -1, 1), (0, 2, 1)),
    (((1, 2, 0), (-1, 2, 4), (2, 1, 2)), (1, 1, 0), (1, 1, 1)),
    (((-1, 2, 1), (2, -1, 2), (2, 1, 0), (2, 1, 3), (-1, 2, 0)), (2, -1, 0), (1, -1, 0)),
    ((), (2, 1, 1), (2, 1, 0)),
    (((-1, 2, 2), (1, 2, 1), (1, -1, 4), (2, 1, 4), (2, -1, 4), (2, -1, 3), (1, 2, 4), (2, 0, 4), (2, 2, 4), (1, 2, 3)), (0, 1, 1), (-1, 2, 0)),
    (((-1, 2, 3), RETENTION, (2, 2, 1), (1, 2, 2), (2, 2, 0)), (1, 2, 0), (2, -1, 1)),
    (((2, 2, 3), (2, 2, 2), W_FAR), (-1, 2, 1), (2, 2, 0)),
    ((), (1, 2, 1), (2, 2, 1)),
)
LAST = ()
PLUS_Y, MINUS_Y, PLUS_Z, MINUS_Z = range(4)
STEPS = ((0, 1), (0, -1), (1, 0), (-1, 0))
ALONG_Y_FIRST = (0, 3, 4)
ONWARD_BY_PLUS = (0, 1, 4)


def nt(a, b, precision=None):
    return lax.dot_general(
        a, b, (((1,), (1,)), ((), ())), preferred_element_type=F32, precision=precision
    )


def mm(a, b, precision=None):
    return jnp.dot(a, b, preferred_element_type=F32, precision=precision)


def head_norm(values, axis):
    return values * lax.rsqrt(jnp.mean(values * values, axis=axis, keepdims=True) + HEAD_EPS)


def routes(dz, dy, quarter):
    y_first = quarter in ALONG_Y_FIRST
    ways = ((PLUS_Y, MINUS_Y), (PLUS_Z, MINUS_Z))
    first, second = ways if y_first else ways[::-1]
    a, b = (dy, dz) if y_first else (dz, dy)
    by_plus = quarter in ONWARD_BY_PLUS
    if a == 0 and b == 0:
        return first + second
    line, at = (first, a) if b == 0 else (second, b)
    onward = ()
    if at == -1 and by_plus:
        onward = (line[0],)
    elif at == 1 and not by_plus:
        onward = (line[1],)
    return onward + (second if b == 0 else ())


def kernel(
    tokens_in, gain_in, wq1, wq2, wk1, wk2, wv, mix_in, hgain_in, wrq, wrk, wrv, logs_in, init_in, wod, wor,
    out,
    tokens, gain, mix, hgain, logs, init, rows, weights, qt, qrecv, kv, states, retp, wout, qpad, acc, peak, denom, sbuf, pbuf, rgate, retq, retadd, retfade, osum,
    dsend, rsend, heads,
    load_sem, x_send, x_recv, w_send, w_recv, kv_send, kv_recv, pair_send, pair_recv,
    st_send, st_recv, st_pair_send, st_pair_recv, q_sem, o_send, o_recv, r_send, r_recv,
):
    sp = lax.axis_index("sp")
    t = lax.axis_index("tp")
    z, y, c = lax.div(sp, 8), lax.rem(lax.div(sp, 2), 4), lax.rem(sp, 2)
    partner = 31 - sp
    sib = (sp + 1 - 2 * c, t)
    left, right, far = lax.rem(t + 3, 4), lax.rem(t + 1, 4), lax.rem(t + 2, 4)

    def chip(dz, dy):
        return lax.rem(z + dz + 4, 4) * 4 + lax.rem(y + dy + 4, 4)

    near = [(chip(dz, dy) * 2 + c, t) for dz, dy in STEPS]

    small = [
        pltpu.make_async_copy(source, held, load_sem.at[3 + k])
        for k, (source, held) in enumerate((
            (tokens_in, tokens), (gain_in, gain), (logs_in, logs),
            (mix_in, mix), (hgain_in, hgain), (init_in, init),
        ))
    ]
    for load in small:
        load.start()
    loads = []
    sources = (
        (wk1, 256, 128), (wk2, 384, 128), (wv, 512, 256), (wq1, 0, 128), (wq2, 128, 128),
        (wrq, 768, 128), (wrk, 896, 128), (wrv, 1024, 256),
    )
    for k, (ref, at, width) in enumerate(sources):
        group = load_sem.at[0 if k < 3 else 1]
        loads.append(pltpu.make_async_copy(ref, weights.at[:, pl.ds(at, width)], group))
    for k, ref in enumerate((wod, wor)):
        loads.append(pltpu.make_async_copy(ref, wout.at[t, k], load_sem.at[2]))
    def drain(piece, sem):
        pltpu.make_async_copy(piece, piece, sem).wait()

    barrier = pltpu.get_barrier_semaphore()
    peers = [(sp, left), (sp, right), (sp, far), sib, *near] + [(partner, d) for d in range(4)]
    for peer in peers:
        pl.semaphore_signal(barrier, inc=1, device_id=peer, device_id_type=MESH)

    for load in loads:
        load.start()
    for load in small[:2]:
        load.wait()
    for chunk in range(2):
        floats = tokens[chunk * 64 : chunk * 64 + 64].astype(F32)
        scale = lax.rsqrt(jnp.mean(floats * floats, axis=-1, keepdims=True) + NORM_EPS)
        rows[t, chunk * 64 : chunk * 64 + 64] = (floats * scale * gain[...]).astype(BF16)
    for load in small[2:]:
        load.wait()
    lg = logs[...]

    pl.semaphore_wait(barrier, len(peers))

    def remote(src, dst, ssem, rsem, dev):
        return pltpu.make_async_remote_copy(
            src_ref=src, dst_ref=dst, send_sem=ssem, recv_sem=rsem, device_id=dev,
            device_id_type=MESH,
        )

    def x_copy(slot, chunk, to, n):
        piece = rows.at[slot, pl.ds(chunk * 64, 64)]
        return remote(piece, piece, x_send, x_recv.at[n // 2], (sp, to))

    def w_copy(slot, part, to, n):
        piece = wout.at[slot, c] if part is None else wout.at[slot, c, pl.ds(part * 128, 128)]
        rsem = w_recv.at[0 if part is None else 1]
        return remote(piece, piece, w_send, rsem, (sp, to))

    def w_sib(slot, n, kind):
        piece = wout.at[slot, kind]
        return remote(piece, piece, w_send, w_recv.at[2], sib)

    def kv_copy(j, q, way, n, dev):
        return remote(kv.at[j, q], kv.at[j, q], kv_send.at[way], kv_recv.at[lax.div(j, 2), q], dev)

    def st_copy(j, way, n, dev):
        return remote(states.at[j], states.at[j], st_send.at[way], st_recv.at[lax.div(j, 2)], dev)

    def pair_copy(j, pair, n):
        piece = kv.at[j, pl.ds(2 * pair, 2)]
        return remote(piece, piece, pair_send, pair_recv.at[lax.div(j, 2), pair], sib)

    def st_pair_copy(j, n):
        return remote(states.at[j], states.at[j], st_pair_send, st_pair_recv, sib)

    kv_used, st_used, pairs_used, st_pairs_used = [0] * 4, [0] * 4, [], []

    def pass_on(dz, dy, q):
        j = chip(dz, dy) * 2 + c
        for way in routes(dz, dy, q):
            kv_copy(j, q, way, kv_used[way], near[way]).start()
            kv_used[way] += 1

    def pass_state_on(dz, dy):
        j = chip(dz, dy) * 2 + c
        for way in routes(dz, dy, 4):
            st_copy(j, way, st_used[way], near[way]).start()
            st_used[way] += 1
        st_pair_copy(j, len(st_pairs_used)).start()
        st_pairs_used.append((dz, dy))

    arrived = set()

    def pair_to_sib(dz, dy, q):
        arrived.add((dz, dy, q))
        if (dz, dy, q ^ 1) in arrived:
            pair_copy(chip(dz, dy) * 2 + c, q // 2, len(pairs_used)).start()
            pairs_used.append((dz, dy, q // 2))

    def arrival(dz, dy, q):
        j = chip(dz, dy) * 2 + c
        if q == 4:
            st_copy(j, 0, 0, sib).wait_recv()
            pass_state_on(dz, dy)
        else:
            kv_copy(j, q, 0, 0, sib).wait_recv()
            pass_on(dz, dy, q)
            pair_to_sib(dz, dy, q)

    x_copy(t, 0, right, 0).start()
    x_copy(t, 1, left, 1).start()
    x_copy(t, 1, right, 2).start()
    x_copy(t, 0, left, 3).start()

    def times(lhs, n):
        return mm(lhs, weights[:, n * 256 : n * 256 + 256])

    spots = (
        ((0, t * 128, 128),),
        ((0, left * 128, 64), (64, right * 128 + 64, 64)),
        ((0, left * 128 + 64, 64), (64, right * 128, 64)),
        ((0, far * 128, 128),),
    )

    def own_quarter(q):
        if q == 0:
            drain(weights.at[:, pl.ds(256, 512)], load_sem.at[0])
            lhs = rows[t]
        elif q == 1:
            drain(rows.at[0], x_recv.at[0])
            x_copy(left, 0, right, 4).start()
            x_copy(right, 1, left, 5).start()
            lhs = jnp.concatenate([rows[left, 0:64], rows[right, 64:128]], axis=0)
        elif q == 2:
            drain(rows.at[0], x_recv.at[1])
            lhs = jnp.concatenate([rows[left, 64:128], rows[right, 0:64]], axis=0)
        else:
            drain(rows.at[0], x_recv.at[2])
            lhs = rows[far]
        kv[sp, q, 0:128] = times(lhs, 1).astype(BF16)
        turned = times(lhs, 2).T.astype(BF16)
        kv[sp, q, 128:256] = jnp.concatenate([turned[0:128], turned[128:256]], axis=1)
        pass_on(0, 0, q)
        pair_to_sib(0, 0, q)
        if q == 0:
            drain(weights.at[:, pl.ds(0, 768)], load_sem.at[1])
        at = q % 2 * 128
        qt[q // 2, :, at : at + 128] = times(lhs, 0).T.astype(BF16)
        for n in range(2):
            block = times(lhs, 3 + n).astype(BF16)
            for here, there, count in spots[q]:
                retp[n, pl.ds(pl.multiple_of(there, 64), count)] = block[here : here + count]
        if q == 1:
            q_copy.start()
            drain(wout.at[t], load_sem.at[2])
            w_copy(t, None, right, 0).start()
            w_copy(t, None, left, 1).start()

    q_copy = remote(qt.at[0], qrecv, q_sem.at[0], q_sem.at[1], (partner, t))
    row = lax.broadcasted_iota(jnp.int32, (256, 256), 0)
    col = lax.broadcasted_iota(jnp.int32, (256, 256), 1)
    lane = lax.broadcasted_iota(jnp.int32, (256, 128), 1)

    for event in SCHEDULE[0][0]:
        if event == (0, 0, 4):
            retention_inside(lg, retp, rgate, retq, retadd, retfade, states, sp, row, col, lane)
            pass_state_on(0, 0)
        elif event[:2] == (0, 0):
            own_quarter(event[2])
        else:
            arrival(*event)

    def queries_of(half, block):
        big = block.astype(F32) * 0.125
        for hm in range(4):
            qpad[half, hm] = jnp.where(lax.div(row, 64) == hm, big, 0.0).astype(BF16)

    queries_of(0, qt[1])
    for half in range(2):
        for hm in range(4):
            peak[half, hm] = jnp.full((1, 256), LOWEST, F32)
            denom[half, hm] = jnp.zeros((1, 256), F32)
            acc[half, hm] = jnp.zeros((128, 256), F32)
    q_copy.wait_recv()
    queries_of(1, qrecv[...])

    def position(index, pair):
        early = jnp.where(
            index < 128, t * 128 + index,
            jnp.where(index < 192, left * 128 + index - 128, right * 128 + index - 128),
        )
        late = jnp.where(
            index < 64, left * 128 + 64 + index,
            jnp.where(index < 128, right * 128 + index - 64, far * 128 + index - 128),
        )
        return jnp.where(pair == 0, early, late)

    def attend(half, units, bound=None):
        def keys(near_chip, pair, l):
            return jnp.concatenate([kv[near_chip * 2 + l, 2 * pair + p, 0:128] for p in range(2)], axis=0)

        def values(near_chip, pair, l, h):
            cut = slice(h * 128, h * 128 + 128)
            return jnp.concatenate(
                [kv[near_chip * 2 + l, 2 * pair + p, 128:256, cut] for p in range(2)], axis=1
            )

        chains = [(n * 4 + hm, hm, *unit) for n, unit in enumerate(units) for hm in range(4)]
        for at, hm, near_chip, pair in chains:
            if bound is not None and hm == 0:
                late = position(col, 1 - half) - position(row, pair) + (bound - near_chip * 2) * 512
            for l in range(2):
                scores = mm(keys(near_chip, pair, l), qpad[half, hm])
                if bound is not None:
                    scores = jnp.where(late >= l * 512, scores, -jnp.inf)
                sbuf[at, l] = scores
        fades = []
        for at, hm, _, _ in chains:
            old = peak[half, hm]
            new = jnp.maximum(
                old, jnp.max(jnp.maximum(sbuf[at, 0], sbuf[at, 1]), axis=0, keepdims=True)
            )
            fade = jnp.exp(old - new)
            total = denom[half, hm] * fade
            for l in range(2):
                term = jnp.exp(sbuf[at, l] - new)
                total = total + jnp.sum(term, axis=0, keepdims=True)
                pbuf[at, l] = term.astype(BF16)
            denom[half, hm] = total
            peak[half, hm] = new
            fades.append(fade)
        for at, hm, near_chip, pair in chains:
            acc[half, hm] = acc[half, hm] * fades[at] + sum(
                mm(values(near_chip, pair, l, hm % 2), pbuf[at, l]) for l in range(2)
            )

    def w_stage(stage):
        if stage == W_NEAR:
            drain(wout.at[0], w_recv.at[0])
            w_copy(left, 0, right, 2).start()
            w_copy(right, 1, left, 3).start()
            w_sib(left, 0, c).start()
            w_sib(right, 1, c).start()
        else:
            drain(wout.at[0, 0], w_recv.at[1])
            w_sib(far, 2, c).start()

    others = (left, right, far)

    def r_copy(slot, n):
        piece = rsend.at[pl.ds(pl.multiple_of(slot * 128, 128), 128)]
        return remote(piece, heads.at[1, t], r_send, r_recv, (sp, slot))

    def chain(j, state):
        own = states[j].astype(F32)
        return state * jnp.exp(own[64:65] + own[65:66] + own[66:67]) + own[0:64]

    def retention_end():
        drain(states.at[pl.ds(0, 16)], st_pair_recv)
        state = lax.fori_loop(0, sp, chain, jnp.concatenate([init[0], init[1]], axis=1))
        state = jnp.concatenate([state[:, 0:128], state[:, 128:256]], axis=0)
        for b in range(2):
            for h in range(2):
                mine = (lane < 64) if h == 0 else (lane >= 64)
                older = mm(jnp.where(mine, retq[b], 0.0), state, HIGHEST)
                r = rgate[b, h] + older
                rsend[b * 256 : b * 256 + 256, h * 128 : h * 128 + 128] = head_norm(r, 1).astype(BF16)
            state = retfade[b] * state + retadd[b]
        for n, slot in enumerate(others):
            r_copy(slot, n).start()
        heads[1, t] = rsend[pl.ds(pl.multiple_of(t * 128, 128), 128)]

    codes = [
        sum(((dz + 1) * 8 + (dy + 1) * 2 + pair) * scale for scale, (dz, dy, pair) in zip((1, 32), units))
        for _, *units in SCHEDULE
    ]

    def happen(events):
        for event in events:
            if event == RETENTION:
                retention_end()
            elif event in (W_NEAR, W_FAR):
                w_stage(event)
            else:
                arrival(*event)

    def handled(s, low, high):
        if high - low > 1:
            middle = (low + high) // 2
            return lax.cond(
                s < middle, lambda: handled(s, low, middle), lambda: handled(s, middle, high)
            )
        if low > 0:
            happen(SCHEDULE[low][0])
        return jnp.int32(codes[low])

    def tick(s, carry):
        code = handled(s, 0, len(SCHEDULE))
        units = []
        for part in (lax.rem(code, 32), lax.div(code, 32)):
            near_chip = chip(lax.div(part, 8) - 1, lax.rem(lax.div(part, 2), 4) - 1)
            pair = lax.rem(part, 2)
            pair_copy(near_chip * 2 + 1 - c, pair, 0).wait_recv()
            units.append((near_chip, pair))
        (chip_a, pair_a), (chip_b, pair_b) = units

        def one_half(half, carry):
            bound = jnp.where(half == 0, sp, partner)
            last = lax.div(bound, 2)
            early_a, early_b = chip_a < last, chip_b < last

            @pl.when(jnp.logical_and(early_a, early_b))
            def _():
                attend(half, units)

            @pl.when(jnp.logical_xor(early_a, early_b))
            def _():
                attend(half, [(jnp.where(early_a, chip_a, chip_b), jnp.where(early_a, pair_a, pair_b))])

            def one_edge(n, carry):
                near_chip = jnp.where(n == 0, chip_a, chip_b)

                @pl.when(near_chip == last)
                def _():
                    attend(half, [(near_chip, jnp.where(n == 0, pair_a, pair_b))], bound)

                return carry

            @pl.when(jnp.logical_or(chip_a == last, chip_b == last))
            def _():
                lax.fori_loop(0, 2, one_edge, 0)

            return carry

        return lax.fori_loop(0, 2, one_half, carry)

    lax.fori_loop(0, len(SCHEDULE), tick, 0)
    happen(LAST)
    assert kv_used == [15] * 4 and len(pairs_used) == 32 and len(st_pairs_used) == 16

    def o_copy(src, at, count, dev, sem):
        place = heads.at[0, t, pl.ds(at, count)]
        return remote(src, place, o_send, o_recv.at[sem], dev)

    def finish(half):
        sides = []
        for h in range(2):
            weight_two = mix[:, h : h + 1]
            first = acc[half, h] / denom[half, h]
            second = acc[half, 2 + h] / denom[half, 2 + h]
            attn = first - weight_two * second
            sides.append((head_norm(attn, 0) * DIFF_SCALE).T * hgain[...])
        dsend[half] = jnp.concatenate(sides, axis=1).astype(BF16)

    def o_copies(half):
        if half == 0:
            return [
                o_copy(dsend.at[0, pl.ds(128, 128)], 0, 128, (sp, far), 1),
                o_copy(dsend.at[0, pl.ds(0, 64)], 64, 64, (sp, left), 0),
                o_copy(dsend.at[0, pl.ds(64, 64)], 0, 64, (sp, right), 0),
            ]
        return [
            o_copy(dsend.at[1, pl.ds(0, 128)], 0, 128, (partner, t), 0),
            o_copy(dsend.at[1, pl.ds(128, 64)], 0, 64, (partner, left), 0),
            o_copy(dsend.at[1, pl.ds(192, 64)], 64, 64, (partner, right), 0),
        ]

    for half in range(2):
        finish(half)
        for copy in o_copies(half):
            copy.start()

    def product(kind, slots, first=False, last=False):
        def columns(n, carry):
            at = pl.ds(pl.multiple_of(n * 512, 512), 512)
            block = jnp.zeros((128, 512), F32) if first else osum[:, at]
            for slot in slots:
                block += mm(heads[kind, slot], wout[slot, kind, :, at])
            if last:
                out[:, at] = block.astype(BF16)
            else:
                osum[:, at] = block
            return carry

        lax.fori_loop(0, 4, columns, 0)

    drain(wout.at[pl.ds(0, 3), 0], w_recv.at[2])
    drain(rsend.at[pl.ds(0, 384)], r_recv)
    product(1, range(4), first=True)

    drain(dsend.at[:, pl.ds(0, 192)], o_recv.at[0])
    product(0, (t, left, right))
    drain(dsend.at[0, pl.ds(0, 128)], o_recv.at[1])
    product(0, (far,), last=True)

    drain(rows.at[pl.ds(0, 3)], x_send)
    drain(wout.at[pl.ds(0, 3)], w_send)
    drain(rsend.at[pl.ds(0, 384)], r_send)
    drain(dsend, o_send)
    q_copy.wait_send()
    for way in range(4):
        drain(kv.at[pl.ds(0, kv_used[way]), 0], kv_send.at[way])
        drain(states.at[pl.ds(0, st_used[way])], st_send.at[way])
    drain(kv.at[:, pl.ds(0, 2)], pair_send)
    drain(states.at[pl.ds(0, 16)], st_pair_send)


def retention_inside(lg, retp, rgate, retq, retadd, retfade, states, sp, row, col, lane):
    state_row = lax.broadcasted_iota(jnp.int32, (128, 128), 0)
    upper = jnp.where(row <= col, 1.0, 0.0)
    adds, fades, lasts_of = [], [], []
    for b in range(2):
        span = slice(b * 256, b * 256 + 256)
        lb = lg[:, span]
        cum_rows = mm(jnp.concatenate([lb, lb, lb, lb], axis=0), upper, HIGHEST)
        rq, rk = retp[0, span, 0:128], retp[0, span, 128:256]
        cols, lasts = [], []
        for h in range(2):
            cum_col = jnp.sum(jnp.where(col <= row, lb[h : h + 1], 0.0), axis=1, keepdims=True)
            cols.append(cum_col)
            lasts.append(jnp.sum(lb[h : h + 1], axis=1, keepdims=True))
            mine = (lane < 64) if h == 0 else (lane >= 64)
            raw = nt(jnp.where(mine, rq, jnp.zeros_like(rq)), rk)
            gap = jnp.where(col <= row, cum_col - cum_rows[h : h + 1], -jnp.inf)
            gate = (raw * 0.125 * jnp.exp(gap)).astype(BF16)
            rgate[b, h] = mm(gate, retp[1, span, h * 128 : h * 128 + 128])
        factor = jnp.where(lane < 64, jnp.exp(lasts[0] - cols[0]), jnp.exp(lasts[1] - cols[1]))
        keys = (rk.astype(F32) * 0.125 * factor).T.astype(BF16)
        both = mm(keys, retp[1, span])
        adds.append(jnp.where(state_row < 64, both[:, 0:128], both[:, 128:256]))
        fades.append(jnp.where(state_row < 64, jnp.exp(lasts[0]), jnp.exp(lasts[1])))
        grow = jnp.where(lane < 64, jnp.exp(cols[0]), jnp.exp(cols[1]))
        retq[b] = rq.astype(F32) * grow
        retadd[b] = adds[b]
        retfade[b] = fades[b]
        lasts_of.append(lasts)
    own = fades[1] * adds[0] + adds[1]
    states[sp, 0:64] = jnp.concatenate([own[0:64], own[64:128]], axis=1).astype(BF16)
    tile_lane = lax.broadcasted_iota(jnp.int32, (16, 256), 1)
    tile_row = lax.broadcasted_iota(jnp.int32, (16, 256), 0)
    total = jnp.where(
        tile_lane < 128, lasts_of[0][0] + lasts_of[1][0], lasts_of[0][1] + lasts_of[1][1]
    )
    high = total.astype(BF16).astype(F32)
    middle = (total - high).astype(BF16).astype(F32)
    low = total - high - middle
    tile = jnp.where(tile_row == 0, high, jnp.where(tile_row == 1, middle, low))
    states[sp, 64:80] = tile.astype(BF16)


def on_device(
    tokens, norm_gain, w_query_one, w_query_two, w_key_one, w_key_two, w_value, mix_lambda,
    head_gain, w_ret_query, w_ret_key, w_ret_value, retain_log, init_state, w_out_diff, w_out_ret,
):
    vmem = pl.BlockSpec(memory_space=pltpu.VMEM)
    hbm = pl.BlockSpec(memory_space=pl.ANY)
    dma = pltpu.SemaphoreType.DMA
    return pl.pallas_call(
        kernel,
        out_shape=jax.ShapeDtypeStruct((128, 2048), BF16),
        in_specs=[hbm] * 16,
        out_specs=vmem,
        scratch_shapes=[
            pltpu.VMEM((128, 2048), BF16),
            pltpu.VMEM((1, 2048), F32),
            pltpu.VMEM((1, 2), F32),
            pltpu.VMEM((1, 128), F32),
            pltpu.VMEM((2, 512), F32),
            pltpu.VMEM((2, 64, 128), F32),
            pltpu.VMEM((4, 128, 2048), BF16),
            pltpu.VMEM((2048, 1280), BF16),
            pltpu.VMEM((2, 256, 256), BF16),
            pltpu.VMEM((256, 256), BF16),
            pltpu.VMEM((32, 4, 256, 256), BF16),
            pltpu.VMEM((32, 80, 256), BF16),
            pltpu.VMEM((2, 512, 256), BF16),
            pltpu.VMEM((4, 2, 256, 2048), BF16),
            pltpu.VMEM((2, 4, 256, 256), BF16),
            pltpu.VMEM((2, 4, 128, 256), F32),
            pltpu.VMEM((2, 4, 1, 256), F32),
            pltpu.VMEM((2, 4, 1, 256), F32),
            pltpu.VMEM((8, 2, 256, 256), F32),
            pltpu.VMEM((8, 2, 256, 256), BF16),
            pltpu.VMEM((2, 2, 256, 128), F32),
            pltpu.VMEM((2, 256, 128), F32),
            pltpu.VMEM((2, 128, 128), F32),
            pltpu.VMEM((2, 128, 128), F32),
            pltpu.VMEM((128, 2048), F32),
            pltpu.VMEM((2, 256, 256), BF16),
            pltpu.VMEM((512, 256), BF16),
            pltpu.VMEM((2, 4, 128, 256), BF16),
            dma((9,)),
            dma,
            dma((3,)),
            dma,
            dma((3,)),
            dma((4,)),
            dma((16, 4)),
            dma,
            dma((16, 2)),
            dma((4,)),
            dma((16,)),
            dma,
            dma,
            dma((2,)),
            dma,
            dma((2,)),
            dma,
            dma,
        ],
        compiler_params=pltpu.CompilerParams(
            collective_id=0, has_side_effects=True, vmem_limit_bytes=60 * 1024 * 1024,
        ),
        cost_estimate=pl.CostEstimate(
            flops=20_000_000_000, bytes_accessed=10_000_000, transcendentals=17_000_000
        ),
        name="layer",
    )(
        tokens, norm_gain.reshape(1, -1), w_query_one, w_query_two, w_key_one, w_key_two, w_value,
        mix_lambda.reshape(1, -1), head_gain.reshape(1, -1),
        w_ret_query, w_ret_key, w_ret_value, retain_log, init_state, w_out_diff, w_out_ret,
    )


def solution(mesh):
    both = ("sp", "tp")
    return jax.shard_map(
        on_device,
        mesh=mesh,
        in_specs=(
            P(both, None), P(), P(None, "tp"), P(None, "tp"), P(None, "tp"), P(None, "tp"),
            P(None, "tp"), P("tp"), P(), P(None, "tp"), P(None, "tp"), P(None, "tp"),
            P("tp", "sp"), P("tp", None, None), P("tp", None), P("tp", None),
        ),
        out_specs=P(both, None),
        check_vma=False,
    )
```

```python
import jax
import jax.numpy as jnp
from jax import lax
from jax.experimental import pallas as pl
from jax.experimental.pallas import tpu as pltpu
from jax.sharding import PartitionSpec as P

NORM_EPS = 1e-06
HEAD_EPS = 1e-05
DIFF_SCALE = 0.8
MESH = pl.DeviceIdType.MESH
F32 = jnp.float32
BF16 = jnp.bfloat16
HIGHEST = lax.Precision.HIGHEST
LOWEST = -3.0e38


W_NEAR, W_FAR, RETENTION = range(3)
SCHEDULE = (
    (((0, 0, 0), (0, -1, 0), (0, 0, 1), (-1, 0, 0), (0, 1, 0), (0, 0, 2), (1, -1, 0), (-1, 0, 1), (0, 1, 1), (0, 0, 3), (1, 0, 0), (0, 0, 4), (0, -1, 1), (0, 1, 2), (1, 0, 2), (0, -1, 2)), (-1, 0, 0), (0, 0, 0)),
    (((1, 0, 3), (2, 0, 0), (0, 1, 3), (0, -1, 4), (-1, 1, 1), (0, -1, 3), (0, 1, 4)), (0, 0, 1), (1, 0, 1)),
    (((-1, 0, 2), (1, 0, 1)), (0, 1, 0), (0, -1, 0)),
    (((2, 0, 1), (-1, 0, 3), (0, 2, 2), (-1, -1, 0), (-1, -1, 1), (-1, 1, 0), (1, 1, 0), (2, 0, 3)), (0, -1, 1), (1, 0, 0)),
    (((2, 0, 2),), (-1, 0, 1), (-1, 1, 0)),
    (((0, 2, 4), (1, -1, 2), (0, 2, 1), (0, 2, 0), (1, 0, 4)), (2, 0, 0), (-1, -1, 0)),
    (((-1, -1, 3), (-1, 1, 3), (1, 1, 3), (1, -1, 1), (-1, 1, 4), (-1, -1, 2), (-1, 1, 2), (1, 1, 4)), (2, 0, 1), (0, 2, 0)),
    ((W_NEAR, (-1, -1, 4), (0, 2, 3), (1, -1, 3), (1, 1, 2), (-1, 0, 4)), (-1, -1, 1), (-1, 1, 1)),
    (((2, -1, 0), (2, -1, 1), (1, 1, 1), (2, 1, 1)), (1, -1, 1), (0, 2, 1)),
    (((1, 2, 0), (-1, 2, 4), (2, 1, 2)), (1, 1, 0), (1, 1, 1)),
    (((-1, 2, 1), (2, -1, 2), (2, 1, 0), (2, 1, 3), (-1, 2, 0)), (2, -1, 0), (1, -1, 0)),
    ((), (2, 1, 1), (2, 1, 0)),
    (((-1, 2, 2), (1, 2, 1), (1, -1, 4), (2, 1, 4), (2, -1, 4), (2, -1, 3), (1, 2, 4), (2, 0, 4), (2, 2, 4), (1, 2, 3)), (0, 1, 1), (-1, 2, 0)),
    (((-1, 2, 3), RETENTION, (2, 2, 1), (1, 2, 2), (2, 2, 0)), (1, 2, 0), (2, -1, 1)),
    (((2, 2, 3), (2, 2, 2), W_FAR), (-1, 2, 1), (2, 2, 0)),
    ((), (1, 2, 1), (2, 2, 1)),
)
LAST = ()
PLUS_Y, MINUS_Y, PLUS_Z, MINUS_Z = range(4)
STEPS = ((0, 1), (0, -1), (1, 0), (-1, 0))
ALONG_Y_FIRST = (0, 3, 4)
ONWARD_BY_PLUS = (0, 1, 4)


def nt(a, b, precision=None):
    return lax.dot_general(
        a, b, (((1,), (1,)), ((), ())), preferred_element_type=F32, precision=precision
    )


def mm(a, b, precision=None):
    return jnp.dot(a, b, preferred_element_type=F32, precision=precision)


def head_norm(values, axis):
    return values * lax.rsqrt(jnp.mean(values * values, axis=axis, keepdims=True) + HEAD_EPS)


def routes(dz, dy, quarter):
    y_first = quarter in ALONG_Y_FIRST
    ways = ((PLUS_Y, MINUS_Y), (PLUS_Z, MINUS_Z))
    first, second = ways if y_first else ways[::-1]
    a, b = (dy, dz) if y_first else (dz, dy)
    by_plus = quarter in ONWARD_BY_PLUS
    if a == 0 and b == 0:
        return first + second
    line, at = (first, a) if b == 0 else (second, b)
    onward = ()
    if at == -1 and by_plus:
        onward = (line[0],)
    elif at == 1 and not by_plus:
        onward = (line[1],)
    return onward + (second if b == 0 else ())


def kernel(
    tokens_in, gain_in, wq1, wq2, wk1, wk2, wv, mix_in, hgain_in, wrq, wrk, wrv, logs_in, init_in, wod, wor,
    out,
    tokens, gain, mix, hgain, logs, init, rows, weights, qt, qrecv, kv, states, retp, wout, qpad, acc, peak, denom, sbuf, pbuf, rgate, retq, retadd, retfade, osum,
    dsend, rsend, heads,
    load_sem, x_send, x_recv, w_send, w_recv, kv_send, kv_recv, pair_send, pair_recv,
    st_send, st_recv, st_pair_send, st_pair_recv, q_sem, o_send, o_recv, r_send, r_recv,
):
    sp = lax.axis_index("sp")
    t = lax.axis_index("tp")
    z, y, c = lax.div(sp, 8), lax.rem(lax.div(sp, 2), 4), lax.rem(sp, 2)
    partner = 31 - sp
    sib = (sp + 1 - 2 * c, t)
    left, right, far = lax.rem(t + 3, 4), lax.rem(t + 1, 4), lax.rem(t + 2, 4)

    def chip(dz, dy):
        return lax.rem(z + dz + 4, 4) * 4 + lax.rem(y + dy + 4, 4)

    near = [(chip(dz, dy) * 2 + c, t) for dz, dy in STEPS]

    small = [
        pltpu.make_async_copy(source, held, load_sem.at[3 + k])
        for k, (source, held) in enumerate((
            (tokens_in, tokens), (gain_in, gain), (logs_in, logs),
            (mix_in, mix), (hgain_in, hgain), (init_in, init),
        ))
    ]
    for load in small:
        load.start()
    loads = []
    sources = (
        (wk1, 256, 128), (wk2, 384, 128), (wv, 512, 256), (wq1, 0, 128), (wq2, 128, 128),
        (wrq, 768, 128), (wrk, 896, 128), (wrv, 1024, 256),
    )
    for k, (ref, at, width) in enumerate(sources):
        group = load_sem.at[0 if k < 3 else 1]
        loads.append(pltpu.make_async_copy(ref, weights.at[:, pl.ds(at, width)], group))
    for k, ref in enumerate((wod, wor)):
        loads.append(pltpu.make_async_copy(ref, wout.at[t, k], load_sem.at[2]))
    def drain(piece, sem):
        pltpu.make_async_copy(piece, piece, sem).wait()

    barrier = pltpu.get_barrier_semaphore()
    peers = [(sp, left), (sp, right), (sp, far), sib, *near] + [(partner, d) for d in range(4)]
    for peer in peers:
        pl.semaphore_signal(barrier, inc=1, device_id=peer, device_id_type=MESH)

    for load in loads[:3]:
        load.start()
    for load in small[:2]:
        load.wait()
    for chunk in range(2):
        floats = tokens[chunk * 64 : chunk * 64 + 64].astype(F32)
        scale = lax.rsqrt(jnp.mean(floats * floats, axis=-1, keepdims=True) + NORM_EPS)
        rows[t, chunk * 64 : chunk * 64 + 64] = (floats * scale * gain[...]).astype(BF16)
    for load in small[2:]:
        load.wait()
    lg = logs[...]

    pl.semaphore_wait(barrier, len(peers))

    def remote(src, dst, ssem, rsem, dev):
        return pltpu.make_async_remote_copy(
            src_ref=src, dst_ref=dst, send_sem=ssem, recv_sem=rsem, device_id=dev,
            device_id_type=MESH,
        )

    def x_copy(slot, chunk, to, n):
        piece = rows.at[slot, pl.ds(chunk * 64, 64)]
        return remote(piece, piece, x_send, x_recv.at[n // 2], (sp, to))

    def w_copy(slot, part, to, n):
        piece = wout.at[slot, c] if part is None else wout.at[slot, c, pl.ds(part * 128, 128)]
        rsem = w_recv.at[0 if part is None else 1]
        return remote(piece, piece, w_send, rsem, (sp, to))

    def w_sib(slot, n, kind):
        piece = wout.at[slot, kind]
        return remote(piece, piece, w_send, w_recv.at[2], sib)

    def kv_copy(j, q, way, n, dev):
        return remote(kv.at[j, q], kv.at[j, q], kv_send.at[way], kv_recv.at[lax.div(j, 2), q], dev)

    def st_copy(j, way, n, dev):
        return remote(states.at[j], states.at[j], st_send.at[way], st_recv.at[lax.div(j, 2)], dev)

    def pair_copy(j, pair, n):
        piece = kv.at[j, pl.ds(2 * pair, 2)]
        return remote(piece, piece, pair_send, pair_recv.at[lax.div(j, 2), pair], sib)

    def st_pair_copy(j, n):
        return remote(states.at[j], states.at[j], st_pair_send, st_pair_recv, sib)

    kv_used, st_used, pairs_used, st_pairs_used = [0] * 4, [0] * 4, [], []

    def pass_on(dz, dy, q):
        j = chip(dz, dy) * 2 + c
        for way in routes(dz, dy, q):
            kv_copy(j, q, way, kv_used[way], near[way]).start()
            kv_used[way] += 1

    def pass_state_on(dz, dy):
        j = chip(dz, dy) * 2 + c
        for way in routes(dz, dy, 4):
            st_copy(j, way, st_used[way], near[way]).start()
            st_used[way] += 1
        st_pair_copy(j, len(st_pairs_used)).start()
        st_pairs_used.append((dz, dy))

    arrived = set()

    def pair_to_sib(dz, dy, q):
        arrived.add((dz, dy, q))
        if (dz, dy, q ^ 1) in arrived:
            pair_copy(chip(dz, dy) * 2 + c, q // 2, len(pairs_used)).start()
            pairs_used.append((dz, dy, q // 2))

    def arrival(dz, dy, q):
        j = chip(dz, dy) * 2 + c
        if q == 4:
            st_copy(j, 0, 0, sib).wait_recv()
            pass_state_on(dz, dy)
        else:
            kv_copy(j, q, 0, 0, sib).wait_recv()
            pass_on(dz, dy, q)
            pair_to_sib(dz, dy, q)

    x_copy(t, 0, right, 0).start()
    x_copy(t, 1, left, 1).start()
    x_copy(t, 1, right, 2).start()
    x_copy(t, 0, left, 3).start()
    for load in loads[3:]:
        load.start()

    def times(lhs, n):
        return mm(lhs, weights[:, n * 256 : n * 256 + 256])

    spots = (
        ((0, t * 128, 128),),
        ((0, left * 128, 64), (64, right * 128 + 64, 64)),
        ((0, left * 128 + 64, 64), (64, right * 128, 64)),
        ((0, far * 128, 128),),
    )

    def own_quarter(q):
        if q == 0:
            drain(weights.at[:, pl.ds(256, 512)], load_sem.at[0])
            lhs = rows[t]
        elif q == 1:
            drain(rows.at[0], x_recv.at[0])
            x_copy(left, 0, right, 4).start()
            x_copy(right, 1, left, 5).start()
            lhs = jnp.concatenate([rows[left, 0:64], rows[right, 64:128]], axis=0)
        elif q == 2:
            drain(rows.at[0], x_recv.at[1])
            lhs = jnp.concatenate([rows[left, 64:128], rows[right, 0:64]], axis=0)
        else:
            drain(rows.at[0], x_recv.at[2])
            lhs = rows[far]
        kv[sp, q, 0:128] = times(lhs, 1).astype(BF16)
        turned = times(lhs, 2).T.astype(BF16)
        kv[sp, q, 128:256] = jnp.concatenate([turned[0:128], turned[128:256]], axis=1)
        pass_on(0, 0, q)
        pair_to_sib(0, 0, q)
        if q == 0:
            drain(weights.at[:, pl.ds(0, 768)], load_sem.at[1])
        at = q % 2 * 128
        qt[q // 2, :, at : at + 128] = times(lhs, 0).T.astype(BF16)
        for n in range(2):
            block = times(lhs, 3 + n).astype(BF16)
            for here, there, count in spots[q]:
                retp[n, pl.ds(pl.multiple_of(there, 64), count)] = block[here : here + count]
        if q == 1:
            q_copy.start()
            drain(wout.at[t], load_sem.at[2])
            w_copy(t, None, right, 0).start()
            w_copy(t, None, left, 1).start()

    q_copy = remote(qt.at[0], qrecv, q_sem.at[0], q_sem.at[1], (partner, t))
    row = lax.broadcasted_iota(jnp.int32, (256, 256), 0)
    col = lax.broadcasted_iota(jnp.int32, (256, 256), 1)
    lane = lax.broadcasted_iota(jnp.int32, (256, 128), 1)

    for event in SCHEDULE[0][0]:
        if event == (0, 0, 4):
            retention_inside(lg, retp, rgate, retq, retadd, retfade, states, sp, row, col, lane)
            pass_state_on(0, 0)
        elif event[:2] == (0, 0):
            own_quarter(event[2])
        else:
            arrival(*event)

    def queries_of(half, block):
        big = block.astype(F32) * 0.125
        for hm in range(4):
            qpad[half, hm] = jnp.where(lax.div(row, 64) == hm, big, 0.0).astype(BF16)

    queries_of(0, qt[1])
    for half in range(2):
        for hm in range(4):
            peak[half, hm] = jnp.full((1, 256), LOWEST, F32)
            denom[half, hm] = jnp.zeros((1, 256), F32)
            acc[half, hm] = jnp.zeros((128, 256), F32)
    q_copy.wait_recv()
    queries_of(1, qrecv[...])

    def position(index, pair):
        early = jnp.where(
            index < 128, t * 128 + index,
            jnp.where(index < 192, left * 128 + index - 128, right * 128 + index - 128),
        )
        late = jnp.where(
            index < 64, left * 128 + 64 + index,
            jnp.where(index < 128, right * 128 + index - 64, far * 128 + index - 128),
        )
        return jnp.where(pair == 0, early, late)

    def attend(half, units, bound=None):
        def keys(near_chip, pair, l):
            return jnp.concatenate([kv[near_chip * 2 + l, 2 * pair + p, 0:128] for p in range(2)], axis=0)

        def values(near_chip, pair, l, h):
            cut = slice(h * 128, h * 128 + 128)
            return jnp.concatenate(
                [kv[near_chip * 2 + l, 2 * pair + p, 128:256, cut] for p in range(2)], axis=1
            )

        chains = [(n * 4 + hm, hm, *unit) for n, unit in enumerate(units) for hm in range(4)]
        for at, hm, near_chip, pair in chains:
            if bound is not None and hm == 0:
                late = position(col, 1 - half) - position(row, pair) + (bound - near_chip * 2) * 512
            for l in range(2):
                scores = mm(keys(near_chip, pair, l), qpad[half, hm])
                if bound is not None:
                    scores = jnp.where(late >= l * 512, scores, -jnp.inf)
                sbuf[at, l] = scores
        fades = []
        for at, hm, _, _ in chains:
            old = peak[half, hm]
            new = jnp.maximum(
                old, jnp.max(jnp.maximum(sbuf[at, 0], sbuf[at, 1]), axis=0, keepdims=True)
            )
            fade = jnp.exp(old - new)
            total = denom[half, hm] * fade
            for l in range(2):
                term = jnp.exp(sbuf[at, l] - new)
                total = total + jnp.sum(term, axis=0, keepdims=True)
                pbuf[at, l] = term.astype(BF16)
            denom[half, hm] = total
            peak[half, hm] = new
            fades.append(fade)
        for at, hm, near_chip, pair in chains:
            acc[half, hm] = acc[half, hm] * fades[at] + sum(
                mm(values(near_chip, pair, l, hm % 2), pbuf[at, l]) for l in range(2)
            )

    def w_stage(stage):
        if stage == W_NEAR:
            drain(wout.at[0], w_recv.at[0])
            w_copy(left, 0, right, 2).start()
            w_copy(right, 1, left, 3).start()
            w_sib(left, 0, c).start()
            w_sib(right, 1, c).start()
        else:
            drain(wout.at[0, 0], w_recv.at[1])
            w_sib(far, 2, c).start()

    others = (left, right, far)

    def r_copy(slot, n):
        piece = rsend.at[pl.ds(pl.multiple_of(slot * 128, 128), 128)]
        return remote(piece, heads.at[1, t], r_send, r_recv, (sp, slot))

    def chain(j, state):
        own = states[j].astype(F32)
        return state * jnp.exp(own[64:65] + own[65:66] + own[66:67]) + own[0:64]

    def retention_end():
        drain(states.at[pl.ds(0, 16)], st_pair_recv)
        state = lax.fori_loop(0, sp, chain, jnp.concatenate([init[0], init[1]], axis=1))
        state = jnp.concatenate([state[:, 0:128], state[:, 128:256]], axis=0)
        for b in range(2):
            for h in range(2):
                mine = (lane < 64) if h == 0 else (lane >= 64)
                older = mm(jnp.where(mine, retq[b], 0.0), state, HIGHEST)
                r = rgate[b, h] + older
                rsend[b * 256 : b * 256 + 256, h * 128 : h * 128 + 128] = head_norm(r, 1).astype(BF16)
            state = retfade[b] * state + retadd[b]
        for n, slot in enumerate(others):
            r_copy(slot, n).start()
        heads[1, t] = rsend[pl.ds(pl.multiple_of(t * 128, 128), 128)]

    codes = [
        sum(((dz + 1) * 8 + (dy + 1) * 2 + pair) * scale for scale, (dz, dy, pair) in zip((1, 32), units))
        for _, *units in SCHEDULE
    ]

    def happen(events):
        for event in events:
            if event == RETENTION:
                retention_end()
            elif event in (W_NEAR, W_FAR):
                w_stage(event)
            else:
                arrival(*event)

    def handled(s, low, high):
        if high - low > 1:
            middle = (low + high) // 2
            return lax.cond(
                s < middle, lambda: handled(s, low, middle), lambda: handled(s, middle, high)
            )
        if low > 0:
            happen(SCHEDULE[low][0])
        return jnp.int32(codes[low])

    def tick(s, carry):
        code = handled(s, 0, len(SCHEDULE))
        units = []
        for part in (lax.rem(code, 32), lax.div(code, 32)):
            near_chip = chip(lax.div(part, 8) - 1, lax.rem(lax.div(part, 2), 4) - 1)
            pair = lax.rem(part, 2)
            pair_copy(near_chip * 2 + 1 - c, pair, 0).wait_recv()
            units.append((near_chip, pair))
        (chip_a, pair_a), (chip_b, pair_b) = units

        def one_half(half, carry):
            bound = jnp.where(half == 0, sp, partner)
            last = lax.div(bound, 2)
            early_a, early_b = chip_a < last, chip_b < last

            @pl.when(jnp.logical_and(early_a, early_b))
            def _():
                attend(half, units)

            @pl.when(jnp.logical_xor(early_a, early_b))
            def _():
                attend(half, [(jnp.where(early_a, chip_a, chip_b), jnp.where(early_a, pair_a, pair_b))])

            def one_edge(n, carry):
                near_chip = jnp.where(n == 0, chip_a, chip_b)

                @pl.when(near_chip == last)
                def _():
                    attend(half, [(near_chip, jnp.where(n == 0, pair_a, pair_b))], bound)

                return carry

            @pl.when(jnp.logical_or(chip_a == last, chip_b == last))
            def _():
                lax.fori_loop(0, 2, one_edge, 0)

            return carry

        return lax.fori_loop(0, 2, one_half, carry)

    lax.fori_loop(0, len(SCHEDULE), tick, 0)
    happen(LAST)
    assert kv_used == [15] * 4 and len(pairs_used) == 32 and len(st_pairs_used) == 16

    def o_copy(src, at, count, dev, sem):
        place = heads.at[0, t, pl.ds(at, count)]
        return remote(src, place, o_send, o_recv.at[sem], dev)

    def finish(half):
        sides = []
        for h in range(2):
            weight_two = mix[:, h : h + 1]
            first = acc[half, h] / denom[half, h]
            second = acc[half, 2 + h] / denom[half, 2 + h]
            attn = first - weight_two * second
            sides.append((head_norm(attn, 0) * DIFF_SCALE).T * hgain[...])
        dsend[half] = jnp.concatenate(sides, axis=1).astype(BF16)

    def o_copies(half):
        if half == 0:
            return [
                o_copy(dsend.at[0, pl.ds(128, 128)], 0, 128, (sp, far), 1),
                o_copy(dsend.at[0, pl.ds(0, 64)], 64, 64, (sp, left), 0),
                o_copy(dsend.at[0, pl.ds(64, 64)], 0, 64, (sp, right), 0),
            ]
        return [
            o_copy(dsend.at[1, pl.ds(0, 128)], 0, 128, (partner, t), 0),
            o_copy(dsend.at[1, pl.ds(128, 64)], 0, 64, (partner, left), 0),
            o_copy(dsend.at[1, pl.ds(192, 64)], 64, 64, (partner, right), 0),
        ]

    for half in range(2):
        finish(half)
        for copy in o_copies(half):
            copy.start()

    def product(kind, slots, first=False, last=False):
        def columns(n, carry):
            at = pl.ds(pl.multiple_of(n * 512, 512), 512)
            block = jnp.zeros((128, 512), F32) if first else osum[:, at]
            for slot in slots:
                block += mm(heads[kind, slot], wout[slot, kind, :, at])
            if last:
                out[:, at] = block.astype(BF16)
            else:
                osum[:, at] = block
            return carry

        lax.fori_loop(0, 4, columns, 0)

    drain(wout.at[pl.ds(0, 3), 0], w_recv.at[2])
    drain(rsend.at[pl.ds(0, 384)], r_recv)
    product(1, range(4), first=True)

    drain(dsend.at[:, pl.ds(0, 192)], o_recv.at[0])
    product(0, (t, left, right))
    drain(dsend.at[0, pl.ds(0, 128)], o_recv.at[1])
    product(0, (far,), last=True)

    drain(rows.at[pl.ds(0, 3)], x_send)
    drain(wout.at[pl.ds(0, 3)], w_send)
    drain(rsend.at[pl.ds(0, 384)], r_send)
    drain(dsend, o_send)
    q_copy.wait_send()
    for way in range(4):
        drain(kv.at[pl.ds(0, kv_used[way]), 0], kv_send.at[way])
        drain(states.at[pl.ds(0, st_used[way])], st_send.at[way])
    drain(kv.at[:, pl.ds(0, 2)], pair_send)
    drain(states.at[pl.ds(0, 16)], st_pair_send)


def retention_inside(lg, retp, rgate, retq, retadd, retfade, states, sp, row, col, lane):
    state_row = lax.broadcasted_iota(jnp.int32, (128, 128), 0)
    upper = jnp.where(row <= col, 1.0, 0.0)
    adds, fades, lasts_of = [], [], []
    for b in range(2):
        span = slice(b * 256, b * 256 + 256)
        lb = lg[:, span]
        cum_rows = mm(jnp.concatenate([lb, lb, lb, lb], axis=0), upper, HIGHEST)
        rq, rk = retp[0, span, 0:128], retp[0, span, 128:256]
        cols, lasts = [], []
        for h in range(2):
            cum_col = jnp.sum(jnp.where(col <= row, lb[h : h + 1], 0.0), axis=1, keepdims=True)
            cols.append(cum_col)
            lasts.append(jnp.sum(lb[h : h + 1], axis=1, keepdims=True))
            mine = (lane < 64) if h == 0 else (lane >= 64)
            raw = nt(jnp.where(mine, rq, jnp.zeros_like(rq)), rk)
            gap = jnp.where(col <= row, cum_col - cum_rows[h : h + 1], -jnp.inf)
            gate = (raw * 0.125 * jnp.exp(gap)).astype(BF16)
            rgate[b, h] = mm(gate, retp[1, span, h * 128 : h * 128 + 128])
        factor = jnp.where(lane < 64, jnp.exp(lasts[0] - cols[0]), jnp.exp(lasts[1] - cols[1]))
        keys = (rk.astype(F32) * 0.125 * factor).T.astype(BF16)
        both = mm(keys, retp[1, span])
        adds.append(jnp.where(state_row < 64, both[:, 0:128], both[:, 128:256]))
        fades.append(jnp.where(state_row < 64, jnp.exp(lasts[0]), jnp.exp(lasts[1])))
        grow = jnp.where(lane < 64, jnp.exp(cols[0]), jnp.exp(cols[1]))
        retq[b] = rq.astype(F32) * grow
        retadd[b] = adds[b]
        retfade[b] = fades[b]
        lasts_of.append(lasts)
    own = fades[1] * adds[0] + adds[1]
    states[sp, 0:64] = jnp.concatenate([own[0:64], own[64:128]], axis=1).astype(BF16)
    tile_lane = lax.broadcasted_iota(jnp.int32, (16, 256), 1)
    tile_row = lax.broadcasted_iota(jnp.int32, (16, 256), 0)
    total = jnp.where(
        tile_lane < 128, lasts_of[0][0] + lasts_of[1][0], lasts_of[0][1] + lasts_of[1][1]
    )
    high = total.astype(BF16).astype(F32)
    middle = (total - high).astype(BF16).astype(F32)
    low = total - high - middle
    tile = jnp.where(tile_row == 0, high, jnp.where(tile_row == 1, middle, low))
    states[sp, 64:80] = tile.astype(BF16)


def on_device(
    tokens, norm_gain, w_query_one, w_query_two, w_key_one, w_key_two, w_value, mix_lambda,
    head_gain, w_ret_query, w_ret_key, w_ret_value, retain_log, init_state, w_out_diff, w_out_ret,
):
    vmem = pl.BlockSpec(memory_space=pltpu.VMEM)
    hbm = pl.BlockSpec(memory_space=pl.ANY)
    dma = pltpu.SemaphoreType.DMA
    return pl.pallas_call(
        kernel,
        out_shape=jax.ShapeDtypeStruct((128, 2048), BF16),
        in_specs=[hbm] * 16,
        out_specs=vmem,
        scratch_shapes=[
            pltpu.VMEM((128, 2048), BF16),
            pltpu.VMEM((1, 2048), F32),
            pltpu.VMEM((1, 2), F32),
            pltpu.VMEM((1, 128), F32),
            pltpu.VMEM((2, 512), F32),
            pltpu.VMEM((2, 64, 128), F32),
            pltpu.VMEM((4, 128, 2048), BF16),
            pltpu.VMEM((2048, 1280), BF16),
            pltpu.VMEM((2, 256, 256), BF16),
            pltpu.VMEM((256, 256), BF16),
            pltpu.VMEM((32, 4, 256, 256), BF16),
            pltpu.VMEM((32, 80, 256), BF16),
            pltpu.VMEM((2, 512, 256), BF16),
            pltpu.VMEM((4, 2, 256, 2048), BF16),
            pltpu.VMEM((2, 4, 256, 256), BF16),
            pltpu.VMEM((2, 4, 128, 256), F32),
            pltpu.VMEM((2, 4, 1, 256), F32),
            pltpu.VMEM((2, 4, 1, 256), F32),
            pltpu.VMEM((8, 2, 256, 256), F32),
            pltpu.VMEM((8, 2, 256, 256), BF16),
            pltpu.VMEM((2, 2, 256, 128), F32),
            pltpu.VMEM((2, 256, 128), F32),
            pltpu.VMEM((2, 128, 128), F32),
            pltpu.VMEM((2, 128, 128), F32),
            pltpu.VMEM((128, 2048), F32),
            pltpu.VMEM((2, 256, 256), BF16),
            pltpu.VMEM((512, 256), BF16),
            pltpu.VMEM((2, 4, 128, 256), BF16),
            dma((9,)),
            dma,
            dma((3,)),
            dma,
            dma((3,)),
            dma((4,)),
            dma((16, 4)),
            dma,
            dma((16, 2)),
            dma((4,)),
            dma((16,)),
            dma,
            dma,
            dma((2,)),
            dma,
            dma((2,)),
            dma,
            dma,
        ],
        compiler_params=pltpu.CompilerParams(
            collective_id=0, has_side_effects=True, vmem_limit_bytes=60 * 1024 * 1024,
        ),
        cost_estimate=pl.CostEstimate(
            flops=20_000_000_000, bytes_accessed=10_000_000, transcendentals=17_000_000
        ),
        name="layer",
    )(
        tokens, norm_gain.reshape(1, -1), w_query_one, w_query_two, w_key_one, w_key_two, w_value,
        mix_lambda.reshape(1, -1), head_gain.reshape(1, -1),
        w_ret_query, w_ret_key, w_ret_value, retain_log, init_state, w_out_diff, w_out_ret,
    )


def solution(mesh):
    both = ("sp", "tp")
    return jax.shard_map(
        on_device,
        mesh=mesh,
        in_specs=(
            P(both, None), P(), P(None, "tp"), P(None, "tp"), P(None, "tp"), P(None, "tp"),
            P(None, "tp"), P("tp"), P(), P(None, "tp"), P(None, "tp"), P(None, "tp"),
            P("tp", "sp"), P("tp", None, None), P("tp", None), P("tp", None),
        ),
        out_specs=P(both, None),
        check_vma=False,
    )
```
